256 devices in a mesh: grp: 2 (over y), sp: 32 (over z, core), tp: 4 (over x).
Axes of the slice: x: 4, y: 2, z: 16, core: 2. Of those that a mesh axis runs over, the one named last changes fastest.
The devices are a block of a 4x16x16 slice.
Arguments:
- residual: bfloat16 [16384, 2048], P(('grp', 'sp')), parts along dimension 0, may hold values from -6 to 6
- queries: bfloat16 [16384, 1024], P(('grp', 'sp'), 'tp'), parts along dimension 0, may hold values from -400 to 400
- keys: bfloat16 [16384, 1024], P(('grp', 'sp'), 'tp'), parts along dimension 0, may hold values from -8 to 8
- values: bfloat16 [16384, 1024], P(('grp', 'sp'), 'tp'), parts along dimension 0, may hold values from -6 to 6
- log_gates: float32 [16384, 16], P(('grp', 'sp'), 'tp'), parts along dimension 0, may hold values from -955 to 0, as said below
- w_out: bfloat16 [1024, 2048], P('tp'), may hold values from -0.75 to 0.75
- norm_gain: float32 [2048], replicated, may hold values from 0.1 to 1.9
- w_gate: bfloat16 [2048, 5632], P('sp', 'tp'), may hold values from -0.125 to 0.125
- w_up: bfloat16 [2048, 5632], P('sp', 'tp'), may hold values from -0.125 to 0.125
- w_down: bfloat16 [5632, 2048], P('tp', 'sp'), may hold values from -0.078125 to 0.078125
Outputs:
- output: bfloat16 [16384, 2048], P(('grp', 'sp', 'tp')), parts along dimension 0
The draws below stay inside these ranges and needn't reach their ends.
There are 2 independent parts, one for each index of `grp`. The reference program is written for one: setup_inputs(seed, part) draws one part's arguments, and reference() takes and returns one part's arrays. A program takes and returns all parts, laid end to end along the dimension named above; an argument that names none is the same for every part. Nothing has to cross between parts.
Inputs may be any that keep to these rules, and one draw needn't show every extreme that they name: `log_gates`: never rises along positions.
All inputs are finite; a program needn't handle non-finite values.
Results may differ from the reference program's by a relative error of at most 0.014.
Values may be sent and summed in bfloat16 or wider, within the bound.
A program may use at most 128 MiB of HBM per device.

```python
import math
import jax
import jax.numpy as jnp
from jax import lax

D = 2048
ATTN_HEAD_COUNT = 16
HEAD_DIM = 64
FF = 5632
TOK_DEV = 256
SEQUENCE_TOKENS = 8192
N_TP = 4


def layout(key):
    random_seed_key = jax.random.fold_in(key, 31)
    random_ordering_key, random_shift_key, random_back_key, random_stride_key, random_spacing_key, random_strong_key, random_select_key, random_spike_key = jax.random.split(random_seed_key, 8)
    block_count = SEQUENCE_TOKENS // TOK_DEV
    inserted_count = block_count - 2
    quarter = max(TOK_DEV // 4, 1)
    head_order = jax.random.permutation(random_ordering_key, ATTN_HEAD_COUNT)
    gradual_heads = head_order < ATTN_HEAD_COUNT // 2
    block_ids = jnp.arange(inserted_count, dtype=jnp.int32) + 2
    places = block_ids * TOK_DEV + jax.random.randint(random_shift_key, (inserted_count,), 0, quarter)
    matches = (block_ids - 1) * TOK_DEV - 1 - jax.random.randint(random_back_key, (inserted_count,), 0, quarter)
    neighbours = matches - jax.random.randint(random_stride_key, (inserted_count,), 1, 5)
    score_gaps = jax.random.uniform(random_spacing_key, (inserted_count, ATTN_HEAD_COUNT), jnp.float32, 1.0, 2.5)
    strong_decline = jax.random.uniform(random_strong_key, (inserted_count, ATTN_HEAD_COUNT), jnp.float32, math.log(0.02), math.log(0.1))
    picked = jax.random.permutation(random_select_key, inserted_count)[:2]
    sudden_spike = jnp.any(jnp.arange(inserted_count, dtype=jnp.int32)[:, None] == picked[None, :], axis=1)
    sudden_decline = jax.random.uniform(random_spike_key, (inserted_count, ATTN_HEAD_COUNT), jnp.float32, math.log(0.5), math.log(0.8))
    gate_changes = jnp.where(gradual_heads[None, :], jnp.where(sudden_spike[:, None], sudden_decline, 0.0), strong_decline)
    return (gradual_heads, places, matches, neighbours, score_gaps, gate_changes)


def planted(key):
    gradual_heads, places, matches, neighbours, score_gaps, gate_changes = layout(key)
    key_query, key_keys = jax.random.split(jax.random.fold_in(key, 11), 2)
    row_width = ATTN_HEAD_COUNT * HEAD_DIM
    query_rows = jnp.clip(jax.random.normal(key_query, (SEQUENCE_TOKENS, row_width), jnp.float32), -6.0, 6.0)
    key_rows = jnp.clip(jax.random.normal(key_keys, (SEQUENCE_TOKENS, row_width), jnp.float32), -6.0, 6.0)
    inserted_count = places.shape[0]
    levels = jnp.array([8.0, 12.0, 16.0], jnp.float32)
    strength = levels[jnp.arange(inserted_count, dtype=jnp.int32) % 3][:, None, None]
    chosen = key_rows[matches].reshape(inserted_count, ATTN_HEAD_COUNT, HEAD_DIM)
    energy = jnp.maximum(jnp.sum(chosen * chosen, axis=-1, keepdims=True), 0.5 * HEAD_DIM)
    planted_rows = strength * 8.0 * math.sqrt(HEAD_DIM) * chosen / energy
    compensate = (score_gaps + gate_changes)[:, :, None]
    neighbour = chosen * (1.0 - compensate / (8.0 * strength))
    query_rows = jnp.clip(query_rows.at[places].set(planted_rows.reshape(inserted_count, row_width)), -400.0, 400.0)
    key_rows = key_rows.at[neighbours].set(neighbour.reshape(inserted_count, row_width))
    return (query_rows, key_rows)


def draw_queries(key, part):
    return planted(key)[0].astype(jnp.bfloat16)


def draw_keys(key, part):
    return planted(key)[1].astype(jnp.bfloat16)


def draw_log_gates(key, part):
    gradual_heads, places, matches, neighbours, score_gaps, gate_changes = layout(key)
    key_factor, key_jitter = jax.random.split(jax.random.fold_in(key, 23), 2)
    block_count = SEQUENCE_TOKENS // TOK_DEV
    block_factor = jnp.exp(jax.random.uniform(key_factor, (block_count, ATTN_HEAD_COUNT), jnp.float32, math.log(0.5), math.log(2.0)))
    block_factor = jnp.repeat(block_factor, TOK_DEV, axis=0)
    roughness = jax.random.uniform(key_jitter, (SEQUENCE_TOKENS, ATTN_HEAD_COUNT), jnp.float32, 0.5, 1.5)
    head_rates = jnp.where(gradual_heads, 0.5 / SEQUENCE_TOKENS, 1.0 / 40.0)
    forget_logits = -head_rates[None, :] * block_factor * roughness
    clusters = jnp.zeros((SEQUENCE_TOKENS, ATTN_HEAD_COUNT), jnp.float32).at[matches].set(gate_changes)
    return jnp.cumsum(forget_logits + clusters, axis=0)


def shard_levels(key, dims, cuts, least, largest):
    def one(position, shards_of):
        steps = jax.random.uniform(jax.random.fold_in(jax.random.fold_in(key, 6), position), (shards_of,), jnp.float32, least / len(cuts), largest / len(cuts))
        return jnp.repeat(jnp.exp(steps), dims[position] // shards_of).reshape((-1,) + (1,) * (len(dims) - position - 1))

    level = one(*cuts[0])
    for cut in cuts[1:]:
        level = level * one(*cut)
    return level


def gaussian(key, shape, spread, limit, shards=(), kind=jnp.bfloat16):
    loudness = shard_levels(key, shape, shards, -0.22, 0.18) if shards else 1.0
    entries = jax.random.normal(key, shape, jnp.float32) * spread * loudness
    return jnp.minimum(jnp.maximum(entries, -limit), limit).astype(kind)


def setup_inputs(seed: int = 0, part: int = 0) -> dict:
    seeds = jax.random.split(jax.random.key(seed), 11)
    part_splits = jax.random.split(jax.random.fold_in(seeds[10], part), 11)
    return {
        "residual": gaussian(part_splits[0], (SEQUENCE_TOKENS, D), 1.0, 6.0, ((0, 32),)),
        "queries": draw_queries(jax.random.fold_in(jax.random.fold_in(seeds[10], part), 71), part),
        "keys": draw_keys(jax.random.fold_in(jax.random.fold_in(seeds[10], part), 71), part),
        "values": gaussian(part_splits[3], (SEQUENCE_TOKENS, ATTN_HEAD_COUNT * HEAD_DIM), 1.0, 6.0, ((0, 32), (1, 4))),
        "log_gates": draw_log_gates(jax.random.fold_in(jax.random.fold_in(seeds[10], part), 71), part),
        "w_out": gaussian(seeds[5], (ATTN_HEAD_COUNT * HEAD_DIM, D), HEAD_DIM ** -0.5, 0.75, ((0, 4),)),
        "norm_gain": jnp.clip(1.0 + 0.18 * jax.random.normal(seeds[6], (D,), jnp.float32), 0.1, 1.9),
        "w_gate": gaussian(seeds[7], (D, FF), D ** -0.5, 0.125, ((0, 32), (1, 4))),
        "w_up": gaussian(seeds[8], (D, FF), D ** -0.5, 0.125, ((0, 32), (1, 4))),
        "w_down": gaussian(seeds[9], (FF, D), FF ** -0.5, 0.078125, ((0, 4), (1, 32))),
    }


def normalize(rows_in, gain):
    floats = rows_in.astype(jnp.float32)
    scaled = floats * lax.rsqrt(lax.optimization_barrier(jnp.mean(floats * floats, axis=-1, keepdims=True)) + 1e-06)
    return (scaled * gain).astype(jnp.bfloat16)

def group_sum(left, right, groups):
    rows_total = left.shape[0]
    width = left.shape[1] // groups
    left_groups = left.reshape(rows_total, groups, width).astype(jnp.float32)
    right_groups = right.reshape(groups, width, right.shape[1]).astype(jnp.float32)
    partial_terms = jnp.einsum('tgc,gcd->gtd', left_groups, right_groups).astype(jnp.bfloat16)
    partial_terms = lax.optimization_barrier(partial_terms)
    return lax.optimization_barrier(jnp.sum(partial_terms.astype(jnp.float32), axis=0))

def reference(residual, queries, keys, values, log_gates, w_out, norm_gain, w_gate, w_up, w_down):
    score_scale = HEAD_DIM ** (-0.5)
    query_heads = queries.reshape(SEQUENCE_TOKENS, ATTN_HEAD_COUNT, HEAD_DIM)
    key_heads = keys.reshape(SEQUENCE_TOKENS, ATTN_HEAD_COUNT, HEAD_DIM).astype(jnp.float32)
    value_heads = values.reshape(SEQUENCE_TOKENS, ATTN_HEAD_COUNT, HEAD_DIM).astype(jnp.float32)
    block_rows = math.gcd(SEQUENCE_TOKENS, 512)
    key_positions = jnp.arange(SEQUENCE_TOKENS, dtype=jnp.int32)

    def one_block(index_block):
        anchor = (index_block * block_rows).astype(jnp.int32)
        query_block = lax.dynamic_slice_in_dim(query_heads, anchor, block_rows, 0).astype(jnp.float32)
        gate_block = lax.dynamic_slice_in_dim(log_gates, anchor, block_rows, 0)
        scores = jnp.einsum('qhd,khd->hqk', query_block, key_heads) * score_scale
        scores = scores + gate_block.T[:, :, None] - log_gates.T[:, None, :]
        query_positions = anchor + jnp.arange(block_rows, dtype=jnp.int32)
        causal = query_positions[:, None] >= key_positions[None, :]
        scores = jnp.where(causal[None], scores, -jnp.inf)
        row_max = lax.optimization_barrier(jnp.max(scores, axis=-1, keepdims=True))
        weights = jnp.where(causal[None], jnp.exp(scores - row_max), 0.0)
        totals = lax.optimization_barrier(jnp.sum(weights, axis=-1))
        rounded = lax.optimization_barrier(weights.astype(jnp.bfloat16)).astype(jnp.float32)
        summed = jnp.einsum('hqk,khd->hqd', rounded, value_heads) / totals[:, :, None]
        return summed.transpose(1, 0, 2).reshape(block_rows, ATTN_HEAD_COUNT * HEAD_DIM).astype(jnp.bfloat16)
    attended = lax.map(one_block, jnp.arange(SEQUENCE_TOKENS // block_rows, dtype=jnp.int32))
    attended = attended.reshape(SEQUENCE_TOKENS, ATTN_HEAD_COUNT * HEAD_DIM)
    projected = group_sum(attended, w_out, N_TP)
    mixed = (residual.astype(jnp.float32) + projected).astype(jnp.bfloat16)
    normed = normalize(mixed, norm_gain)
    gate_proj = jnp.dot(normed, w_gate, preferred_element_type=jnp.float32)
    up_proj = jnp.dot(normed, w_up, preferred_element_type=jnp.float32)
    hidden = (jax.nn.silu(gate_proj) * up_proj).astype(jnp.bfloat16)
    down_sum = group_sum(hidden, w_down, N_TP)
    summed = mixed.astype(jnp.float32) + 0.5 * down_sum
    scaled = summed * lax.rsqrt(lax.optimization_barrier(jnp.mean(summed * summed, axis=-1, keepdims=True)) + 1e-06)
    return scaled.astype(jnp.bfloat16)
```

```python
import functools

import jax
import jax.numpy as jnp
from jax import lax
from jax.experimental import pallas as pl
from jax.experimental.pallas import tpu as pltpu
from jax.sharding import PartitionSpec as P

MESH = pl.DeviceIdType.MESH
F32 = jnp.float32
BF16 = jnp.bfloat16
NT_DIMS = (((1,), (1,)), ((), ()))
LANES = 128


def layer_kernel(
    n_sp, n_tp, heads,
    q_ref, kg_ref, v_ref, res_ref, wout_ref, gain_ref, g_ref, u_ref, d_ref,
    out_ref,
    kbuf, vbuf, gbuf, ubuf, dbuf, q4, m_s, l_s, acc, att, pbuf, rsbuf, resv, mixed, nbuf, hid, dsend, drecv, total,
    send_sem, recv_sem, sib_sem, loc_sem, x_send, x_recv,
):
    s = lax.axis_index("sp")
    t = lax.axis_index("tp")
    c = lax.rem(s, 2)
    z = s // 2
    nz = n_sp // 2
    far, near = nz // 2, nz - 1 - nz // 2
    rows, width = q_ref.shape
    head_width = width // heads
    own_rows = rows // n_tp
    drow, ff = g_ref.shape
    model = drow * n_sp

    def chip(offset):
        return lax.rem(z + offset + nz, nz)

    right = chip(1) * 2 + c
    left = chip(-1) * 2 + c
    sibling = s + 1 - 2 * c
    peers = [lax.rem(t + d, n_tp) for d in range(1, n_tp)]
    sources = [lax.rem(t - d + n_tp, n_tp) for d in range(1, n_tp)]

    half = drow // 2
    views = (
        (kbuf, 0, kbuf.shape[1]), (vbuf, 0, vbuf.shape[1]), (gbuf, 0, drow), (ubuf, 0, drow),
        (dbuf, 0, half), (dbuf, half, half),
    )

    def piece(st, slot):
        buf, start, size = views[st]
        return buf.at[slot, pl.ds(start, size)]

    def reach(st):
        return (far, near) if st % 2 == 0 else (near, far)

    def link_copy(st, slot, direction, step):
        return pltpu.make_async_remote_copy(
            src_ref=piece(st, slot), dst_ref=piece(st, slot), send_sem=send_sem.at[st],
            recv_sem=recv_sem.at[st, direction, step - 1],
            device_id={"sp": right if direction == 0 else left}, device_id_type=MESH,
        )

    def sib_copy(st, slot, index):
        return pltpu.make_async_remote_copy(
            src_ref=piece(st, slot), dst_ref=piece(st, slot), send_sem=send_sem.at[st],
            recv_sem=sib_sem.at[st, index], device_id={"sp": sibling}, device_id_type=MESH,
        )

    def send_own(st):
        for direction in (0, 1):
            link_copy(st, s, direction, 1).start()
        sib_copy(st, s, 0).start()

    def arrive(pair, step):
        for st in pair:
            for direction, limit in enumerate(reach(st)):
                @pl.when(step <= limit)
                def _():
                    slot = chip(-step if direction == 0 else step) * 2 + c
                    link_copy(st, slot, direction, step).wait_recv()

                    @pl.when(step < limit)
                    def _():
                        link_copy(st, slot, direction, step + 1).start()

                    sib_copy(st, slot, step + far * direction).start()

    def sib_arrive(pair, step):
        for st in pair:
            for direction, limit in enumerate(reach(st)):
                @pl.when(jnp.logical_and(step >= 1, step <= limit))
                def _():
                    slot = chip(-step if direction == 0 else step) * 2 + 1 - c
                    sib_copy(st, slot, step + far * direction).wait_recv()

            @pl.when(step == 0)
            def _():
                sib_copy(st, sibling, 0).wait_recv()

    def local(src, st, index):
        buf = views[st][0]
        return pltpu.make_async_copy(src, buf.at[s], loc_sem.at[index])

    own_slice = pl.ds(pl.multiple_of(t * own_rows, own_rows), own_rows)
    loads = [local(kg_ref, 0, 0), local(v_ref, 1, 1), local(g_ref, 2, 2), local(u_ref, 3, 3), local(d_ref, 4, 4)]
    loads.append(pltpu.make_async_copy(res_ref.at[own_slice], resv, loc_sem.at[5]))
    for load in loads:
        load.start()

    barrier = pltpu.get_barrier_semaphore()
    for neighbour in (left, right, sibling):
        pl.semaphore_signal(barrier, inc=1, device_id={"sp": neighbour}, device_id_type=MESH)
    for peer in peers:
        pl.semaphore_signal(barrier, inc=1, device_id={"tp": peer}, device_id_type=MESH)
    pl.semaphore_wait(barrier, 3 + n_tp - 1)

    loads[0].wait()
    send_own(0)
    loads[1].wait()
    send_own(1)
    for load in loads[2:]:
        load.wait()

    scaled = q_ref[...].astype(F32) * (head_width ** -0.5)
    lane_head = lax.broadcasted_iota(jnp.int32, (rows, width), 1) // head_width
    for h in range(heads):
        q4[h] = jnp.where(lane_head == h, scaled, 0.0).astype(BF16)
        m_s[h] = jnp.full((rows, LANES), -1e30, F32)
        l_s[h] = jnp.zeros((rows, LANES), F32)
        acc[h] = jnp.zeros((rows, width), F32)

    def wide(x, size):
        return jnp.concatenate([x] * (size // LANES), axis=1) if size >= LANES else x[:, :size]

    def attend(slot, diagonal):
        key = kbuf[slot, 0:rows, :]
        parts = kbuf[slot, rows:rows + 16, :].astype(F32)
        gates = parts[0:heads] + parts[heads:2 * heads] + parts[2 * heads:3 * heads]
        value = vbuf[slot]
        for h in range(heads):
            score = lax.dot_general(q4[h], key, NT_DIMS, preferred_element_type=F32) - gates[h:h + 1, :rows]
            if diagonal:
                at = lax.broadcasted_iota(jnp.int32, (rows, rows), 0)
                col = lax.broadcasted_iota(jnp.int32, (rows, rows), 1)
                score = jnp.where(col <= at, score, -1e30)
            before = m_s[h]
            top = jnp.maximum(before, jnp.max(score, axis=1, keepdims=True))
            weight = jnp.exp(score - wide(top, rows))
            rescale = jnp.exp(before - top)
            lanes = weight[:, 0:LANES]
            for k in range(1, rows // LANES):
                lanes = lanes + weight[:, k * LANES:(k + 1) * LANES]
            l_s[h] = l_s[h] * rescale + lanes
            product = jnp.dot(weight.astype(BF16), value, preferred_element_type=F32)
            acc[h] = acc[h] * wide(rescale, width) + product
            m_s[h] = top

    attend(s, True)

    kv, gu, dn = (0, 1), (2, 3), (4, 5)

    def kv_step(i, _):
        @pl.when(i <= far)
        def _():
            arrive(kv, i)

        @pl.when(i == far - 1)
        def _():
            for st in gu:
                send_own(st)

        j = i - 1
        sib_arrive(kv, j)

        def block(b, _):
            side, core = b // 2, lax.rem(b, 2)
            offset = jnp.where(side == 0, -j, j)
            earlier = jnp.where(side == 0, z - j >= 0, jnp.logical_and(z + j >= nz, j <= near))
            own_chip = jnp.logical_and(side == 0, jnp.logical_and(core == 0, c == 1))
            needed = jnp.where(j == 0, own_chip, earlier)

            @pl.when(needed)
            def _():
                attend(chip(offset) * 2 + core, False)

            return 0

        lax.fori_loop(0, 4, block, 0)
        return 0

    lax.fori_loop(1, far + 2, kv_step, 0)

    arrive(gu, 1)
    merged = jnp.zeros((rows, width), F32)
    for h in range(heads):
        norm = jnp.sum(l_s[h], axis=1, keepdims=True)
        merged = jnp.where(lane_head == h, acc[h] / norm, merged)
    att[...] = merged.astype(BF16)

    tile = min(512, model)

    def project(k, _):
        at = pl.ds(pl.multiple_of(k * tile, tile), tile)
        y = jnp.dot(att[...], wout_ref[:, at], preferred_element_type=F32).astype(BF16)
        pbuf[:, :, at] = y.reshape(n_tp, own_rows, tile)
        return 0

    lax.fori_loop(0, model // tile, project, 0)

    def reduce_copy(d):
        return pltpu.make_async_remote_copy(
            src_ref=pbuf.at[peers[d]], dst_ref=rsbuf.at[t], send_sem=x_send.at[0], recv_sem=x_recv.at[0, d],
            device_id={"tp": peers[d]}, device_id_type=MESH,
        )

    def gather_copy(d):
        return pltpu.make_async_remote_copy(
            src_ref=nbuf.at[t], dst_ref=nbuf.at[t], send_sem=x_send.at[1], recv_sem=x_recv.at[1, d],
            device_id={"tp": peers[d]}, device_id_type=MESH,
        )

    def arrival(buf, sem):
        return pltpu.make_async_copy(buf, buf, sem)

    for d in range(n_tp - 1):
        reduce_copy(d).start()
    arrive(gu, 2)
    arrive(gu, 3)
    for d in range(n_tp - 1):
        arrival(rsbuf.at[sources[d]], x_recv.at[0, d]).wait()
    summed = resv[...].astype(F32) + pbuf[t].astype(F32)
    for d in range(n_tp - 1):
        summed = summed + rsbuf[sources[d]].astype(F32)
    mixed[...] = summed.astype(BF16)
    floats = mixed[...].astype(F32)
    mean = jnp.sum(floats * floats, axis=1, keepdims=True) * (1.0 / model)
    nbuf[t] = (floats * lax.rsqrt(mean + 1e-6) * gain_ref[...]).astype(BF16)
    for d in range(n_tp - 1):
        gather_copy(d).start()

    def gu_step(i, _):
        @pl.when(i == far)
        def _():
            for st in dn:
                send_own(st)

        arrive(gu, i)
        return 0

    lax.fori_loop(4, far + 1, gu_step, 0)

    def gu_sib(i, _):
        sib_arrive(gu, i)
        return 0

    lax.fori_loop(0, far + 1, gu_sib, 0)
    for d in range(n_tp - 1):
        arrival(nbuf.at[sources[d]], x_recv.at[1, d]).wait()

    def ffn(k, _):
        at = pl.ds(pl.multiple_of(k * LANES, LANES), LANES)
        weights = jnp.concatenate(
            [gbuf[:, :, at].reshape(model, LANES), ubuf[:, :, at].reshape(model, LANES)], axis=1
        )
        both = jnp.dot(nbuf[...].reshape(rows, model), weights, preferred_element_type=F32)
        gate, up = both[:, :LANES], both[:, LANES:]
        hid[:, at] = (gate / (1.0 + jnp.exp(-gate)) * up).astype(BF16)

        @pl.when(jnp.logical_and(lax.rem(k, 3) == 2, (k + 1) // 3 <= far))
        def _():
            arrive(dn, (k + 1) // 3)

        return 0

    tiles = ff // LANES
    lax.fori_loop(0, tiles, ffn, 0)
    handled = tiles // 3

    def column_copy(d, at):
        return pltpu.make_async_remote_copy(
            src_ref=dsend.at[at, peers[d]], dst_ref=drecv.at[t, at], send_sem=x_send.at[2],
            recv_sem=x_recv.at[2, d], device_id={"tp": peers[d]}, device_id_type=MESH,
        )

    def down_step(j, _):
        @pl.when(jnp.logical_and(j + 1 > handled, j + 1 <= far))
        def _():
            arrive(dn, j + 1)

        sib_arrive(dn, j)
        back, ahead = chip(-j), chip(j)
        weights = jnp.concatenate(
            [dbuf[pl.ds(at * 2, 2)].reshape(2 * drow, ff) for at in (back, ahead)], axis=0
        )
        y = lax.dot_general(hid[...], weights, NT_DIMS, preferred_element_type=F32).astype(BF16)
        y = y.reshape(n_tp, own_rows, 4 * drow)
        dsend[back] = y[:, :, :2 * drow]
        for d in range(n_tp - 1):
            column_copy(d, back).start()

        @pl.when(jnp.logical_and(j >= 1, j <= near))
        def _():
            dsend[ahead] = y[:, :, 2 * drow:]
            for d in range(n_tp - 1):
                column_copy(d, ahead).start()

        return 0

    lax.fori_loop(0, far + 1, down_step, 0)

    for d in range(n_tp - 1):
        arrival(drecv.at[sources[d]], x_recv.at[2, d]).wait()
    square = jnp.zeros((own_rows, 2 * drow), F32)
    for at in range(nz):
        cols = slice(at * 2 * drow, (at + 1) * 2 * drow)
        down = dsend[at, t].astype(F32)
        for d in range(n_tp - 1):
            down = down + drecv[sources[d], at].astype(F32)
        value = mixed[:, cols].astype(F32) + 0.5 * down
        total[:, cols] = value
        square = square + value * value
    mean = jnp.sum(square, axis=1, keepdims=True) * (1.0 / model)
    out_ref[...] = (total[...] * lax.rsqrt(mean + 1e-6)).astype(BF16)

    for st in range(len(views)):
        buf, start, size = views[st]
        arrival(buf.at[pl.ds(0, 2 * nz - 1), pl.ds(start, size)], send_sem.at[st]).wait()
    arrival(pbuf.at[pl.ds(0, n_tp - 1)], x_send.at[0]).wait()
    arrival(nbuf.at[pl.ds(0, n_tp - 1)], x_send.at[1]).wait()
    arrival(drecv.at[pl.ds(0, n_tp - 1)], x_send.at[2]).wait()


def body(residual, queries, keys, values, log_gates, w_out, norm_gain, w_gate, w_up, w_down):
    n_sp, n_tp = lax.axis_size("sp"), lax.axis_size("tp")
    rows, width = queries.shape
    heads = log_gates.shape[1]
    model = residual.shape[1]
    drow, ff = w_gate.shape
    own_rows = rows // n_tp
    nz = n_sp // 2
    far = nz // 2

    gates = log_gates.T
    high = lax.reduce_precision(gates, 8, 7)
    middle = lax.reduce_precision(gates - high, 8, 7)
    low = gates - high - middle
    extra = jnp.concatenate([high, middle, low, jnp.zeros((16 - 3 * heads, rows), F32)], axis=0).astype(BF16)
    if rows < width:
        extra = jnp.pad(extra, ((0, 0), (0, width - rows)))
    keys_gates = jnp.concatenate([keys, extra], axis=0)

    vmem = pl.BlockSpec(memory_space=pltpu.VMEM)
    hbm = pl.BlockSpec(memory_space=pl.ANY)
    return pl.pallas_call(
        functools.partial(layer_kernel, n_sp, n_tp, heads),
        out_shape=jax.ShapeDtypeStruct((own_rows, model), BF16),
        in_specs=[vmem, hbm, hbm, hbm, vmem, vmem, hbm, hbm, hbm],
        out_specs=vmem,
        scratch_shapes=[
            pltpu.VMEM((n_sp, rows + 16, width), BF16),
            pltpu.VMEM((n_sp, rows, width), BF16),
            pltpu.VMEM((n_sp, drow, ff), BF16),
            pltpu.VMEM((n_sp, drow, ff), BF16),
            pltpu.VMEM((n_sp, drow, ff), BF16),
            pltpu.VMEM((heads, rows, width), BF16),
            pltpu.VMEM((heads, rows, LANES), F32),
            pltpu.VMEM((heads, rows, LANES), F32),
            pltpu.VMEM((heads, rows, width), F32),
            pltpu.VMEM((rows, width), BF16),
            pltpu.VMEM((n_tp, own_rows, model), BF16),
            pltpu.VMEM((n_tp, own_rows, model), BF16),
            pltpu.VMEM((own_rows, model), BF16),
            pltpu.VMEM((own_rows, model), BF16),
            pltpu.VMEM((n_tp, own_rows, model), BF16),
            pltpu.VMEM((rows, ff), BF16),
            pltpu.VMEM((nz, n_tp, own_rows, 2 * drow), BF16),
            pltpu.VMEM((n_tp, nz, own_rows, 2 * drow), BF16),
            pltpu.VMEM((own_rows, model), F32),
            pltpu.SemaphoreType.DMA((6,)),
            pltpu.SemaphoreType.DMA((6, 2, far)),
            pltpu.SemaphoreType.DMA((6, 2 * far + 1)),
            pltpu.SemaphoreType.DMA((6,)),
            pltpu.SemaphoreType.DMA((3,)),
            pltpu.SemaphoreType.DMA((3, n_tp - 1)),
        ],
        compiler_params=pltpu.CompilerParams(
            collective_id=0, has_side_effects=True, vmem_limit_bytes=60 * 1024 * 1024
        ),
    )(queries, keys_gates, values, residual, w_out, norm_gain.reshape(1, -1), w_gate, w_up, w_down.T)


def solution(mesh):
    in_specs = (
        P(("grp", "sp"), None),
        P(("grp", "sp"), "tp"),
        P(("grp", "sp"), "tp"),
        P(("grp", "sp"), "tp"),
        P(("grp", "sp"), "tp"),
        P("tp", None),
        P(),
        P("sp", "tp"),
        P("sp", "tp"),
        P("tp", "sp"),
    )
    out_specs = P(("grp", "sp", "tp"), None)
    return jax.shard_map(body, mesh=mesh, in_specs=in_specs, out_specs=out_specs, check_vma=False)
```

```python
import functools

import jax
import jax.numpy as jnp
from jax import lax
from jax.experimental import pallas as pl
from jax.experimental.pallas import tpu as pltpu
from jax.sharding import PartitionSpec as P

MESH = pl.DeviceIdType.MESH
F32 = jnp.float32
BF16 = jnp.bfloat16
NT_DIMS = (((1,), (1,)), ((), ()))
LANES = 128


def layer_kernel(
    n_sp, n_tp, heads,
    q_ref, k_ref, x_ref, v_ref, res_ref, wout_ref, gain_ref, g_ref, u_ref, d_ref,
    out_ref,
    kbuf, vbuf, gbuf, ubuf, dbuf, q4, m_s, l_s, acc, att, pbuf, rsbuf, resv, mixed, nbuf, hacc, hid, dsend, drecv, total,
    send_sem, recv_sem, sib_sem, loc_sem, x_send, x_recv, ack,
):
    s = lax.axis_index("sp")
    t = lax.axis_index("tp")
    c = lax.rem(s, 2)
    z = s // 2
    nz = n_sp // 2
    far, near = nz // 2, nz - 1 - nz // 2
    rows, width = q_ref.shape
    head_width = width // heads
    own_rows = rows // n_tp
    drow, ff = g_ref.shape
    model = drow * n_sp

    def chip(offset):
        return lax.rem(z + offset + nz, nz)

    right = chip(1) * 2 + c
    left = chip(-1) * 2 + c
    sibling = s + 1 - 2 * c
    peers = [lax.rem(t + d, n_tp) for d in range(1, n_tp)]
    sources = [lax.rem(t - d + n_tp, n_tp) for d in range(1, n_tp)]

    half = drow // 2
    views = (
        (kbuf, 0, kbuf.shape[1]), (vbuf, 0, vbuf.shape[1]), (gbuf, 0, drow), (ubuf, 0, drow),
        (dbuf, 0, half), (dbuf, half, half),
    )

    def piece(st, slot):
        buf, start, size = views[st]
        return buf.at[slot, pl.ds(start, size)]

    def reach(st):
        return (far, near) if st % 2 == 0 else (near, far)

    def link_copy(st, slot, direction, step):
        return pltpu.make_async_remote_copy(
            src_ref=piece(st, slot), dst_ref=piece(st, slot), send_sem=send_sem.at[st],
            recv_sem=recv_sem.at[st, direction, step - 1],
            device_id={"sp": jnp.where(direction == 0, right, left)}, device_id_type=MESH,
        )

    def sib_copy(st, slot, index):
        return pltpu.make_async_remote_copy(
            src_ref=piece(st, slot), dst_ref=piece(st, slot), send_sem=send_sem.at[st],
            recv_sem=sib_sem.at[st, index], device_id={"sp": sibling}, device_id_type=MESH,
        )

    def send_own(st):
        for direction in (0, 1):
            link_copy(st, s, direction, 1).start()
        sib_copy(st, s, 0).start()

    def sib_send(st, step):
        for direction, limit in enumerate(reach(st)):
            @pl.when(step <= limit)
            def _():
                slot = chip(-step if direction == 0 else step) * 2 + c
                sib_copy(st, slot, step + far * direction).start()

    def arrive(st, step):
        for direction, limit in enumerate(reach(st)):
            @pl.when(step <= limit)
            def _():
                slot = chip(-step if direction == 0 else step) * 2 + c
                link_copy(st, slot, direction, step).wait_recv()

                @pl.when(step < limit)
                def _():
                    link_copy(st, slot, direction, step + 1).start()

    def arrive_both(st, step):
        arrive(st, step)
        sib_send(st, step)

    def sib_arrive(pair, step):
        for st in pair:
            for direction, limit in enumerate(reach(st)):
                @pl.when(jnp.logical_and(step >= 1, step <= limit))
                def _():
                    slot = chip(-step if direction == 0 else step) * 2 + 1 - c
                    sib_copy(st, slot, step + far * direction).wait_recv()

            @pl.when(step == 0)
            def _():
                sib_copy(st, sibling, 0).wait_recv()

    def local(src, dst, index):
        return pltpu.make_async_copy(src, dst, loc_sem.at[index])

    own_slice = pl.ds(pl.multiple_of(t * own_rows, own_rows), own_rows)
    loads = [
        local(k_ref, kbuf.at[s, pl.ds(0, rows)], 0), local(x_ref, kbuf.at[s, pl.ds(rows, 16)], 1),
        local(v_ref, vbuf.at[s], 2), local(g_ref, gbuf.at[s], 3), local(u_ref, ubuf.at[s], 4),
        local(d_ref, dbuf.at[s], 5), local(res_ref.at[own_slice], resv, 6),
    ]
    for load in loads:
        load.start()

    lower = [z > 0, z == nz - 1, c == 1] + [peer < t for peer in peers]
    axis = ["sp", "sp", "sp"] + ["tp"] * (n_tp - 1)
    partner = [left, right, sibling] + peers
    theirs = [1, 0, 2] + [2 + n_tp - d for d in range(1, n_tp)]
    barrier = pltpu.get_barrier_semaphore()
    for k in range(2 + n_tp):
        @pl.when(lower[k])
        def _():
            pl.semaphore_signal(barrier, inc=1, device_id={axis[k]: partner[k]}, device_id_type=MESH)

    higher = sum(jnp.where(low, 0, 1) for low in lower)

    @pl.when(higher > 0)
    def _():
        pl.semaphore_wait(barrier, higher)

    for k in range(2 + n_tp):
        @pl.when(jnp.logical_not(lower[k]))
        def _():
            pl.semaphore_signal(
                ack.at[theirs[k]], inc=1, device_id={axis[k]: partner[k]}, device_id_type=MESH
            )

    def ready(k):
        @pl.when(lower[k])
        def _():
            pl.semaphore_wait(ack.at[k], 1)

    last = z == nz - 1
    loads[0].wait()
    loads[1].wait()
    loads[2].wait()
    for turn in (0, 1):
        for direction in (0, 1):
            @pl.when(last == (direction != turn))
            def _():
                ready(1 - direction)
                link_copy(0, s, direction, 1).start()
                link_copy(1, s, direction, 1).start()

    for load in loads[3:]:
        load.wait()

    scaled = q_ref[...].astype(F32) * (head_width ** -0.5)
    lane_head = lax.broadcasted_iota(jnp.int32, (rows, width), 1) // head_width
    for h in range(heads):
        q4[h] = jnp.where(lane_head == h, scaled, 0.0).astype(BF16)
        m_s[h] = jnp.full((rows, LANES), -1e30, F32)
        l_s[h] = jnp.zeros((rows, LANES), F32)
        acc[h] = jnp.zeros((rows, width), F32)

    def wide(x, size):
        return jnp.concatenate([x] * (size // LANES), axis=1) if size >= LANES else x[:, :size]

    def attend(slot, diagonal):
        key = kbuf[slot, 0:rows, :]
        parts = kbuf[slot, rows:rows + 16, :].astype(F32)
        gates = parts[0:heads] + parts[heads:2 * heads] + parts[2 * heads:3 * heads]
        value = vbuf[slot]
        for h in range(heads):
            score = lax.dot_general(q4[h], key, NT_DIMS, preferred_element_type=F32) - gates[h:h + 1, :rows]
            if diagonal:
                at = lax.broadcasted_iota(jnp.int32, (rows, rows), 0)
                col = lax.broadcasted_iota(jnp.int32, (rows, rows), 1)
                score = jnp.where(col <= at, score, -1e30)
            before = m_s[h]
            top = jnp.maximum(before, jnp.max(score, axis=1, keepdims=True))
            weight = jnp.exp(score - wide(top, rows))
            rescale = jnp.exp(before - top)
            lanes = weight[:, 0:LANES]
            for k in range(1, rows // LANES):
                lanes = lanes + weight[:, k * LANES:(k + 1) * LANES]
            l_s[h] = l_s[h] * rescale + lanes
            product = jnp.dot(weight.astype(BF16), value, preferred_element_type=F32)
            acc[h] = acc[h] * wide(rescale, width) + product
            m_s[h] = top

    attend(s, True)

    kv, gu, dn = (0, 1), (2, 3), (4, 5)
    hold = min(3, far - 1)

    def kv_step(i, _):
        for half, st in enumerate(kv):
            @pl.when(i <= far)
            def _():
                arrive(st, i)

                @pl.when(i == hold)
                def _():
                    if half == 0:
                        ready(2)
                    sib_copy(st, s, 0).start()
                    for step in range(1, hold):
                        sib_send(st, step)

                @pl.when(i >= hold)
                def _():
                    sib_send(st, i)

            if half == 1:
                @pl.when(i == far - 1)
                def _():
                    for own in gu:
                        send_own(own)

            late = 2 * (i - far // 2 - 1) + half

            @pl.when(jnp.logical_and(late >= 0, late <= far))
            def _():
                sib_arrive(kv, late)

            def block(b, _):
                own = b == 0
                j = jnp.where(own, i - 1, late)
                core = jnp.where(own, c, 1 - c)
                back = jnp.where(own, half == 0, b == 1)
                offset = jnp.where(back, -j, j)
                earlier = jnp.where(back, z - j >= 0, jnp.logical_and(z + j >= nz, j <= near))
                at_home = jnp.logical_and(jnp.logical_not(own), jnp.logical_and(back, c == 1))
                needed = jnp.where(j == 0, at_home, earlier)

                @pl.when(jnp.logical_and(needed, jnp.logical_and(j >= 0, j <= far)))
                def _():
                    attend(chip(offset) * 2 + core, False)

                return 0

            lax.fori_loop(0, 3, block, 0)
        return 0

    lax.fori_loop(1, far + 2, kv_step, 0)

    for st in gu:
        arrive_both(st, 1)
    merged = jnp.zeros((rows, width), F32)
    for h in range(heads):
        norm = jnp.sum(l_s[h], axis=1, keepdims=True)
        merged = jnp.where(lane_head == h, acc[h] / norm, merged)
    att[...] = merged.astype(BF16)

    tile = min(512, model)

    def project(k, _):
        at = pl.ds(pl.multiple_of(k * tile, tile), tile)
        y = jnp.dot(att[...], wout_ref[:, at], preferred_element_type=F32).astype(BF16)
        pbuf[:, :, at] = y.reshape(n_tp, own_rows, tile)
        return 0

    lax.fori_loop(0, model // tile, project, 0)

    def reduce_copy(d):
        return pltpu.make_async_remote_copy(
            src_ref=pbuf.at[peers[d]], dst_ref=rsbuf.at[t], send_sem=x_send.at[0], recv_sem=x_recv.at[0, d],
            device_id={"tp": peers[d]}, device_id_type=MESH,
        )

    def gather_copy(d):
        return pltpu.make_async_remote_copy(
            src_ref=nbuf.at[t], dst_ref=nbuf.at[t], send_sem=x_send.at[1], recv_sem=x_recv.at[1, d],
            device_id={"tp": peers[d]}, device_id_type=MESH,
        )

    def arrival(buf, sem):
        return pltpu.make_async_copy(buf, buf, sem)

    arrive_both(gu[0], 2)
    for d in range(n_tp - 1):
        ready(3 + d)
        reduce_copy(d).start()
    arrive_both(gu[1], 2)
    for st in gu:
        arrive_both(st, 3)
    for d in range(n_tp - 1):
        arrival(rsbuf.at[sources[d]], x_recv.at[0, d]).wait()
    summed = resv[...].astype(F32) + pbuf[t].astype(F32)
    for d in range(n_tp - 1):
        summed = summed + rsbuf[sources[d]].astype(F32)
    mixed[...] = summed.astype(BF16)
    floats = mixed[...].astype(F32)
    mean = jnp.sum(floats * floats, axis=1, keepdims=True) * (1.0 / model)
    nbuf[t] = (floats * lax.rsqrt(mean + 1e-6) * gain_ref[...]).astype(BF16)
    for d in range(n_tp - 1):
        gather_copy(d).start()

    def gu_step(i, _):
        for st in gu:
            arrive_both(st, i)
        return 0

    lax.fori_loop(4, far - 2, gu_step, 0)

    tiles = ff // LANES
    chip_rows = 2 * drow

    def accumulate(offsets, first, final):
        for j in sorted({abs(o) for o in offsets}):
            sib_arrive(gu, j)
        chips = [chip(o) for o in offsets]
        left_side = jnp.concatenate(
            [nbuf[:, :, pl.ds(pl.multiple_of(at * chip_rows, chip_rows), chip_rows)] for at in chips], axis=2
        ).reshape(rows, len(chips) * chip_rows)

        def one(k, _):
            at = pl.ds(pl.multiple_of(k * LANES, LANES), LANES)
            sides = [
                jnp.concatenate(
                    [buf[pl.ds(2 * chosen, 2), :, at].reshape(chip_rows, LANES) for chosen in chips], axis=0
                )
                for buf in (gbuf, ubuf)
            ]
            both = jnp.dot(left_side, jnp.concatenate(sides, axis=1), preferred_element_type=F32)
            if not first:
                both = both + hacc[k]
            if final:
                gate, up = both[:, :LANES], both[:, LANES:]
                hid[:, at] = (gate / (1.0 + jnp.exp(-gate)) * up).astype(BF16)
            else:
                hacc[k] = both
            return 0

        lax.fori_loop(0, tiles, one, 0)

    def around(*distances):
        return [o for j in distances for o in (-j, j)]

    arrive_both(gu[0], far - 2)
    for d in range(n_tp - 1):
        arrival(nbuf.at[sources[d]], x_recv.at[1, d]).wait()
    accumulate([0] + around(1), True, False)
    arrive_both(gu[1], far - 2)
    accumulate(around(2, 3), False, False)
    arrive_both(gu[0], far - 1)
    accumulate(around(*range(4, far - 2)), False, False)
    arrive_both(gu[1], far - 1)
    for st in dn:
        send_own(st)
    accumulate(around(far - 2), False, False)
    arrive_both(gu[0], far)
    accumulate(around(far - 1), False, False)
    arrive_both(gu[1], far)
    accumulate([-far], False, True)

    def column_copy(d, at):
        return pltpu.make_async_remote_copy(
            src_ref=dsend.at[at, peers[d]], dst_ref=drecv.at[t, at], send_sem=x_send.at[2],
            recv_sem=x_recv.at[2, d], device_id={"tp": peers[d]}, device_id_type=MESH,
        )

    def down_step(j, _):
        @pl.when(j + 1 <= far)
        def _():
            for st in dn:
                arrive_both(st, j + 1)

        sib_arrive(dn, j)
        back, ahead = chip(-j), chip(j)
        weights = jnp.concatenate(
            [dbuf[pl.ds(at * 2, 2)].reshape(2 * drow, ff) for at in (back, ahead)], axis=0
        )
        y = lax.dot_general(hid[...], weights, NT_DIMS, preferred_element_type=F32).astype(BF16)
        y = y.reshape(n_tp, own_rows, 4 * drow)
        dsend[back] = y[:, :, :2 * drow]
        for d in range(n_tp - 1):
            column_copy(d, back).start()

        @pl.when(jnp.logical_and(j >= 1, j <= near))
        def _():
            dsend[ahead] = y[:, :, 2 * drow:]
            for d in range(n_tp - 1):
                column_copy(d, ahead).start()

        return 0

    lax.fori_loop(0, far + 1, down_step, 0)

    for d in range(n_tp - 1):
        arrival(drecv.at[sources[d]], x_recv.at[2, d]).wait()
    square = jnp.zeros((own_rows, 2 * drow), F32)
    for at in range(nz):
        cols = slice(at * 2 * drow, (at + 1) * 2 * drow)
        down = dsend[at, t].astype(F32)
        for d in range(n_tp - 1):
            down = down + drecv[sources[d], at].astype(F32)
        value = mixed[:, cols].astype(F32) + 0.5 * down
        total[:, cols] = value
        square = square + value * value
    mean = jnp.sum(square, axis=1, keepdims=True) * (1.0 / model)
    out_ref[...] = (total[...] * lax.rsqrt(mean + 1e-6)).astype(BF16)

    for st in range(len(views)):
        buf, start, size = views[st]
        arrival(buf.at[pl.ds(0, 2 * nz - 1), pl.ds(start, size)], send_sem.at[st]).wait()
    arrival(pbuf.at[pl.ds(0, n_tp - 1)], x_send.at[0]).wait()
    arrival(nbuf.at[pl.ds(0, n_tp - 1)], x_send.at[1]).wait()
    arrival(drecv.at[pl.ds(0, n_tp - 1)], x_send.at[2]).wait()


def body(residual, queries, keys, values, log_gates, w_out, norm_gain, w_gate, w_up, w_down):
    n_sp, n_tp = lax.axis_size("sp"), lax.axis_size("tp")
    rows, width = queries.shape
    heads = log_gates.shape[1]
    model = residual.shape[1]
    drow, ff = w_gate.shape
    own_rows = rows // n_tp
    nz = n_sp // 2
    far = nz // 2

    gates = log_gates.T
    high = lax.reduce_precision(gates, 8, 7)
    middle = lax.reduce_precision(gates - high, 8, 7)
    low = gates - high - middle
    extra = jnp.concatenate([high, middle, low, jnp.zeros((16 - 3 * heads, rows), F32)], axis=0).astype(BF16)
    vmem = pl.BlockSpec(memory_space=pltpu.VMEM)
    hbm = pl.BlockSpec(memory_space=pl.ANY)
    return pl.pallas_call(
        functools.partial(layer_kernel, n_sp, n_tp, heads),
        out_shape=jax.ShapeDtypeStruct((own_rows, model), BF16),
        in_specs=[vmem, hbm, hbm, hbm, hbm, vmem, vmem, hbm, hbm, hbm],
        out_specs=vmem,
        scratch_shapes=[
            pltpu.VMEM((n_sp, rows + 16, width), BF16),
            pltpu.VMEM((n_sp, rows, width), BF16),
            pltpu.VMEM((n_sp, drow, ff), BF16),
            pltpu.VMEM((n_sp, drow, ff), BF16),
            pltpu.VMEM((n_sp, drow, ff), BF16),
            pltpu.VMEM((heads, rows, width), BF16),
            pltpu.VMEM((heads, rows, LANES), F32),
            pltpu.VMEM((heads, rows, LANES), F32),
            pltpu.VMEM((heads, rows, width), F32),
            pltpu.VMEM((rows, width), BF16),
            pltpu.VMEM((n_tp, own_rows, model), BF16),
            pltpu.VMEM((n_tp, own_rows, model), BF16),
            pltpu.VMEM((own_rows, model), BF16),
            pltpu.VMEM((own_rows, model), BF16),
            pltpu.VMEM((n_tp, own_rows, model), BF16),
            pltpu.VMEM((ff // LANES, rows, 2 * LANES), F32),
            pltpu.VMEM((rows, ff), BF16),
            pltpu.VMEM((nz, n_tp, own_rows, 2 * drow), BF16),
            pltpu.VMEM((n_tp, nz, own_rows, 2 * drow), BF16),
            pltpu.VMEM((own_rows, model), F32),
            pltpu.SemaphoreType.DMA((6,)),
            pltpu.SemaphoreType.DMA((6, 2, far)),
            pltpu.SemaphoreType.DMA((6, 2 * far + 1)),
            pltpu.SemaphoreType.DMA((7,)),
            pltpu.SemaphoreType.DMA((3,)),
            pltpu.SemaphoreType.DMA((3, n_tp - 1)),
            pltpu.SemaphoreType.REGULAR((2 + n_tp,)),
        ],
        compiler_params=pltpu.CompilerParams(
            collective_id=0, has_side_effects=True, vmem_limit_bytes=60 * 1024 * 1024
        ),
    )(queries, keys, extra, values, residual, w_out, norm_gain.reshape(1, -1), w_gate, w_up, w_down.T)


def solution(mesh):
    in_specs = (
        P(("grp", "sp"), None),
        P(("grp", "sp"), "tp"),
        P(("grp", "sp"), "tp"),
        P(("grp", "sp"), "tp"),
        P(("grp", "sp"), "tp"),
        P("tp", None),
        P(),
        P("sp", "tp"),
        P("sp", "tp"),
        P("tp", "sp"),
    )
    out_specs = P(("grp", "sp", "tp"), None)
    return jax.shard_map(body, mesh=mesh, in_specs=in_specs, out_specs=out_specs, check_vma=False)
```

```python
import functools

import jax
import jax.numpy as jnp
from jax import lax
from jax.experimental import pallas as pl
from jax.experimental.pallas import tpu as pltpu
from jax.sharding import PartitionSpec as P

MESH = pl.DeviceIdType.MESH
F32 = jnp.float32
BF16 = jnp.bfloat16
NT_DIMS = (((1,), (1,)), ((), ()))
LANES = 128


def layer_kernel(
    n_sp, n_tp, heads,
    q_ref, k_ref, x_ref, v_ref, res_ref, wout_ref, gain_ref, g_ref, u_ref, d_ref,
    out_ref,
    kbuf, vbuf, gbuf, ubuf, dbuf, q4, m_s, l_s, acc, att, pbuf, rsbuf, resv, mixed, nbuf, hacc, hid, dsend, drecv, total,
    qfar, ofar, osend, sfar, ssend,
    send_sem, recv_sem, sib_sem, loc_sem, x_send, x_recv, ack, kv_send, kv_sib, pair_sem,
):
    s = lax.axis_index("sp")
    t = lax.axis_index("tp")
    c = lax.rem(s, 2)
    z = s // 2
    nz = n_sp // 2
    far, near = nz // 2, nz - 1 - nz // 2
    rows, width = q_ref.shape
    head_width = width // heads
    own_rows = rows // n_tp
    drow, ff = g_ref.shape
    model = drow * n_sp

    def chip(offset):
        return lax.rem(z + offset + nz, nz)

    right = chip(1) * 2 + c
    left = chip(-1) * 2 + c
    sibling = s + 1 - 2 * c
    pair = chip(far) * 2 + c
    upper = z >= far
    peers = [lax.rem(t + d, n_tp) for d in range(1, n_tp)]
    sources = [lax.rem(t - d + n_tp, n_tp) for d in range(1, n_tp)]

    half = drow // 2
    views = (
        (kbuf, 0, kbuf.shape[1]), (vbuf, 0, vbuf.shape[1]), (gbuf, 0, drow), (ubuf, 0, drow),
        (dbuf, 0, half), (dbuf, half, half),
    )

    def piece(st, slot):
        buf, start, size = views[st]
        return buf.at[slot, pl.ds(start, size)]

    reaches = ((near, 0), (near, 0), (near - 1, far + 1), (near, far), (near, far), (near, far))
    ways = nz

    def reach(st):
        return reaches[st]

    def link_copy(st, slot, direction, step):
        return pltpu.make_async_remote_copy(
            src_ref=piece(st, slot), dst_ref=piece(st, slot),
            send_sem=kv_send.at[st, step - 1] if st < 2 else send_sem.at[st],
            recv_sem=recv_sem.at[st, direction, step - 1],
            device_id={"sp": right if direction == 0 else left}, device_id_type=MESH,
        )

    def sib_copy(st, slot, index):
        return pltpu.make_async_remote_copy(
            src_ref=piece(st, slot), dst_ref=piece(st, slot),
            send_sem=kv_sib.at[st, index] if st < 2 else send_sem.at[st],
            recv_sem=sib_sem.at[st, index], device_id={"sp": sibling}, device_id_type=MESH,
        )

    def usable(st, direction, step):
        fits = jnp.logical_and(step >= 1, step <= reach(st)[direction])
        return jnp.logical_and(fits, z - step >= 0) if st < 2 else fits

    def source(direction, step):
        return chip(-step if direction == 0 else step)

    def send_own(st, direction):
        link_copy(st, s, direction, 1).start()

    def arrive(st, direction, step):
        @pl.when(usable(st, direction, step))
        def _():
            slot = source(direction, step) * 2 + c
            link_copy(st, slot, direction, step).wait_recv()
            onward = step < reach(st)[direction]

            @pl.when(jnp.logical_and(onward, z < nz - 1) if st < 2 else onward)
            def _():
                link_copy(st, slot, direction, step + 1).start()

            sib_copy(st, slot, step + ways * direction).start()

    def sib_arrive(pair_of, step):
        for st in pair_of:
            for direction in (0, 1):
                @pl.when(usable(st, direction, step))
                def _():
                    slot = source(direction, step) * 2 + 1 - c
                    sib_copy(st, slot, step + ways * direction).wait_recv()

            @pl.when(step == 0)
            def _():
                sib_copy(st, sibling, 0).wait_recv()

    def local(src, dst, index):
        return pltpu.make_async_copy(src, dst, loc_sem.at[index])

    own_slice = pl.ds(pl.multiple_of(t * own_rows, own_rows), own_rows)
    loads = [
        local(k_ref, kbuf.at[s, pl.ds(0, rows)], 0), local(x_ref, kbuf.at[s, pl.ds(rows, 16)], 1),
        local(v_ref, vbuf.at[s], 2), local(g_ref, gbuf.at[s], 3), local(u_ref, ubuf.at[s], 4),
        local(d_ref, dbuf.at[s], 5), local(res_ref.at[own_slice], resv, 6),
    ]
    for load in loads:
        load.start()

    lower = [z == 0, z < nz - 1, c == 1, jnp.logical_not(upper)] + [peer < t for peer in peers]
    axis = ["sp", "sp", "sp", "sp"] + ["tp"] * (n_tp - 1)
    partner = [left, right, sibling, pair] + peers
    theirs = [1, 0, 2, 3] + [3 + n_tp - d for d in range(1, n_tp)]
    barrier = pltpu.get_barrier_semaphore()
    for k in range(3 + n_tp):
        @pl.when(lower[k])
        def _():
            pl.semaphore_signal(barrier, inc=1, device_id={axis[k]: partner[k]}, device_id_type=MESH)

    higher = sum(jnp.where(low, 0, 1) for low in lower)

    @pl.when(higher > 0)
    def _():
        pl.semaphore_wait(barrier, higher)

    for k in range(3 + n_tp):
        @pl.when(jnp.logical_not(lower[k]))
        def _():
            pl.semaphore_signal(
                ack.at[theirs[k]], inc=1, device_id={axis[k]: partner[k]}, device_id_type=MESH
            )

    def ready(k):
        @pl.when(lower[k])
        def _():
            pl.semaphore_wait(ack.at[k], 1)

    kv, gu, dn = (0, 1), (2, 3), (4, 5)
    edge = jnp.logical_or(z == 0, z == nz - 1)
    for load in loads[:3]:
        load.wait()
    ready(1)

    @pl.when(z < nz - 1)
    def _():
        for st in kv:
            send_own(st, 0)

    query_copy = pltpu.make_async_remote_copy(
        src_ref=q_ref, dst_ref=qfar, send_sem=pair_sem.at[0], recv_sem=pair_sem.at[1],
        device_id={"sp": pair}, device_id_type=MESH,
    )

    @pl.when(upper)
    def _():
        query_copy.start()

    for load in loads[3:]:
        load.wait()

    @pl.when(edge)
    def _():
        for st in gu:
            send_own(st, 0)

    ready(2)
    for st in kv:
        sib_copy(st, s, 0).start()
    ready(0)
    for st in gu:
        send_own(st, 1)
    for st in gu + dn:
        sib_copy(st, s, 0).start()

    lane_head = lax.broadcasted_iota(jnp.int32, (rows, width), 1) // head_width

    def prepare(which, ref):
        scaled = ref[...].astype(F32) * (head_width ** -0.5)
        for h in range(heads):
            q4[which, h] = jnp.where(lane_head == h, scaled, 0.0).astype(BF16)
            m_s[which, h] = jnp.full((rows, LANES), -1e30, F32)
            l_s[which, h] = jnp.zeros((rows, LANES), F32)
            acc[which, h] = jnp.zeros((rows, width), F32)

    prepare(0, q_ref)

    def wide(x, size):
        return jnp.concatenate([x] * (size // LANES), axis=1) if size >= LANES else x[:, :size]

    def attend(which, slot, diagonal):
        key = kbuf[slot, 0:rows, :]
        parts = kbuf[slot, rows:rows + 16, :].astype(F32)
        gates = parts[0:heads] + parts[heads:2 * heads] + parts[2 * heads:3 * heads]
        value = vbuf[slot]
        for h in range(heads):
            score = lax.dot_general(q4[which, h], key, NT_DIMS, preferred_element_type=F32) - gates[h:h + 1, :rows]
            if diagonal:
                at = lax.broadcasted_iota(jnp.int32, (rows, rows), 0)
                col = lax.broadcasted_iota(jnp.int32, (rows, rows), 1)
                score = jnp.where(col <= at, score, -1e30)
            before = m_s[which, h]
            top = jnp.maximum(before, jnp.max(score, axis=1, keepdims=True))
            weight = jnp.exp(score - wide(top, rows))
            rescale = jnp.exp(before - top)
            lanes = weight[:, 0:LANES]
            for k in range(1, rows // LANES):
                lanes = lanes + weight[:, k * LANES:(k + 1) * LANES]
            l_s[which, h] = l_s[which, h] * rescale + lanes
            product = jnp.dot(weight.astype(BF16), value, preferred_element_type=F32)
            acc[which, h] = acc[which, h] * wide(rescale, width) + product
            m_s[which, h] = top

    attend(0, s, True)

    ahead_from = near - 1

    def kv_step(i, _):
        for half, st in enumerate(kv):
            arrive(st, 0, i)
            if half == 1:
                @pl.when(jnp.logical_and(jnp.logical_not(edge), i == jnp.minimum(z, near - 1)))
                def _():
                    for own in gu:
                        send_own(own, 0)

                @pl.when(lax.rem(i, 2) == 0)
                def _():
                    for own in gu:
                        arrive(own, 1, jnp.where(i <= near, i // 2, 0))

                @pl.when(i <= far)
                def _():
                    sib_arrive(kv, i - 1)

                @pl.when(jnp.logical_and(i == ahead_from - 1, jnp.logical_not(upper)))
                def _():
                    query_copy.wait_recv()
                    prepare(1, qfar)

            turn = 2 * (i - ahead_from) + half

            def block(b, _):
                which = jnp.where(b == 0, 0, 1)
                j = jnp.where(b == 0, i - 1, turn)
                core = jnp.where(b == 0, c if half == 0 else 1 - c, b - 1)
                fits = jnp.logical_and(jnp.logical_and(j >= 0, j <= near), z - j >= 0)
                own = jnp.logical_or(j > 0, jnp.logical_and(half == 1, c == 1))
                needed = jnp.logical_and(fits, jnp.where(b == 0, own, jnp.logical_not(upper)))

                @pl.when(needed)
                def _():
                    attend(which, chip(-j) * 2 + core, False)

                return 0

            lax.fori_loop(0, 3, block, 0)
        return 0

    lax.fori_loop(1, far + 2, kv_step, 0)

    early = near // 2

    def gu_step(k):
        for st in gu:
            arrive(st, 0, k)
            arrive(st, 1, k + early)

    def merge(which):
        merged = jnp.zeros((rows, width), F32)
        for h in range(heads):
            norm = jnp.sum(l_s[which, h], axis=1, keepdims=True)
            merged = jnp.where(lane_head == h, acc[which, h] / norm, merged)
        return merged

    def far_copy(k):
        return pltpu.make_async_remote_copy(
            src_ref=(osend, ssend)[k], dst_ref=(ofar, sfar)[k], send_sem=pair_sem.at[2 + k],
            recv_sem=pair_sem.at[4 + k], device_id={"sp": pair}, device_id_type=MESH,
        )

    lane = lax.broadcasted_iota(jnp.int32, (rows, LANES), 1)

    @pl.when(jnp.logical_not(upper))
    def _():
        osend[...] = merge(1).astype(BF16)
        stats = jnp.zeros((rows, LANES), F32)
        for h in range(heads):
            stats = jnp.where(lane == h, m_s[1, h], stats)
            stats = jnp.where(lane == heads + h, jnp.sum(l_s[1, h], axis=1, keepdims=True), stats)
        ssend[...] = stats.T[0:2 * heads, :]

    for direction_step in (1,):
        gu_step(direction_step)

    @pl.when(jnp.logical_not(upper))
    def _():
        ready(3)
        for k in (0, 1):
            far_copy(k).start()
        att[...] = merge(0).astype(BF16)

    gu_step(2)

    @pl.when(upper)
    def _():
        for k in (0, 1):
            far_copy(k).wait_recv()
        stats = jnp.concatenate([sfar[...], jnp.zeros((LANES - 2 * heads, rows), F32)], axis=0).T
        other = ofar[...].astype(F32)
        merged = jnp.zeros((rows, width), F32)
        for h in range(heads):
            mine, theirs_max = m_s[0, h][:, 0:1], stats[:, h:h + 1]
            top = jnp.maximum(mine, theirs_max)
            mine_scale = jnp.exp(mine - top)
            theirs_sum = stats[:, heads + h:heads + h + 1] * jnp.exp(theirs_max - top)
            norm = jnp.sum(l_s[0, h], axis=1, keepdims=True) * mine_scale + theirs_sum
            merged = jnp.where(lane_head == h, (acc[0, h] * mine_scale + other * theirs_sum) / norm, merged)
        att[...] = merged.astype(BF16)

    tile = min(512, model)

    def project(k, _):
        at = pl.ds(pl.multiple_of(k * tile, tile), tile)
        y = jnp.dot(att[...], wout_ref[:, at], preferred_element_type=F32).astype(BF16)
        pbuf[:, :, at] = y.reshape(n_tp, own_rows, tile)
        return 0

    lax.fori_loop(0, model // tile, project, 0)

    def reduce_copy(d):
        return pltpu.make_async_remote_copy(
            src_ref=pbuf.at[peers[d]], dst_ref=rsbuf.at[t], send_sem=x_send.at[0], recv_sem=x_recv.at[0, d],
            device_id={"tp": peers[d]}, device_id_type=MESH,
        )

    def gather_copy(d):
        return pltpu.make_async_remote_copy(
            src_ref=nbuf.at[t], dst_ref=nbuf.at[t], send_sem=x_send.at[1], recv_sem=x_recv.at[1, d],
            device_id={"tp": peers[d]}, device_id_type=MESH,
        )

    def arrival(buf, sem):
        return pltpu.make_async_copy(buf, buf, sem)

    gu_step(3)
    for d in range(n_tp - 1):
        ready(4 + d)
        reduce_copy(d).start()
    for k in range(4, near - 1):
        gu_step(k)
    for d in range(n_tp - 1):
        arrival(rsbuf.at[sources[d]], x_recv.at[0, d]).wait()
    summed = resv[...].astype(F32) + pbuf[t].astype(F32)
    for d in range(n_tp - 1):
        summed = summed + rsbuf[sources[d]].astype(F32)
    mixed[...] = summed.astype(BF16)
    floats = mixed[...].astype(F32)
    mean = jnp.sum(floats * floats, axis=1, keepdims=True) * (1.0 / model)
    nbuf[t] = (floats * lax.rsqrt(mean + 1e-6) * gain_ref[...]).astype(BF16)
    for d in range(n_tp - 1):
        gather_copy(d).start()

    gu_step(near - 1)
    for st in dn:
        send_own(st, 1)
        send_own(st, 0)
    gu_step(near)

    def gu_sib(i, _):
        sib_arrive(gu, i)
        return 0

    lax.fori_loop(0, far + 2, gu_sib, 0)
    for d in range(n_tp - 1):
        arrival(nbuf.at[sources[d]], x_recv.at[1, d]).wait()

    tiles = ff // LANES
    chip_rows = 2 * drow

    def accumulate(offsets, first, final):
        chips = [chip(o) for o in offsets]
        left_side = jnp.concatenate(
            [nbuf[:, :, pl.ds(pl.multiple_of(at * chip_rows, chip_rows), chip_rows)] for at in chips], axis=2
        ).reshape(rows, len(chips) * chip_rows)

        def one(k, _):
            at = pl.ds(pl.multiple_of(k * LANES, LANES), LANES)
            sides = [
                jnp.concatenate(
                    [buf[pl.ds(2 * chosen, 2), :, at].reshape(chip_rows, LANES) for chosen in chips], axis=0
                )
                for buf in (gbuf, ubuf)
            ]
            both = jnp.dot(left_side, jnp.concatenate(sides, axis=1), preferred_element_type=F32)
            if not first:
                both = both + hacc[k]
            if final:
                gate, up = both[:, :LANES], both[:, LANES:]
                hid[:, at] = (gate / (1.0 + jnp.exp(-gate)) * up).astype(BF16)
            else:
                hacc[k] = both
            return 0

        lax.fori_loop(0, tiles, one, 0)

    def dn_step(k):
        for st in dn:
            for direction in (0, 1):
                arrive(st, direction, k)

    offsets = [0] + [o for j in range(1, far) for o in (-j, j)] + [far]
    group = -(-len(offsets) // 4)
    for k in range(4):
        accumulate(offsets[k * group:(k + 1) * group], k == 0, k == 3)
        dn_step(k + 1)

    def column_copy(d, at):
        return pltpu.make_async_remote_copy(
            src_ref=dsend.at[at, peers[d]], dst_ref=drecv.at[t, at], send_sem=x_send.at[2],
            recv_sem=x_recv.at[2, d], device_id={"tp": peers[d]}, device_id_type=MESH,
        )

    def down_step(j, _):
        @pl.when(jnp.logical_and(j + 2 > 4, j + 2 <= far))
        def _():
            dn_step(j + 2)

        sib_arrive(dn, j)
        back, ahead = chip(j), chip(-j)
        weights = jnp.concatenate(
            [dbuf[pl.ds(at * 2, 2)].reshape(2 * drow, ff) for at in (back, ahead)], axis=0
        )
        y = lax.dot_general(hid[...], weights, NT_DIMS, preferred_element_type=F32).astype(BF16)
        y = y.reshape(n_tp, own_rows, 4 * drow)
        dsend[back] = y[:, :, :2 * drow]
        for d in range(n_tp - 1):
            column_copy(d, back).start()

        @pl.when(jnp.logical_and(j >= 1, j <= near))
        def _():
            dsend[ahead] = y[:, :, 2 * drow:]
            for d in range(n_tp - 1):
                column_copy(d, ahead).start()

        return 0

    lax.fori_loop(0, far + 1, down_step, 0)

    for d in range(n_tp - 1):
        arrival(drecv.at[sources[d]], x_recv.at[2, d]).wait()
    square = jnp.zeros((own_rows, 2 * drow), F32)
    for at in range(nz):
        cols = slice(at * 2 * drow, (at + 1) * 2 * drow)
        down = dsend[at, t].astype(F32)
        for d in range(n_tp - 1):
            down = down + drecv[sources[d], at].astype(F32)
        value = mixed[:, cols].astype(F32) + 0.5 * down
        total[:, cols] = value
        square = square + value * value
    mean = jnp.sum(square, axis=1, keepdims=True) * (1.0 / model)
    out_ref[...] = (total[...] * lax.rsqrt(mean + 1e-6)).astype(BF16)

    for st in kv:
        for k in range(near):
            @pl.when(jnp.logical_and(z < nz - 1, z >= k))
            def _():
                link_copy(st, s, 0, k + 1).wait_send()

        for k in range(near + 1):
            @pl.when(z >= k)
            def _():
                sib_copy(st, s, k).wait_send()

    @pl.when(upper)
    def _():
        query_copy.wait_send()

    @pl.when(jnp.logical_not(upper))
    def _():
        for k in (0, 1):
            far_copy(k).wait_send()

    for st in gu + dn:
        buf, start, size = views[st]
        arrival(buf.at[pl.ds(0, 2 * nz - 1), pl.ds(start, size)], send_sem.at[st]).wait()
    arrival(pbuf.at[pl.ds(0, n_tp - 1)], x_send.at[0]).wait()
    arrival(nbuf.at[pl.ds(0, n_tp - 1)], x_send.at[1]).wait()
    arrival(drecv.at[pl.ds(0, n_tp - 1)], x_send.at[2]).wait()


def body(residual, queries, keys, values, log_gates, w_out, norm_gain, w_gate, w_up, w_down):
    n_sp, n_tp = lax.axis_size("sp"), lax.axis_size("tp")
    rows, width = queries.shape
    heads = log_gates.shape[1]
    model = residual.shape[1]
    drow, ff = w_gate.shape
    own_rows = rows // n_tp
    nz = n_sp // 2
    far = nz // 2

    gates = log_gates.T
    high = lax.reduce_precision(gates, 8, 7)
    middle = lax.reduce_precision(gates - high, 8, 7)
    low = gates - high - middle
    extra = jnp.concatenate([high, middle, low, jnp.zeros((16 - 3 * heads, rows), F32)], axis=0).astype(BF16)
    vmem = pl.BlockSpec(memory_space=pltpu.VMEM)
    hbm = pl.BlockSpec(memory_space=pl.ANY)
    return pl.pallas_call(
        functools.partial(layer_kernel, n_sp, n_tp, heads),
        out_shape=jax.ShapeDtypeStruct((own_rows, model), BF16),
        in_specs=[vmem, hbm, hbm, hbm, hbm, vmem, vmem, hbm, hbm, hbm],
        out_specs=vmem,
        scratch_shapes=[
            pltpu.VMEM((n_sp, rows + 16, width), BF16),
            pltpu.VMEM((n_sp, rows, width), BF16),
            pltpu.VMEM((n_sp, drow, ff), BF16),
            pltpu.VMEM((n_sp, drow, ff), BF16),
            pltpu.VMEM((n_sp, drow, ff), BF16),
            pltpu.VMEM((2, heads, rows, width), BF16),
            pltpu.VMEM((2, heads, rows, LANES), F32),
            pltpu.VMEM((2, heads, rows, LANES), F32),
            pltpu.VMEM((2, heads, rows, width), F32),
            pltpu.VMEM((rows, width), BF16),
            pltpu.VMEM((n_tp, own_rows, model), BF16),
            pltpu.VMEM((n_tp, own_rows, model), BF16),
            pltpu.VMEM((own_rows, model), BF16),
            pltpu.VMEM((own_rows, model), BF16),
            pltpu.VMEM((n_tp, own_rows, model), BF16),
            pltpu.VMEM((ff // LANES, rows, 2 * LANES), F32),
            pltpu.VMEM((rows, ff), BF16),
            pltpu.VMEM((nz, n_tp, own_rows, 2 * drow), BF16),
            pltpu.VMEM((n_tp, nz, own_rows, 2 * drow), BF16),
            pltpu.VMEM((own_rows, model), F32),
            pltpu.VMEM((rows, width), BF16),
            pltpu.VMEM((rows, width), BF16),
            pltpu.VMEM((rows, width), BF16),
            pltpu.VMEM((2 * heads, rows), F32),
            pltpu.VMEM((2 * heads, rows), F32),
            pltpu.SemaphoreType.DMA((6,)),
            pltpu.SemaphoreType.DMA((6, 2, far + 1)),
            pltpu.SemaphoreType.DMA((6, nz + far + 2)),
            pltpu.SemaphoreType.DMA((7,)),
            pltpu.SemaphoreType.DMA((3,)),
            pltpu.SemaphoreType.DMA((3, n_tp - 1)),
            pltpu.SemaphoreType.REGULAR((3 + n_tp,)),
            pltpu.SemaphoreType.DMA((2, far)),
            pltpu.SemaphoreType.DMA((2, far)),
            pltpu.SemaphoreType.DMA((6,)),
        ],
        compiler_params=pltpu.CompilerParams(
            collective_id=0, has_side_effects=True, vmem_limit_bytes=60 * 1024 * 1024
        ),
    )(queries, keys, extra, values, residual, w_out, norm_gain.reshape(1, -1), w_gate, w_up, w_down.T)


def solution(mesh):
    in_specs = (
        P(("grp", "sp"), None),
        P(("grp", "sp"), "tp"),
        P(("grp", "sp"), "tp"),
        P(("grp", "sp"), "tp"),
        P(("grp", "sp"), "tp"),
        P("tp", None),
        P(),
        P("sp", "tp"),
        P("sp", "tp"),
        P("tp", "sp"),
    )
    out_specs = P(("grp", "sp", "tp"), None)
    return jax.shard_map(body, mesh=mesh, in_specs=in_specs, out_specs=out_specs, check_vma=False)
```

```python
import functools

import jax
import jax.numpy as jnp
from jax import lax
from jax.experimental import pallas as pl
from jax.experimental.pallas import tpu as pltpu
from jax.sharding import PartitionSpec as P

MESH = pl.DeviceIdType.MESH
F32 = jnp.float32
BF16 = jnp.bfloat16
NT_DIMS = (((1,), (1,)), ((), ()))
LANES = 128


def layer_kernel(
    n_sp, n_tp, heads,
    q_ref, k_ref, x_ref, v_ref, res_ref, wout_ref, gain_ref, g_ref, u_ref, d_ref,
    out_ref,
    kbuf, vbuf, gbuf, ubuf, dbuf, q4, m_s, l_s, acc, att, pbuf, rsbuf, resv, mixed, nbuf, hacc, hid, dsend, drecv, total,
    qfar, ofar, osend, sfar, ssend,
    send_sem, recv_sem, sib_sem, loc_sem, x_send, x_recv, ack, kv_send, kv_sib, pair_sem,
):
    s = lax.axis_index("sp")
    t = lax.axis_index("tp")
    c = lax.rem(s, 2)
    z = s // 2
    nz = n_sp // 2
    far, near = nz // 2, nz - 1 - nz // 2
    rows, width = q_ref.shape
    head_width = width // heads
    own_rows = rows // n_tp
    drow, ff = g_ref.shape
    model = drow * n_sp

    def chip(offset):
        return lax.rem(z + offset + nz, nz)

    right = chip(1) * 2 + c
    left = chip(-1) * 2 + c
    sibling = s + 1 - 2 * c
    pair = chip(far) * 2 + c
    upper = z >= far
    peers = [lax.rem(t + d, n_tp) for d in range(1, n_tp)]
    sources = [lax.rem(t - d + n_tp, n_tp) for d in range(1, n_tp)]

    half = drow // 2
    views = (
        (kbuf, 0, kbuf.shape[1]), (vbuf, 0, vbuf.shape[1]), (gbuf, 0, drow), (ubuf, 0, drow),
        (dbuf, 0, half), (dbuf, half, half),
    )

    def piece(st, slot):
        buf, start, size = views[st]
        return buf.at[slot, pl.ds(start, size)]

    right_hops = nz // 4 + 1
    left_hops = nz - 1 - right_hops
    both_ways = (right_hops, left_hops)
    reaches = ((near, 0), (near, 0), (right_hops - 1, left_hops + 1), both_ways, both_ways, both_ways)
    ways = nz

    def reach(st):
        return reaches[st]

    def link_copy(st, slot, direction, step):
        return pltpu.make_async_remote_copy(
            src_ref=piece(st, slot), dst_ref=piece(st, slot),
            send_sem=kv_send.at[st, step - 1] if st < 2 else send_sem.at[st],
            recv_sem=recv_sem.at[st, direction, step - 1],
            device_id={"sp": right if direction == 0 else left}, device_id_type=MESH,
        )

    def sib_copy(st, slot, index):
        return pltpu.make_async_remote_copy(
            src_ref=piece(st, slot), dst_ref=piece(st, slot),
            send_sem=kv_sib.at[st, index] if st < 2 else send_sem.at[st],
            recv_sem=sib_sem.at[st, index], device_id={"sp": sibling}, device_id_type=MESH,
        )

    def usable(st, direction, step):
        fits = jnp.logical_and(step >= 1, step <= reach(st)[direction])
        return jnp.logical_and(fits, z - step >= 0) if st < 2 else fits

    def source(direction, step):
        return chip(-step if direction == 0 else step)

    def send_own(st, direction):
        link_copy(st, s, direction, 1).start()

    def arrive(st, direction, step):
        @pl.when(usable(st, direction, step))
        def _():
            slot = source(direction, step) * 2 + c
            link_copy(st, slot, direction, step).wait_recv()
            onward = step < reach(st)[direction]

            @pl.when(jnp.logical_and(onward, z < nz - 1) if st < 2 else onward)
            def _():
                link_copy(st, slot, direction, step + 1).start()

            sib_copy(st, slot, step + ways * direction).start()

    def sib_arrive(pair_of, step):
        for st in pair_of:
            for direction in (0, 1):
                @pl.when(usable(st, direction, step))
                def _():
                    slot = source(direction, step) * 2 + 1 - c
                    sib_copy(st, slot, step + ways * direction).wait_recv()

            @pl.when(step == 0)
            def _():
                sib_copy(st, sibling, 0).wait_recv()

    def local(src, dst, index):
        return pltpu.make_async_copy(src, dst, loc_sem.at[index])

    own_slice = pl.ds(pl.multiple_of(t * own_rows, own_rows), own_rows)
    loads = [
        local(k_ref, kbuf.at[s, pl.ds(0, rows)], 0), local(x_ref, kbuf.at[s, pl.ds(rows, 16)], 1),
        local(v_ref, vbuf.at[s], 2), local(g_ref, gbuf.at[s], 3), local(u_ref, ubuf.at[s], 4),
        local(d_ref, dbuf.at[s], 5), local(res_ref.at[own_slice], resv, 6),
    ]
    for load in loads:
        load.start()

    lower = [z == 0, z < nz - 1, c == 1, jnp.logical_not(upper)] + [peer < t for peer in peers]
    axis = ["sp", "sp", "sp", "sp"] + ["tp"] * (n_tp - 1)
    partner = [left, right, sibling, pair] + peers
    theirs = [1, 0, 2, 3] + [3 + n_tp - d for d in range(1, n_tp)]
    barrier = pltpu.get_barrier_semaphore()
    for k in range(3 + n_tp):
        @pl.when(lower[k])
        def _():
            pl.semaphore_signal(barrier, inc=1, device_id={axis[k]: partner[k]}, device_id_type=MESH)

    higher = sum(jnp.where(low, 0, 1) for low in lower)

    @pl.when(higher > 0)
    def _():
        pl.semaphore_wait(barrier, higher)

    for k in range(3 + n_tp):
        @pl.when(jnp.logical_not(lower[k]))
        def _():
            pl.semaphore_signal(
                ack.at[theirs[k]], inc=1, device_id={axis[k]: partner[k]}, device_id_type=MESH
            )

    def ready(k):
        @pl.when(lower[k])
        def _():
            pl.semaphore_wait(ack.at[k], 1)

    kv, gu, dn = (0, 1), (2, 3), (4, 5)
    edge = jnp.logical_or(z == 0, z == nz - 1)
    for load in loads[:3]:
        load.wait()
    ready(1)

    @pl.when(z < nz - 1)
    def _():
        for st in kv:
            send_own(st, 0)

    query_copy = pltpu.make_async_remote_copy(
        src_ref=q_ref, dst_ref=qfar, send_sem=pair_sem.at[0], recv_sem=pair_sem.at[1],
        device_id={"sp": pair}, device_id_type=MESH,
    )

    @pl.when(upper)
    def _():
        query_copy.start()

    for load in loads[3:]:
        load.wait()

    @pl.when(edge)
    def _():
        for st in gu:
            send_own(st, 0)

    ready(2)
    for st in kv:
        sib_copy(st, s, 0).start()
    ready(0)
    for st in gu:
        send_own(st, 1)
    for st in gu + dn:
        sib_copy(st, s, 0).start()

    lane_head = lax.broadcasted_iota(jnp.int32, (rows, width), 1) // head_width

    def prepare(which, ref):
        scaled = ref[...].astype(F32) * (head_width ** -0.5)
        for h in range(heads):
            q4[which, h] = jnp.where(lane_head == h, scaled, 0.0).astype(BF16)
            m_s[which, h] = jnp.full((rows, LANES), -1e30, F32)
            l_s[which, h] = jnp.zeros((rows, LANES), F32)
            acc[which, h] = jnp.zeros((rows, width), F32)

    prepare(0, q_ref)

    def wide(x, size):
        return jnp.concatenate([x] * (size // LANES), axis=1) if size >= LANES else x[:, :size]

    def attend(which, slot, diagonal):
        key = kbuf[slot, 0:rows, :]
        parts = kbuf[slot, rows:rows + 16, :].astype(F32)
        gates = parts[0:heads] + parts[heads:2 * heads] + parts[2 * heads:3 * heads]
        value = vbuf[slot]
        for h in range(heads):
            score = lax.dot_general(q4[which, h], key, NT_DIMS, preferred_element_type=F32) - gates[h:h + 1, :rows]
            if diagonal:
                at = lax.broadcasted_iota(jnp.int32, (rows, rows), 0)
                col = lax.broadcasted_iota(jnp.int32, (rows, rows), 1)
                score = jnp.where(col <= at, score, -1e30)
            before = m_s[which, h]
            top = jnp.maximum(before, jnp.max(score, axis=1, keepdims=True))
            weight = jnp.exp(score - wide(top, rows))
            rescale = jnp.exp(before - top)
            lanes = weight[:, 0:LANES]
            for k in range(1, rows // LANES):
                lanes = lanes + weight[:, k * LANES:(k + 1) * LANES]
            l_s[which, h] = l_s[which, h] * rescale + lanes
            product = jnp.dot(weight.astype(BF16), value, preferred_element_type=F32)
            acc[which, h] = acc[which, h] * wide(rescale, width) + product
            m_s[which, h] = top

    attend(0, s, True)

    ahead_from = near - 1

    def kv_step(i, _):
        for half, st in enumerate(kv):
            arrive(st, 0, i)
            if half == 1:
                @pl.when(jnp.logical_and(jnp.logical_not(edge), i == jnp.minimum(z, near - 1)))
                def _():
                    for own in gu:
                        send_own(own, 0)

                for own in gu:
                    arrive(own, 1, jnp.where(i <= near, i, 0))

                @pl.when(i <= far)
                def _():
                    sib_arrive(kv, i - 1)

                @pl.when(jnp.logical_and(i == ahead_from - 1, jnp.logical_not(upper)))
                def _():
                    query_copy.wait_recv()
                    prepare(1, qfar)

            turn = 2 * (i - ahead_from) + half

            def block(b, _):
                which = jnp.where(b == 0, 0, 1)
                j = jnp.where(b == 0, i - 1, turn)
                core = jnp.where(b == 0, c if half == 0 else 1 - c, b - 1)
                fits = jnp.logical_and(jnp.logical_and(j >= 0, j <= near), z - j >= 0)
                own = jnp.logical_or(j > 0, jnp.logical_and(half == 1, c == 1))
                needed = jnp.logical_and(fits, jnp.where(b == 0, own, jnp.logical_not(upper)))

                @pl.when(needed)
                def _():
                    attend(which, chip(-j) * 2 + core, False)

                return 0

            lax.fori_loop(0, 3, block, 0)
        return 0

    lax.fori_loop(1, far + 2, kv_step, 0)

    lag = jnp.minimum(near + 3, jnp.maximum(near, near + 5 - z))
    down_from = 2 * (left_hops + 2)

    def pump(h, _):
        for st in gu:
            arrive(st, 1, jnp.where(lax.rem(h, 2) == 0, h // 2, 0))

        @pl.when(h == 2 * left_hops)
        def _():
            for st in dn:
                send_own(st, 1)

        for st in dn:
            arrive(st, 1, h - down_from + 1)
        turn = jnp.where(lax.rem(h, 2) == 0, h // 2 - lag, 0)
        for st in gu:
            arrive(st, 0, turn)

        @pl.when(turn == right_hops - 1)
        def _():
            for st in dn:
                send_own(st, 0)

        for st in dn:
            arrive(st, 0, h - 2 * (lag + right_hops + 1) + 1)
        return 0

    def pumps(first, last):
        lax.fori_loop(first, last, pump, 0)

    def merge(which):
        merged = jnp.zeros((rows, width), F32)
        for h in range(heads):
            norm = jnp.sum(l_s[which, h], axis=1, keepdims=True)
            merged = jnp.where(lane_head == h, acc[which, h] / norm, merged)
        return merged

    def far_copy(k):
        return pltpu.make_async_remote_copy(
            src_ref=(osend, ssend)[k], dst_ref=(ofar, sfar)[k], send_sem=pair_sem.at[2 + k],
            recv_sem=pair_sem.at[4 + k], device_id={"sp": pair}, device_id_type=MESH,
        )

    lane = lax.broadcasted_iota(jnp.int32, (rows, LANES), 1)

    @pl.when(jnp.logical_not(upper))
    def _():
        osend[...] = merge(1).astype(BF16)
        stats = jnp.zeros((rows, LANES), F32)
        for h in range(heads):
            stats = jnp.where(lane == h, m_s[1, h], stats)
            stats = jnp.where(lane == heads + h, jnp.sum(l_s[1, h], axis=1, keepdims=True), stats)
        ssend[...] = stats.T[0:2 * heads, :]

    @pl.when(jnp.logical_not(upper))
    def _():
        att[...] = merge(0).astype(BF16)
        ready(3)
        for k in (0, 1):
            far_copy(k).start()

    start = 2 * (near + 1)
    pumps(start, start + 3)

    @pl.when(upper)
    def _():
        for k in (0, 1):
            far_copy(k).wait_recv()
        stats = jnp.concatenate([sfar[...], jnp.zeros((LANES - 2 * heads, rows), F32)], axis=0).T
        other = ofar[...].astype(F32)
        merged = jnp.zeros((rows, width), F32)
        for h in range(heads):
            mine, theirs_max = m_s[0, h][:, 0:1], stats[:, h:h + 1]
            top = jnp.maximum(mine, theirs_max)
            mine_scale = jnp.exp(mine - top)
            theirs_sum = stats[:, heads + h:heads + h + 1] * jnp.exp(theirs_max - top)
            norm = jnp.sum(l_s[0, h], axis=1, keepdims=True) * mine_scale + theirs_sum
            merged = jnp.where(lane_head == h, (acc[0, h] * mine_scale + other * theirs_sum) / norm, merged)
        att[...] = merged.astype(BF16)

    tile = min(512, model)

    def project(k, _):
        at = pl.ds(pl.multiple_of(k * tile, tile), tile)
        y = jnp.dot(att[...], wout_ref[:, at], preferred_element_type=F32).astype(BF16)
        pbuf[:, :, at] = y.reshape(n_tp, own_rows, tile)
        return 0

    lax.fori_loop(0, model // tile, project, 0)

    def reduce_copy(d):
        return pltpu.make_async_remote_copy(
            src_ref=pbuf.at[peers[d]], dst_ref=rsbuf.at[t], send_sem=x_send.at[0], recv_sem=x_recv.at[0, d],
            device_id={"tp": peers[d]}, device_id_type=MESH,
        )

    def gather_copy(d):
        return pltpu.make_async_remote_copy(
            src_ref=nbuf.at[t], dst_ref=nbuf.at[t], send_sem=x_send.at[1], recv_sem=x_recv.at[1, d],
            device_id={"tp": peers[d]}, device_id_type=MESH,
        )

    def arrival(buf, sem):
        return pltpu.make_async_copy(buf, buf, sem)

    pumps(start + 3, start + 4)
    for d in range(n_tp - 1):
        ready(4 + d)
        reduce_copy(d).start()
    pumps(start + 4, down_from + 1)
    for d in range(n_tp - 1):
        arrival(rsbuf.at[sources[d]], x_recv.at[0, d]).wait()
    summed = resv[...].astype(F32) + pbuf[t].astype(F32)
    for d in range(n_tp - 1):
        summed = summed + rsbuf[sources[d]].astype(F32)
    mixed[...] = summed.astype(BF16)
    floats = mixed[...].astype(F32)
    mean = jnp.sum(floats * floats, axis=1, keepdims=True) * (1.0 / model)
    nbuf[t] = (floats * lax.rsqrt(mean + 1e-6) * gain_ref[...]).astype(BF16)
    for d in range(n_tp - 1):
        gather_copy(d).start()

    fill = down_from + 5
    pumps(down_from + 1, fill)

    def sib_offset(streams, offset):
        for st in streams:
            if offset == 0:
                index = 0
            elif offset > 0:
                index = offset + ways
            else:
                index = -offset if -offset <= reach(st)[0] else nz + offset + ways
            sib_copy(st, chip(offset) * 2 + 1 - c, index).wait_recv()

    for d in range(n_tp - 1):
        arrival(nbuf.at[sources[d]], x_recv.at[1, d]).wait()

    tiles = ff // LANES
    chip_rows = 2 * drow

    def accumulate(offsets, first, final):
        for offset in offsets:
            sib_offset(gu, offset)
        chips = [chip(o) for o in offsets]
        left_side = jnp.concatenate(
            [nbuf[:, :, pl.ds(pl.multiple_of(at * chip_rows, chip_rows), chip_rows)] for at in chips], axis=2
        ).reshape(rows, len(chips) * chip_rows)

        def one(k, _):
            at = pl.ds(pl.multiple_of(k * LANES, LANES), LANES)
            sides = [
                jnp.concatenate(
                    [buf[pl.ds(2 * chosen, 2), :, at].reshape(chip_rows, LANES) for chosen in chips], axis=0
                )
                for buf in (gbuf, ubuf)
            ]
            both = jnp.dot(left_side, jnp.concatenate(sides, axis=1), preferred_element_type=F32)
            if not first:
                both = both + hacc[k]
            if final:
                gate, up = both[:, :LANES], both[:, LANES:]
                hid[:, at] = (gate / (1.0 + jnp.exp(-gate)) * up).astype(BF16)
            else:
                hacc[k] = both
            return 0

        lax.fori_loop(0, tiles, one, 0)

    spread = [0] + list(range(1, left_hops + 1)) + [-j for j in range(1, right_hops + 1)]
    group = -(-len(spread) // 4)
    for k in range(4):
        accumulate(spread[k * group:(k + 1) * group], k == 0, k == 3)
        pumps(fill + k, fill + k + 1)

    def column_copy(d, at):
        return pltpu.make_async_remote_copy(
            src_ref=dsend.at[at, peers[d]], dst_ref=drecv.at[t, at], send_sem=x_send.at[2],
            recv_sem=x_recv.at[2, d], device_id={"tp": peers[d]}, device_id_type=MESH,
        )

    def down(offsets):
        for offset in offsets:
            sib_offset(dn, offset)
        chips = [chip(offset) for offset in offsets]
        weights = jnp.concatenate([dbuf[pl.ds(at * 2, 2)].reshape(2 * drow, ff) for at in chips], axis=0)
        y = lax.dot_general(hid[...], weights, NT_DIMS, preferred_element_type=F32).astype(BF16)
        y = y.reshape(n_tp, own_rows, 4 * drow)
        for k, at in enumerate(chips):
            dsend[at] = y[:, :, 2 * drow * k:2 * drow * (k + 1)]
        for at in chips:
            for d in range(n_tp - 1):
                column_copy(d, at).start()

    backs, fronts = [-j for j in range(1, right_hops + 1)], list(range(1, left_hops + 1))
    sequence = [0] + fronts[:len(fronts) - right_hops]
    for ahead, back in zip(fronts[len(fronts) - right_hops:], backs):
        sequence += [ahead, back]
    last = 2 * (near + 3 + right_hops + 1) + right_hops
    at_pump = fill + 4
    while sequence:
        down(sequence[:2])
        sequence = sequence[2:]
        if len(sequence) <= 2 * (last - at_pump) and at_pump < last:
            pumps(at_pump, at_pump + 1)
            at_pump += 1

    for d in range(n_tp - 1):
        arrival(drecv.at[sources[d]], x_recv.at[2, d]).wait()
    square = jnp.zeros((own_rows, 2 * drow), F32)
    for at in range(nz):
        cols = slice(at * 2 * drow, (at + 1) * 2 * drow)
        down = dsend[at, t].astype(F32)
        for d in range(n_tp - 1):
            down = down + drecv[sources[d], at].astype(F32)
        value = mixed[:, cols].astype(F32) + 0.5 * down
        total[:, cols] = value
        square = square + value * value
    mean = jnp.sum(square, axis=1, keepdims=True) * (1.0 / model)
    out_ref[...] = (total[...] * lax.rsqrt(mean + 1e-6)).astype(BF16)

    for st in kv:
        for k in range(near):
            @pl.when(jnp.logical_and(z < nz - 1, z >= k))
            def _():
                link_copy(st, s, 0, k + 1).wait_send()

        for k in range(near + 1):
            @pl.when(z >= k)
            def _():
                sib_copy(st, s, k).wait_send()

    @pl.when(upper)
    def _():
        query_copy.wait_send()

    @pl.when(jnp.logical_not(upper))
    def _():
        for k in (0, 1):
            far_copy(k).wait_send()

    for st in gu + dn:
        buf, start, size = views[st]
        arrival(buf.at[pl.ds(0, 2 * nz - 1), pl.ds(start, size)], send_sem.at[st]).wait()
    arrival(pbuf.at[pl.ds(0, n_tp - 1)], x_send.at[0]).wait()
    arrival(nbuf.at[pl.ds(0, n_tp - 1)], x_send.at[1]).wait()
    arrival(drecv.at[pl.ds(0, n_tp - 1)], x_send.at[2]).wait()


def body(residual, queries, keys, values, log_gates, w_out, norm_gain, w_gate, w_up, w_down):
    n_sp, n_tp = lax.axis_size("sp"), lax.axis_size("tp")
    rows, width = queries.shape
    heads = log_gates.shape[1]
    model = residual.shape[1]
    drow, ff = w_gate.shape
    own_rows = rows // n_tp
    nz = n_sp // 2
    far = nz // 2

    gates = log_gates.T
    high = lax.reduce_precision(gates, 8, 7)
    middle = lax.reduce_precision(gates - high, 8, 7)
    low = gates - high - middle
    extra = jnp.concatenate([high, middle, low, jnp.zeros((16 - 3 * heads, rows), F32)], axis=0).astype(BF16)
    vmem = pl.BlockSpec(memory_space=pltpu.VMEM)
    hbm = pl.BlockSpec(memory_space=pl.ANY)
    return pl.pallas_call(
        functools.partial(layer_kernel, n_sp, n_tp, heads),
        out_shape=jax.ShapeDtypeStruct((own_rows, model), BF16),
        in_specs=[vmem, hbm, hbm, hbm, hbm, vmem, vmem, hbm, hbm, hbm],
        out_specs=vmem,
        scratch_shapes=[
            pltpu.VMEM((n_sp, rows + 16, width), BF16),
            pltpu.VMEM((n_sp, rows, width), BF16),
            pltpu.VMEM((n_sp, drow, ff), BF16),
            pltpu.VMEM((n_sp, drow, ff), BF16),
            pltpu.VMEM((n_sp, drow, ff), BF16),
            pltpu.VMEM((2, heads, rows, width), BF16),
            pltpu.VMEM((2, heads, rows, LANES), F32),
            pltpu.VMEM((2, heads, rows, LANES), F32),
            pltpu.VMEM((2, heads, rows, width), F32),
            pltpu.VMEM((rows, width), BF16),
            pltpu.VMEM((n_tp, own_rows, model), BF16),
            pltpu.VMEM((n_tp, own_rows, model), BF16),
            pltpu.VMEM((own_rows, model), BF16),
            pltpu.VMEM((own_rows, model), BF16),
            pltpu.VMEM((n_tp, own_rows, model), BF16),
            pltpu.VMEM((ff // LANES, rows, 2 * LANES), F32),
            pltpu.VMEM((rows, ff), BF16),
            pltpu.VMEM((nz, n_tp, own_rows, 2 * drow), BF16),
            pltpu.VMEM((n_tp, nz, own_rows, 2 * drow), BF16),
            pltpu.VMEM((own_rows, model), F32),
            pltpu.VMEM((rows, width), BF16),
            pltpu.VMEM((rows, width), BF16),
            pltpu.VMEM((rows, width), BF16),
            pltpu.VMEM((2 * heads, rows), F32),
            pltpu.VMEM((2 * heads, rows), F32),
            pltpu.SemaphoreType.DMA((6,)),
            pltpu.SemaphoreType.DMA((6, 2, nz)),
            pltpu.SemaphoreType.DMA((6, 2 * nz)),
            pltpu.SemaphoreType.DMA((7,)),
            pltpu.SemaphoreType.DMA((3,)),
            pltpu.SemaphoreType.DMA((3, n_tp - 1)),
            pltpu.SemaphoreType.REGULAR((3 + n_tp,)),
            pltpu.SemaphoreType.DMA((2, far)),
            pltpu.SemaphoreType.DMA((2, far)),
            pltpu.SemaphoreType.DMA((6,)),
        ],
        compiler_params=pltpu.CompilerParams(
            collective_id=0, has_side_effects=True, vmem_limit_bytes=60 * 1024 * 1024
        ),
    )(queries, keys, extra, values, residual, w_out, norm_gain.reshape(1, -1), w_gate, w_up, w_down.T)


def solution(mesh):
    in_specs = (
        P(("grp", "sp"), None),
        P(("grp", "sp"), "tp"),
        P(("grp", "sp"), "tp"),
        P(("grp", "sp"), "tp"),
        P(("grp", "sp"), "tp"),
        P("tp", None),
        P(),
        P("sp", "tp"),
        P("sp", "tp"),
        P("tp", "sp"),
    )
    out_specs = P(("grp", "sp", "tp"), None)
    return jax.shard_map(body, mesh=mesh, in_specs=in_specs, out_specs=out_specs, check_vma=False)
```

```python
import functools

import jax
import jax.numpy as jnp
from jax import lax
from jax.experimental import pallas as pl
from jax.experimental.pallas import tpu as pltpu
from jax.sharding import PartitionSpec as P

MESH = pl.DeviceIdType.MESH
F32 = jnp.float32
BF16 = jnp.bfloat16
NT_DIMS = (((1,), (1,)), ((), ()))
LANES = 128


def layer_kernel(
    n_sp, n_tp, heads,
    q_ref, k_ref, x_ref, v_ref, res_ref, wout_ref, gain_ref, g_ref, u_ref, d_ref,
    out_ref,
    kbuf, vbuf, gbuf, ubuf, dbuf, q4, m_s, l_s, acc, att, pbuf, rsbuf, resv, mixed, nbuf, hacc, hid, dsend, drecv, total,
    qmid, qfar, omid, ofar, osend, smid, sfar, ssend,
    send_sem, recv_sem, sib_sem, loc_sem, x_send, x_recv, ack, kv_send, kv_sib, pair_sem,
):
    s = lax.axis_index("sp")
    t = lax.axis_index("tp")
    c = lax.rem(s, 2)
    z = s // 2
    nz = n_sp // 2
    far, near = nz // 2, nz - 1 - nz // 2
    rows, width = q_ref.shape
    head_width = width // heads
    own_rows = rows // n_tp
    drow, ff = g_ref.shape
    model = drow * n_sp

    def chip(offset):
        return lax.rem(z + offset + nz, nz)

    right = chip(1) * 2 + c
    left = chip(-1) * 2 + c
    sibling = s + 1 - 2 * c
    quarter = nz // 4
    behind, beyond = chip(-quarter) * 2 + c, chip(quarter) * 2 + c
    upper = z >= far
    passes_query = jnp.logical_and(z >= quarter, z < nz - quarter)
    passes_output = jnp.logical_not(passes_query)
    peers = [lax.rem(t + d, n_tp) for d in range(1, n_tp)]
    sources = [lax.rem(t - d + n_tp, n_tp) for d in range(1, n_tp)]

    half = drow // 2
    views = (
        (kbuf, 0, kbuf.shape[1]), (vbuf, 0, vbuf.shape[1]), (gbuf, 0, drow), (ubuf, 0, drow),
        (dbuf, 0, half), (dbuf, half, half),
    )

    def piece(st, slot):
        buf, start, size = views[st]
        return buf.at[slot, pl.ds(start, size)]

    reaches = ((near, 0), (near, 0), (near - 1, far + 1), (near, far), (near, far), (near, far))
    ways = nz

    def reach(st):
        return reaches[st]

    def link_copy(st, slot, direction, step):
        return pltpu.make_async_remote_copy(
            src_ref=piece(st, slot), dst_ref=piece(st, slot),
            send_sem=kv_send.at[st, step - 1] if st < 2 else send_sem.at[st],
            recv_sem=recv_sem.at[st, direction, step - 1],
            device_id={"sp": right if direction == 0 else left}, device_id_type=MESH,
        )

    def sib_copy(st, slot, index):
        return pltpu.make_async_remote_copy(
            src_ref=piece(st, slot), dst_ref=piece(st, slot),
            send_sem=kv_sib.at[st, index] if st < 2 else send_sem.at[st],
            recv_sem=sib_sem.at[st, index], device_id={"sp": sibling}, device_id_type=MESH,
        )

    def usable(st, direction, step):
        fits = jnp.logical_and(step >= 1, step <= reach(st)[direction])
        return jnp.logical_and(fits, z - step >= 0) if st < 2 else fits

    def source(direction, step):
        return chip(-step if direction == 0 else step)

    def send_own(st, direction):
        link_copy(st, s, direction, 1).start()

    def arrive(st, direction, step):
        @pl.when(usable(st, direction, step))
        def _():
            slot = source(direction, step) * 2 + c
            link_copy(st, slot, direction, step).wait_recv()
            onward = step < reach(st)[direction]

            @pl.when(jnp.logical_and(onward, z < nz - 1) if st < 2 else onward)
            def _():
                link_copy(st, slot, direction, step + 1).start()

            sib_copy(st, slot, step + ways * direction).start()

    def sib_arrive(pair_of, step):
        for st in pair_of:
            for direction in (0, 1):
                @pl.when(usable(st, direction, step))
                def _():
                    slot = source(direction, step) * 2 + 1 - c
                    sib_copy(st, slot, step + ways * direction).wait_recv()

            @pl.when(step == 0)
            def _():
                sib_copy(st, sibling, 0).wait_recv()

    def local(src, dst, index):
        return pltpu.make_async_copy(src, dst, loc_sem.at[index])

    own_slice = pl.ds(pl.multiple_of(t * own_rows, own_rows), own_rows)
    loads = [
        local(k_ref, kbuf.at[s, pl.ds(0, rows)], 0), local(x_ref, kbuf.at[s, pl.ds(rows, 16)], 1),
        local(v_ref, vbuf.at[s], 2), local(g_ref, gbuf.at[s], 3), local(u_ref, ubuf.at[s], 4),
        local(d_ref, dbuf.at[s], 5), local(res_ref.at[own_slice], resv, 6),
    ]
    for load in loads:
        load.start()

    lower = [z == 0, z < nz - 1, c == 1, z < quarter, z < nz - quarter]
    lower += [peer < t for peer in peers]
    axis = ["sp"] * 5 + ["tp"] * (n_tp - 1)
    partner = [left, right, sibling, behind, beyond] + peers
    theirs = [1, 0, 2, None, 3] + [4 + n_tp - d for d in range(1, n_tp)]
    barrier = pltpu.get_barrier_semaphore()
    for k in range(4 + n_tp):
        @pl.when(lower[k])
        def _():
            pl.semaphore_signal(barrier, inc=1, device_id={axis[k]: partner[k]}, device_id_type=MESH)

    higher = sum(jnp.where(low, 0, 1) for low in lower)

    @pl.when(higher > 0)
    def _():
        pl.semaphore_wait(barrier, higher)

    for k in range(4 + n_tp):
        if theirs[k] is None:
            continue

        @pl.when(jnp.logical_not(lower[k]))
        def _():
            pl.semaphore_signal(
                ack.at[theirs[k]], inc=1, device_id={axis[k]: partner[k]}, device_id_type=MESH
            )

    def ready(k):
        @pl.when(lower[k])
        def _():
            pl.semaphore_wait(ack.at[k], 1)

    kv, gu, dn = (0, 1), (2, 3), (4, 5)
    edge = jnp.logical_or(z == 0, z == nz - 1)
    for load in loads[:3]:
        load.wait()
    ready(1)

    @pl.when(z < nz - 1)
    def _():
        for st in kv:
            send_own(st, 0)

    def back_copy(src, dst, send, receive):
        return pltpu.make_async_remote_copy(
            src_ref=src, dst_ref=dst, send_sem=pair_sem.at[send], recv_sem=pair_sem.at[receive],
            device_id={"sp": behind}, device_id_type=MESH,
        )

    query_copy = back_copy(q_ref, qmid, 0, 2)
    query_relay = back_copy(qmid, qfar, 1, 3)
    outputs = [back_copy(osend, omid, 4, 8), back_copy(ssend, smid, 5, 9)]
    output_relays = [back_copy(omid, ofar, 6, 10), back_copy(smid, sfar, 7, 11)]

    @pl.when(upper)
    def _():
        query_copy.start()

    for load in loads[3:]:
        load.wait()

    @pl.when(edge)
    def _():
        for st in gu:
            send_own(st, 0)

    ready(2)
    for st in kv:
        sib_copy(st, s, 0).start()
    ready(0)
    for st in gu:
        send_own(st, 1)
    for st in gu + dn:
        sib_copy(st, s, 0).start()

    lane_head = lax.broadcasted_iota(jnp.int32, (rows, width), 1) // head_width

    def prepare(which, ref):
        scaled = ref[...].astype(F32) * (head_width ** -0.5)
        for h in range(heads):
            q4[which, h] = jnp.where(lane_head == h, scaled, 0.0).astype(BF16)
            m_s[which, h] = jnp.full((rows, LANES), -1e30, F32)
            l_s[which, h] = jnp.zeros((rows, LANES), F32)
            acc[which, h] = jnp.zeros((rows, width), F32)

    prepare(0, q_ref)

    def wide(x, size):
        return jnp.concatenate([x] * (size // LANES), axis=1) if size >= LANES else x[:, :size]

    def attend(which, slot, diagonal):
        key = kbuf[slot, 0:rows, :]
        parts = kbuf[slot, rows:rows + 16, :].astype(F32)
        gates = parts[0:heads] + parts[heads:2 * heads] + parts[2 * heads:3 * heads]
        value = vbuf[slot]
        for h in range(heads):
            score = lax.dot_general(q4[which, h], key, NT_DIMS, preferred_element_type=F32) - gates[h:h + 1, :rows]
            if diagonal:
                at = lax.broadcasted_iota(jnp.int32, (rows, rows), 0)
                col = lax.broadcasted_iota(jnp.int32, (rows, rows), 1)
                score = jnp.where(col <= at, score, -1e30)
            before = m_s[which, h]
            top = jnp.maximum(before, jnp.max(score, axis=1, keepdims=True))
            weight = jnp.exp(score - wide(top, rows))
            rescale = jnp.exp(before - top)
            lanes = weight[:, 0:LANES]
            for k in range(1, rows // LANES):
                lanes = lanes + weight[:, k * LANES:(k + 1) * LANES]
            l_s[which, h] = l_s[which, h] * rescale + lanes
            product = jnp.dot(weight.astype(BF16), value, preferred_element_type=F32)
            acc[which, h] = acc[which, h] * wide(rescale, width) + product
            m_s[which, h] = top

    attend(0, s, True)

    ahead_from = near - 1

    def kv_step(i, _):
        for half, st in enumerate(kv):
            arrive(st, 0, i)
            if half == 1:
                @pl.when(jnp.logical_and(jnp.logical_not(edge), i == jnp.minimum(z, near - 1)))
                def _():
                    for own in gu:
                        send_own(own, 0)

                @pl.when(lax.rem(i, 2) == 0)
                def _():
                    for own in gu:
                        arrive(own, 1, jnp.where(i <= near, i // 2, 0))

                @pl.when(i <= far)
                def _():
                    sib_arrive(kv, i - 1)

                @pl.when(jnp.logical_and(i == 2, passes_query))
                def _():
                    query_copy.wait_recv()
                    query_relay.start()

                @pl.when(jnp.logical_and(i == ahead_from - 1, jnp.logical_not(upper)))
                def _():
                    query_relay.wait_recv()
                    prepare(1, qfar)

            turn = 2 * (i - ahead_from) + half

            def block(b, _):
                which = jnp.where(b == 0, 0, 1)
                j = jnp.where(b == 0, i - 1, turn)
                core = jnp.where(b == 0, c if half == 0 else 1 - c, b - 1)
                fits = jnp.logical_and(jnp.logical_and(j >= 0, j <= near), z - j >= 0)
                own = jnp.logical_or(j > 0, jnp.logical_and(half == 1, c == 1))
                needed = jnp.logical_and(fits, jnp.where(b == 0, own, jnp.logical_not(upper)))

                @pl.when(needed)
                def _():
                    attend(which, chip(-j) * 2 + core, False)

                return 0

            lax.fori_loop(0, 3, block, 0)
        return 0

    lax.fori_loop(1, far + 2, kv_step, 0)

    early = near // 2

    def gu_step(k):
        for st in gu:
            arrive(st, 0, k)
            arrive(st, 1, k + early)

    def merge(which):
        merged = jnp.zeros((rows, width), F32)
        for h in range(heads):
            norm = jnp.sum(l_s[which, h], axis=1, keepdims=True)
            merged = jnp.where(lane_head == h, acc[which, h] / norm, merged)
        return merged

    lane = lax.broadcasted_iota(jnp.int32, (rows, LANES), 1)

    @pl.when(jnp.logical_not(upper))
    def _():
        osend[...] = merge(1).astype(BF16)
        stats = jnp.zeros((rows, LANES), F32)
        for h in range(heads):
            stats = jnp.where(lane == h, m_s[1, h], stats)
            stats = jnp.where(lane == heads + h, jnp.sum(l_s[1, h], axis=1, keepdims=True), stats)
        ssend[...] = stats.T[0:2 * heads, :]

    @pl.when(jnp.logical_not(upper))
    def _():
        att[...] = merge(0).astype(BF16)
        ready(3)
        for copy in outputs:
            copy.start()

    gu_step(1)

    @pl.when(passes_output)
    def _():
        for copy in outputs:
            copy.wait_recv()
        for copy in output_relays:
            copy.start()

    gu_step(2)

    @pl.when(upper)
    def _():
        for copy in output_relays:
            copy.wait_recv()
        stats = jnp.concatenate([sfar[...], jnp.zeros((LANES - 2 * heads, rows), F32)], axis=0).T
        other = ofar[...].astype(F32)
        merged = jnp.zeros((rows, width), F32)
        for h in range(heads):
            mine, theirs_max = m_s[0, h][:, 0:1], stats[:, h:h + 1]
            top = jnp.maximum(mine, theirs_max)
            mine_scale = jnp.exp(mine - top)
            theirs_sum = stats[:, heads + h:heads + h + 1] * jnp.exp(theirs_max - top)
            norm = jnp.sum(l_s[0, h], axis=1, keepdims=True) * mine_scale + theirs_sum
            merged = jnp.where(lane_head == h, (acc[0, h] * mine_scale + other * theirs_sum) / norm, merged)
        att[...] = merged.astype(BF16)

    tile = min(512, model)

    def project(k, _):
        at = pl.ds(pl.multiple_of(k * tile, tile), tile)
        y = jnp.dot(att[...], wout_ref[:, at], preferred_element_type=F32).astype(BF16)
        pbuf[:, :, at] = y.reshape(n_tp, own_rows, tile)
        return 0

    lax.fori_loop(0, model // tile, project, 0)

    def reduce_copy(d):
        return pltpu.make_async_remote_copy(
            src_ref=pbuf.at[peers[d]], dst_ref=rsbuf.at[t], send_sem=x_send.at[0], recv_sem=x_recv.at[0, d],
            device_id={"tp": peers[d]}, device_id_type=MESH,
        )

    def gather_copy(d):
        return pltpu.make_async_remote_copy(
            src_ref=nbuf.at[t], dst_ref=nbuf.at[t], send_sem=x_send.at[1], recv_sem=x_recv.at[1, d],
            device_id={"tp": peers[d]}, device_id_type=MESH,
        )

    def arrival(buf, sem):
        return pltpu.make_async_copy(buf, buf, sem)

    gu_step(3)
    for d in range(n_tp - 1):
        ready(5 + d)
        reduce_copy(d).start()
    for k in range(4, near - 1):
        gu_step(k)
    for d in range(n_tp - 1):
        arrival(rsbuf.at[sources[d]], x_recv.at[0, d]).wait()
    summed = resv[...].astype(F32) + pbuf[t].astype(F32)
    for d in range(n_tp - 1):
        summed = summed + rsbuf[sources[d]].astype(F32)
    mixed[...] = summed.astype(BF16)
    floats = mixed[...].astype(F32)
    mean = jnp.sum(floats * floats, axis=1, keepdims=True) * (1.0 / model)
    nbuf[t] = (floats * lax.rsqrt(mean + 1e-6) * gain_ref[...]).astype(BF16)
    for d in range(n_tp - 1):
        gather_copy(d).start()

    gu_step(near - 1)
    for st in dn:
        send_own(st, 1)
        send_own(st, 0)
    gu_step(near)

    def gu_sib(i, _):
        sib_arrive(gu, i)
        return 0

    lax.fori_loop(0, far + 2, gu_sib, 0)
    for d in range(n_tp - 1):
        arrival(nbuf.at[sources[d]], x_recv.at[1, d]).wait()

    tiles = ff // LANES
    chip_rows = 2 * drow

    def accumulate(offsets, first, final):
        chips = [chip(o) for o in offsets]
        left_side = jnp.concatenate(
            [nbuf[:, :, pl.ds(pl.multiple_of(at * chip_rows, chip_rows), chip_rows)] for at in chips], axis=2
        ).reshape(rows, len(chips) * chip_rows)

        def one(k, _):
            at = pl.ds(pl.multiple_of(k * LANES, LANES), LANES)
            sides = [
                jnp.concatenate(
                    [buf[pl.ds(2 * chosen, 2), :, at].reshape(chip_rows, LANES) for chosen in chips], axis=0
                )
                for buf in (gbuf, ubuf)
            ]
            both = jnp.dot(left_side, jnp.concatenate(sides, axis=1), preferred_element_type=F32)
            if not first:
                both = both + hacc[k]
            if final:
                gate, up = both[:, :LANES], both[:, LANES:]
                hid[:, at] = (gate / (1.0 + jnp.exp(-gate)) * up).astype(BF16)
            else:
                hacc[k] = both
            return 0

        lax.fori_loop(0, tiles, one, 0)

    def dn_step(k):
        for st in dn:
            for direction in (0, 1):
                arrive(st, direction, k)

    offsets = [0] + [o for j in range(1, far) for o in (-j, j)] + [far]
    group = -(-len(offsets) // 4)
    for k in range(4):
        accumulate(offsets[k * group:(k + 1) * group], k == 0, k == 3)
        dn_step(k + 1)

    def column_copy(d, at):
        return pltpu.make_async_remote_copy(
            src_ref=dsend.at[at, peers[d]], dst_ref=drecv.at[t, at], send_sem=x_send.at[2],
            recv_sem=x_recv.at[2, d], device_id={"tp": peers[d]}, device_id_type=MESH,
        )

    def down_step(j, _):
        @pl.when(jnp.logical_and(j + 2 > 4, j + 2 <= far))
        def _():
            dn_step(j + 2)

        sib_arrive(dn, j)
        back, ahead = chip(j), chip(-j)
        weights = jnp.concatenate(
            [dbuf[pl.ds(at * 2, 2)].reshape(2 * drow, ff) for at in (back, ahead)], axis=0
        )
        y = lax.dot_general(hid[...], weights, NT_DIMS, preferred_element_type=F32).astype(BF16)
        y = y.reshape(n_tp, own_rows, 4 * drow)
        dsend[back] = y[:, :, :2 * drow]
        for d in range(n_tp - 1):
            column_copy(d, back).start()

        @pl.when(jnp.logical_and(j >= 1, j <= near))
        def _():
            dsend[ahead] = y[:, :, 2 * drow:]
            for d in range(n_tp - 1):
                column_copy(d, ahead).start()

        return 0

    lax.fori_loop(0, far + 1, down_step, 0)

    for d in range(n_tp - 1):
        arrival(drecv.at[sources[d]], x_recv.at[2, d]).wait()
    square = jnp.zeros((own_rows, 2 * drow), F32)
    for at in range(nz):
        cols = slice(at * 2 * drow, (at + 1) * 2 * drow)
        down = dsend[at, t].astype(F32)
        for d in range(n_tp - 1):
            down = down + drecv[sources[d], at].astype(F32)
        value = mixed[:, cols].astype(F32) + 0.5 * down
        total[:, cols] = value
        square = square + value * value
    mean = jnp.sum(square, axis=1, keepdims=True) * (1.0 / model)
    out_ref[...] = (total[...] * lax.rsqrt(mean + 1e-6)).astype(BF16)

    for st in kv:
        for k in range(near):
            @pl.when(jnp.logical_and(z < nz - 1, z >= k))
            def _():
                link_copy(st, s, 0, k + 1).wait_send()

        for k in range(near + 1):
            @pl.when(z >= k)
            def _():
                sib_copy(st, s, k).wait_send()

    @pl.when(upper)
    def _():
        query_copy.wait_send()

    @pl.when(passes_query)
    def _():
        query_relay.wait_send()

    @pl.when(jnp.logical_not(upper))
    def _():
        for copy in outputs:
            copy.wait_send()

    @pl.when(passes_output)
    def _():
        for copy in output_relays:
            copy.wait_send()

    for st in gu + dn:
        buf, start, size = views[st]
        arrival(buf.at[pl.ds(0, 2 * nz - 1), pl.ds(start, size)], send_sem.at[st]).wait()
    arrival(pbuf.at[pl.ds(0, n_tp - 1)], x_send.at[0]).wait()
    arrival(nbuf.at[pl.ds(0, n_tp - 1)], x_send.at[1]).wait()
    arrival(drecv.at[pl.ds(0, n_tp - 1)], x_send.at[2]).wait()


def body(residual, queries, keys, values, log_gates, w_out, norm_gain, w_gate, w_up, w_down):
    n_sp, n_tp = lax.axis_size("sp"), lax.axis_size("tp")
    rows, width = queries.shape
    heads = log_gates.shape[1]
    model = residual.shape[1]
    drow, ff = w_gate.shape
    own_rows = rows // n_tp
    nz = n_sp // 2
    far = nz // 2

    gates = log_gates.T
    high = lax.reduce_precision(gates, 8, 7)
    middle = lax.reduce_precision(gates - high, 8, 7)
    low = gates - high - middle
    extra = jnp.concatenate([high, middle, low, jnp.zeros((16 - 3 * heads, rows), F32)], axis=0).astype(BF16)
    vmem = pl.BlockSpec(memory_space=pltpu.VMEM)
    hbm = pl.BlockSpec(memory_space=pl.ANY)
    return pl.pallas_call(
        functools.partial(layer_kernel, n_sp, n_tp, heads),
        out_shape=jax.ShapeDtypeStruct((own_rows, model), BF16),
        in_specs=[vmem, hbm, hbm, hbm, hbm, vmem, vmem, hbm, hbm, hbm],
        out_specs=vmem,
        scratch_shapes=[
            pltpu.VMEM((n_sp, rows + 16, width), BF16),
            pltpu.VMEM((n_sp, rows, width), BF16),
            pltpu.VMEM((n_sp, drow, ff), BF16),
            pltpu.VMEM((n_sp, drow, ff), BF16),
            pltpu.VMEM((n_sp, drow, ff), BF16),
            pltpu.VMEM((2, heads, rows, width), BF16),
            pltpu.VMEM((2, heads, rows, LANES), F32),
            pltpu.VMEM((2, heads, rows, LANES), F32),
            pltpu.VMEM((2, heads, rows, width), F32),
            pltpu.VMEM((rows, width), BF16),
            pltpu.VMEM((n_tp, own_rows, model), BF16),
            pltpu.VMEM((n_tp, own_rows, model), BF16),
            pltpu.VMEM((own_rows, model), BF16),
            pltpu.VMEM((own_rows, model), BF16),
            pltpu.VMEM((n_tp, own_rows, model), BF16),
            pltpu.VMEM((ff // LANES, rows, 2 * LANES), F32),
            pltpu.VMEM((rows, ff), BF16),
            pltpu.VMEM((nz, n_tp, own_rows, 2 * drow), BF16),
            pltpu.VMEM((n_tp, nz, own_rows, 2 * drow), BF16),
            pltpu.VMEM((own_rows, model), F32),
            *[pltpu.VMEM((rows, width), BF16) for _ in range(5)],
            *[pltpu.VMEM((2 * heads, rows), F32) for _ in range(3)],
            pltpu.SemaphoreType.DMA((6,)),
            pltpu.SemaphoreType.DMA((6, 2, far + 1)),
            pltpu.SemaphoreType.DMA((6, nz + far + 2)),
            pltpu.SemaphoreType.DMA((7,)),
            pltpu.SemaphoreType.DMA((3,)),
            pltpu.SemaphoreType.DMA((3, n_tp - 1)),
            pltpu.SemaphoreType.REGULAR((4 + n_tp,)),
            pltpu.SemaphoreType.DMA((2, far)),
            pltpu.SemaphoreType.DMA((2, far)),
            pltpu.SemaphoreType.DMA((12,)),
        ],
        compiler_params=pltpu.CompilerParams(
            collective_id=0, has_side_effects=True, vmem_limit_bytes=60 * 1024 * 1024
        ),
    )(queries, keys, extra, values, residual, w_out, norm_gain.reshape(1, -1), w_gate, w_up, w_down.T)


def solution(mesh):
    in_specs = (
        P(("grp", "sp"), None),
        P(("grp", "sp"), "tp"),
        P(("grp", "sp"), "tp"),
        P(("grp", "sp"), "tp"),
        P(("grp", "sp"), "tp"),
        P("tp", None),
        P(),
        P("sp", "tp"),
        P("sp", "tp"),
        P("tp", "sp"),
    )
    out_specs = P(("grp", "sp", "tp"), None)
    return jax.shard_map(body, mesh=mesh, in_specs=in_specs, out_specs=out_specs, check_vma=False)
```

```python
import functools

import jax
import jax.numpy as jnp
from jax import lax
from jax.experimental import pallas as pl
from jax.experimental.pallas import tpu as pltpu
from jax.sharding import PartitionSpec as P

MESH = pl.DeviceIdType.MESH
F32 = jnp.float32
BF16 = jnp.bfloat16
NT_DIMS = (((1,), (1,)), ((), ()))
LANES = 128


def layer_kernel(
    n_sp, n_tp, heads,
    q_ref, k_ref, x_ref, v_ref, res_ref, wout_ref, gain_ref, g_ref, u_ref, d_ref,
    out_ref,
    kbuf, vbuf, gbuf, ubuf, dbuf, q4, m_s, l_s, acc, att, pbuf, rsbuf, resv, mixed, nbuf, hacc, hid, dsend, drecv, total,
    qmid, qfar, omid, ofar, osend, smid, sfar, ssend,
    send_sem, recv_sem, sib_sem, loc_sem, x_send, x_recv, ack, kv_send, kv_sib, pair_sem,
):
    s = lax.axis_index("sp")
    t = lax.axis_index("tp")
    c = lax.rem(s, 2)
    z = s // 2
    nz = n_sp // 2
    far, near = nz // 2, nz - 1 - nz // 2
    rows, width = q_ref.shape
    head_width = width // heads
    own_rows = rows // n_tp
    drow, ff = g_ref.shape
    model = drow * n_sp

    def chip(offset):
        return lax.rem(z + offset + nz, nz)

    right = chip(1) * 2 + c
    left = chip(-1) * 2 + c
    sibling = s + 1 - 2 * c
    quarter = nz // 4
    behind, beyond = chip(-quarter) * 2 + c, chip(quarter) * 2 + c
    upper = z >= far
    passes_query = jnp.logical_and(z >= quarter, z < nz - quarter)
    passes_output = jnp.logical_not(passes_query)
    peers = [lax.rem(t + d, n_tp) for d in range(1, n_tp)]
    sources = [lax.rem(t - d + n_tp, n_tp) for d in range(1, n_tp)]

    half = drow // 2
    views = (
        (kbuf, 0, kbuf.shape[1]), (vbuf, 0, vbuf.shape[1]), (gbuf, 0, drow), (ubuf, 0, drow),
        (dbuf, 0, half), (dbuf, half, half),
    )

    def piece(st, slot):
        buf, start, size = views[st]
        return buf.at[slot, pl.ds(start, size)]

    reaches = ((near, 0), (near, 0), (near - 1, far + 1), (near, far), (near, far), (near, far))
    ways = nz

    def reach(st):
        return reaches[st]

    def link_copy(st, slot, direction, step):
        return pltpu.make_async_remote_copy(
            src_ref=piece(st, slot), dst_ref=piece(st, slot),
            send_sem=kv_send.at[st, step - 1] if st < 2 else send_sem.at[st],
            recv_sem=recv_sem.at[st, direction, step - 1],
            device_id={"sp": right if direction == 0 else left}, device_id_type=MESH,
        )

    def sib_copy(st, slot, index):
        return pltpu.make_async_remote_copy(
            src_ref=piece(st, slot), dst_ref=piece(st, slot),
            send_sem=kv_sib.at[st, index] if st < 2 else send_sem.at[st],
            recv_sem=sib_sem.at[st, index], device_id={"sp": sibling}, device_id_type=MESH,
        )

    def usable(st, direction, step):
        fits = jnp.logical_and(step >= 1, step <= reach(st)[direction])
        return jnp.logical_and(fits, z - step >= 0) if st < 2 else fits

    def source(direction, step):
        return chip(-step if direction == 0 else step)

    def send_own(st, direction):
        link_copy(st, s, direction, 1).start()

    def arrive(st, direction, step):
        @pl.when(usable(st, direction, step))
        def _():
            slot = source(direction, step) * 2 + c
            link_copy(st, slot, direction, step).wait_recv()
            onward = step < reach(st)[direction]

            @pl.when(jnp.logical_and(onward, z < nz - 1) if st < 2 else onward)
            def _():
                link_copy(st, slot, direction, step + 1).start()

            sib_copy(st, slot, step + ways * direction).start()

    def sib_arrive(pair_of, step):
        for st in pair_of:
            for direction in (0, 1):
                @pl.when(usable(st, direction, step))
                def _():
                    slot = source(direction, step) * 2 + 1 - c
                    sib_copy(st, slot, step + ways * direction).wait_recv()

            @pl.when(step == 0)
            def _():
                sib_copy(st, sibling, 0).wait_recv()

    def local(src, dst, index):
        return pltpu.make_async_copy(src, dst, loc_sem.at[index])

    own_slice = pl.ds(pl.multiple_of(t * own_rows, own_rows), own_rows)
    loads = [
        local(k_ref, kbuf.at[s, pl.ds(0, rows)], 0), local(x_ref, kbuf.at[s, pl.ds(rows, 16)], 1),
        local(v_ref, vbuf.at[s], 2), local(g_ref, gbuf.at[s], 3), local(u_ref, ubuf.at[s], 4),
        local(d_ref, dbuf.at[s], 5), local(res_ref.at[own_slice], resv, 6),
    ]
    for load in loads:
        load.start()

    lower = [z == 0, z < nz - 1, c == 1, z < quarter, z < nz - quarter]
    lower += [peer < t for peer in peers]
    axis = ["sp"] * 5 + ["tp"] * (n_tp - 1)
    partner = [left, right, sibling, behind, beyond] + peers
    theirs = [1, 0, 2, None, 3] + [4 + n_tp - d for d in range(1, n_tp)]
    barrier = pltpu.get_barrier_semaphore()
    for k in range(4 + n_tp):
        @pl.when(lower[k])
        def _():
            pl.semaphore_signal(barrier, inc=1, device_id={axis[k]: partner[k]}, device_id_type=MESH)

    higher = sum(jnp.where(low, 0, 1) for low in lower)

    @pl.when(higher > 0)
    def _():
        pl.semaphore_wait(barrier, higher)

    for k in range(4 + n_tp):
        if theirs[k] is None:
            continue

        @pl.when(jnp.logical_not(lower[k]))
        def _():
            pl.semaphore_signal(
                ack.at[theirs[k]], inc=1, device_id={axis[k]: partner[k]}, device_id_type=MESH
            )

    def ready(k):
        @pl.when(lower[k])
        def _():
            pl.semaphore_wait(ack.at[k], 1)

    kv, gu, dn = (0, 1), (2, 3), (4, 5)
    edge = jnp.logical_or(z == 0, z == nz - 1)
    for load in loads[:3]:
        load.wait()
    ready(1)

    @pl.when(z < nz - 1)
    def _():
        for st in kv:
            send_own(st, 0)

    def back_copy(src, dst, send, receive):
        return pltpu.make_async_remote_copy(
            src_ref=src, dst_ref=dst, send_sem=pair_sem.at[send], recv_sem=pair_sem.at[receive],
            device_id={"sp": behind}, device_id_type=MESH,
        )

    query_copy = back_copy(q_ref, qmid, 0, 2)
    query_relay = back_copy(qmid, qfar, 1, 3)
    outputs = [back_copy(osend, omid, 4, 8), back_copy(ssend, smid, 5, 9)]
    output_relays = [back_copy(omid, ofar, 6, 10), back_copy(smid, sfar, 7, 11)]

    @pl.when(upper)
    def _():
        query_copy.start()

    for load in loads[3:]:
        load.wait()

    @pl.when(edge)
    def _():
        for st in gu:
            send_own(st, 0)

    ready(2)
    for st in kv:
        sib_copy(st, s, 0).start()
    ready(0)
    for st in gu:
        send_own(st, 1)
    for st in gu + dn:
        sib_copy(st, s, 0).start()

    lane_head = lax.broadcasted_iota(jnp.int32, (rows, width), 1) // head_width

    def prepare(which, ref):
        scaled = ref[...].astype(F32) * (head_width ** -0.5)
        for h in range(heads):
            q4[which, h] = jnp.where(lane_head == h, scaled, 0.0).astype(BF16)
            m_s[which, h] = jnp.full((rows, LANES), -1e30, F32)
            l_s[which, h] = jnp.zeros((rows, LANES), F32)
            acc[which, h] = jnp.zeros((rows, width), F32)

    prepare(0, q_ref)

    def wide(x, size):
        return jnp.concatenate([x] * (size // LANES), axis=1) if size >= LANES else x[:, :size]

    def attend(which, slot, diagonal):
        key = kbuf[slot, 0:rows, :]
        parts = kbuf[slot, rows:rows + 16, :].astype(F32)
        gates = parts[0:heads] + parts[heads:2 * heads] + parts[2 * heads:3 * heads]
        value = vbuf[slot]
        for h in range(heads):
            score = lax.dot_general(q4[which, h], key, NT_DIMS, preferred_element_type=F32) - gates[h:h + 1, :rows]
            if diagonal:
                at = lax.broadcasted_iota(jnp.int32, (rows, rows), 0)
                col = lax.broadcasted_iota(jnp.int32, (rows, rows), 1)
                score = jnp.where(col <= at, score, -1e30)
            before = m_s[which, h]
            top = jnp.maximum(before, jnp.max(score, axis=1, keepdims=True))
            weight = jnp.exp(score - wide(top, rows))
            rescale = jnp.exp(before - top)
            lanes = weight[:, 0:LANES]
            for k in range(1, rows // LANES):
                lanes = lanes + weight[:, k * LANES:(k + 1) * LANES]
            l_s[which, h] = l_s[which, h] * rescale + lanes
            product = jnp.dot(weight.astype(BF16), value, preferred_element_type=F32)
            acc[which, h] = acc[which, h] * wide(rescale, width) + product
            m_s[which, h] = top

    attend(0, s, True)

    ahead_from = near - 2

    def kv_step(i, _):
        for half, st in enumerate(kv):
            arrive(st, 0, i)
            if half == 1:
                @pl.when(jnp.logical_and(jnp.logical_not(edge), i == jnp.minimum(z, near - 1)))
                def _():
                    for own in gu:
                        send_own(own, 0)

                for own in gu:
                    arrive(own, 1, jnp.where(i >= far - 2, i - far + 4, jnp.where(i == far - 4, 1, 0)) * (i <= near))

                @pl.when(i <= far)
                def _():
                    sib_arrive(kv, i - 1)

                @pl.when(jnp.logical_and(i == 2, passes_query))
                def _():
                    query_copy.wait_recv()
                    query_relay.start()

                @pl.when(jnp.logical_and(i == ahead_from - 1, jnp.logical_not(upper)))
                def _():
                    query_relay.wait_recv()
                    prepare(1, qfar)

            turn = 2 * (i - ahead_from) + half

            def block(b, _):
                which = jnp.where(b == 0, 0, 1)
                j = jnp.where(b == 0, i - 1, turn)
                core = jnp.where(b == 0, c if half == 0 else 1 - c, b - 1)
                fits = jnp.logical_and(jnp.logical_and(j >= 0, j <= near), z - j >= 0)
                own = jnp.logical_or(j > 0, jnp.logical_and(half == 1, c == 1))
                needed = jnp.logical_and(fits, jnp.where(b == 0, own, jnp.logical_not(upper)))

                @pl.when(needed)
                def _():
                    attend(which, chip(-j) * 2 + core, False)

                return 0

            lax.fori_loop(0, 3, block, 0)
        return 0

    lax.fori_loop(1, far + 1, kv_step, 0)

    early = 3

    def gu_step(k):
        for st in gu:
            arrive(st, 0, k)
            arrive(st, 1, k + early)

    def merge(which):
        merged = jnp.zeros((rows, width), F32)
        for h in range(heads):
            norm = jnp.sum(l_s[which, h], axis=1, keepdims=True)
            merged = jnp.where(lane_head == h, acc[which, h] / norm, merged)
        return merged

    lane = lax.broadcasted_iota(jnp.int32, (rows, LANES), 1)

    @pl.when(jnp.logical_not(upper))
    def _():
        osend[...] = merge(1).astype(BF16)
        stats = jnp.zeros((rows, LANES), F32)
        for h in range(heads):
            stats = jnp.where(lane == h, m_s[1, h], stats)
            stats = jnp.where(lane == heads + h, jnp.sum(l_s[1, h], axis=1, keepdims=True), stats)
        ssend[...] = stats.T[0:2 * heads, :]

    @pl.when(jnp.logical_not(upper))
    def _():
        att[...] = merge(0).astype(BF16)
        ready(3)
        for copy in outputs:
            copy.start()

    gu_step(1)

    @pl.when(passes_output)
    def _():
        for copy in outputs:
            copy.wait_recv()
        for copy in output_relays:
            copy.start()

    gu_step(2)

    @pl.when(upper)
    def _():
        for copy in output_relays:
            copy.wait_recv()
        stats = jnp.concatenate([sfar[...], jnp.zeros((LANES - 2 * heads, rows), F32)], axis=0).T
        other = ofar[...].astype(F32)
        merged = jnp.zeros((rows, width), F32)
        for h in range(heads):
            mine, theirs_max = m_s[0, h][:, 0:1], stats[:, h:h + 1]
            top = jnp.maximum(mine, theirs_max)
            mine_scale = jnp.exp(mine - top)
            theirs_sum = stats[:, heads + h:heads + h + 1] * jnp.exp(theirs_max - top)
            norm = jnp.sum(l_s[0, h], axis=1, keepdims=True) * mine_scale + theirs_sum
            merged = jnp.where(lane_head == h, (acc[0, h] * mine_scale + other * theirs_sum) / norm, merged)
        att[...] = merged.astype(BF16)

    tile = min(512, model)

    def project(k, _):
        at = pl.ds(pl.multiple_of(k * tile, tile), tile)
        y = jnp.dot(att[...], wout_ref[:, at], preferred_element_type=F32).astype(BF16)
        pbuf[:, :, at] = y.reshape(n_tp, own_rows, tile)
        return 0

    lax.fori_loop(0, model // tile, project, 0)

    def reduce_copy(d):
        return pltpu.make_async_remote_copy(
            src_ref=pbuf.at[peers[d]], dst_ref=rsbuf.at[t], send_sem=x_send.at[0], recv_sem=x_recv.at[0, d],
            device_id={"tp": peers[d]}, device_id_type=MESH,
        )

    def gather_copy(d):
        return pltpu.make_async_remote_copy(
            src_ref=nbuf.at[t], dst_ref=nbuf.at[t], send_sem=x_send.at[1], recv_sem=x_recv.at[1, d],
            device_id={"tp": peers[d]}, device_id_type=MESH,
        )

    def arrival(buf, sem):
        return pltpu.make_async_copy(buf, buf, sem)

    arrive(gu[0], 0, 3)
    arrive(gu[0], 1, 3 + early)
    for d in range(n_tp - 1):
        ready(5 + d)
        reduce_copy(d).start()
    arrive(gu[1], 0, 3)
    arrive(gu[1], 1, 3 + early)
    for k in range(4, near - 1):
        gu_step(k)
    for d in range(n_tp - 1):
        arrival(rsbuf.at[sources[d]], x_recv.at[0, d]).wait()
    summed = resv[...].astype(F32) + pbuf[t].astype(F32)
    for d in range(n_tp - 1):
        summed = summed + rsbuf[sources[d]].astype(F32)
    mixed[...] = summed.astype(BF16)
    floats = mixed[...].astype(F32)
    mean = jnp.sum(floats * floats, axis=1, keepdims=True) * (1.0 / model)
    nbuf[t] = (floats * lax.rsqrt(mean + 1e-6) * gain_ref[...]).astype(BF16)
    for d in range(n_tp - 1):
        gather_copy(d).start()

    gu_step(near - 1)
    for st in dn:
        send_own(st, 1)
        send_own(st, 0)
    gu_step(near)

    def dn_step(k):
        for st in dn:
            for direction in (0, 1):
                arrive(st, direction, k)

    dn_step(1)

    def gu_sib(i, _):
        sib_arrive(gu, i)
        return 0

    lax.fori_loop(0, far + 2, gu_sib, 0)
    for d in range(n_tp - 1):
        arrival(nbuf.at[sources[d]], x_recv.at[1, d]).wait()

    tiles = ff // LANES
    chip_rows = 2 * drow

    def accumulate(offsets, first, final):
        chips = [chip(o) for o in offsets]
        left_side = jnp.concatenate(
            [nbuf[:, :, pl.ds(pl.multiple_of(at * chip_rows, chip_rows), chip_rows)] for at in chips], axis=2
        ).reshape(rows, len(chips) * chip_rows)

        def one(k, _):
            at = pl.ds(pl.multiple_of(k * LANES, LANES), LANES)
            sides = [
                jnp.concatenate(
                    [buf[pl.ds(2 * chosen, 2), :, at].reshape(chip_rows, LANES) for chosen in chips], axis=0
                )
                for buf in (gbuf, ubuf)
            ]
            both = jnp.dot(left_side, jnp.concatenate(sides, axis=1), preferred_element_type=F32)
            if not first:
                both = both + hacc[k]
            if final:
                gate, up = both[:, :LANES], both[:, LANES:]
                hid[:, at] = (gate / (1.0 + jnp.exp(-gate)) * up).astype(BF16)
            else:
                hacc[k] = both
            return 0

        lax.fori_loop(0, tiles, one, 0)

    offsets = [0] + [o for j in range(1, far) for o in (-j, j)] + [far]
    group = -(-len(offsets) // 4)
    for k in range(4):
        accumulate(offsets[k * group:(k + 1) * group], k == 0, k == 3)
        dn_step(k + 2)

    def column_copy(d, at):
        return pltpu.make_async_remote_copy(
            src_ref=dsend.at[at, peers[d]], dst_ref=drecv.at[t, at], send_sem=x_send.at[2],
            recv_sem=x_recv.at[2, d], device_id={"tp": peers[d]}, device_id_type=MESH,
        )

    def down_step(j, _):
        @pl.when(jnp.logical_and(lax.rem(j, 3) == 0, 6 + j // 3 <= far))
        def _():
            dn_step(6 + j // 3)

        sib_arrive(dn, j)
        back, ahead = chip(j), chip(-j)
        weights = jnp.concatenate(
            [dbuf[pl.ds(at * 2, 2)].reshape(2 * drow, ff) for at in (back, ahead)], axis=0
        )
        y = lax.dot_general(hid[...], weights, NT_DIMS, preferred_element_type=F32).astype(BF16)
        y = y.reshape(n_tp, own_rows, 4 * drow)
        dsend[back] = y[:, :, :2 * drow]
        for d in range(n_tp - 1):
            column_copy(d, back).start()

        @pl.when(jnp.logical_and(j >= 1, j <= near))
        def _():
            dsend[ahead] = y[:, :, 2 * drow:]
            for d in range(n_tp - 1):
                column_copy(d, ahead).start()

        return 0

    lax.fori_loop(0, far + 1, down_step, 0)

    for d in range(n_tp - 1):
        arrival(drecv.at[sources[d]], x_recv.at[2, d]).wait()
    square = jnp.zeros((own_rows, 2 * drow), F32)
    for at in range(nz):
        cols = slice(at * 2 * drow, (at + 1) * 2 * drow)
        down = dsend[at, t].astype(F32)
        for d in range(n_tp - 1):
            down = down + drecv[sources[d], at].astype(F32)
        value = mixed[:, cols].astype(F32) + 0.5 * down
        total[:, cols] = value
        square = square + value * value
    mean = jnp.sum(square, axis=1, keepdims=True) * (1.0 / model)
    out_ref[...] = (total[...] * lax.rsqrt(mean + 1e-6)).astype(BF16)

    for st in kv:
        for k in range(near):
            @pl.when(jnp.logical_and(z < nz - 1, z >= k))
            def _():
                link_copy(st, s, 0, k + 1).wait_send()

        for k in range(near + 1):
            @pl.when(z >= k)
            def _():
                sib_copy(st, s, k).wait_send()

    @pl.when(upper)
    def _():
        query_copy.wait_send()

    @pl.when(passes_query)
    def _():
        query_relay.wait_send()

    @pl.when(jnp.logical_not(upper))
    def _():
        for copy in outputs:
            copy.wait_send()

    @pl.when(passes_output)
    def _():
        for copy in output_relays:
            copy.wait_send()

    for st in gu + dn:
        buf, start, size = views[st]
        arrival(buf.at[pl.ds(0, 2 * nz - 1), pl.ds(start, size)], send_sem.at[st]).wait()
    arrival(pbuf.at[pl.ds(0, n_tp - 1)], x_send.at[0]).wait()
    arrival(nbuf.at[pl.ds(0, n_tp - 1)], x_send.at[1]).wait()
    arrival(drecv.at[pl.ds(0, n_tp - 1)], x_send.at[2]).wait()


def body(residual, queries, keys, values, log_gates, w_out, norm_gain, w_gate, w_up, w_down):
    n_sp, n_tp = lax.axis_size("sp"), lax.axis_size("tp")
    rows, width = queries.shape
    heads = log_gates.shape[1]
    model = residual.shape[1]
    drow, ff = w_gate.shape
    own_rows = rows // n_tp
    nz = n_sp // 2
    far = nz // 2

    gates = log_gates.T
    high = lax.reduce_precision(gates, 8, 7)
    middle = lax.reduce_precision(gates - high, 8, 7)
    low = gates - high - middle
    extra = jnp.concatenate([high, middle, low, jnp.zeros((16 - 3 * heads, rows), F32)], axis=0).astype(BF16)
    vmem = pl.BlockSpec(memory_space=pltpu.VMEM)
    hbm = pl.BlockSpec(memory_space=pl.ANY)
    return pl.pallas_call(
        functools.partial(layer_kernel, n_sp, n_tp, heads),
        out_shape=jax.ShapeDtypeStruct((own_rows, model), BF16),
        in_specs=[vmem, hbm, hbm, hbm, hbm, vmem, vmem, hbm, hbm, hbm],
        out_specs=vmem,
        scratch_shapes=[
            pltpu.VMEM((n_sp, rows + 16, width), BF16),
            pltpu.VMEM((n_sp, rows, width), BF16),
            pltpu.VMEM((n_sp, drow, ff), BF16),
            pltpu.VMEM((n_sp, drow, ff), BF16),
            pltpu.VMEM((n_sp, drow, ff), BF16),
            pltpu.VMEM((2, heads, rows, width), BF16),
            pltpu.VMEM((2, heads, rows, LANES), F32),
            pltpu.VMEM((2, heads, rows, LANES), F32),
            pltpu.VMEM((2, heads, rows, width), F32),
            pltpu.VMEM((rows, width), BF16),
            pltpu.VMEM((n_tp, own_rows, model), BF16),
            pltpu.VMEM((n_tp, own_rows, model), BF16),
            pltpu.VMEM((own_rows, model), BF16),
            pltpu.VMEM((own_rows, model), BF16),
            pltpu.VMEM((n_tp, own_rows, model), BF16),
            pltpu.VMEM((ff // LANES, rows, 2 * LANES), F32),
            pltpu.VMEM((rows, ff), BF16),
            pltpu.VMEM((nz, n_tp, own_rows, 2 * drow), BF16),
            pltpu.VMEM((n_tp, nz, own_rows, 2 * drow), BF16),
            pltpu.VMEM((own_rows, model), F32),
            *[pltpu.VMEM((rows, width), BF16) for _ in range(5)],
            *[pltpu.VMEM((2 * heads, rows), F32) for _ in range(3)],
            pltpu.SemaphoreType.DMA((6,)),
            pltpu.SemaphoreType.DMA((6, 2, far + 1)),
            pltpu.SemaphoreType.DMA((6, nz + far + 2)),
            pltpu.SemaphoreType.DMA((7,)),
            pltpu.SemaphoreType.DMA((3,)),
            pltpu.SemaphoreType.DMA((3, n_tp - 1)),
            pltpu.SemaphoreType.REGULAR((4 + n_tp,)),
            pltpu.SemaphoreType.DMA((2, far)),
            pltpu.SemaphoreType.DMA((2, far)),
            pltpu.SemaphoreType.DMA((12,)),
        ],
        compiler_params=pltpu.CompilerParams(
            collective_id=0, has_side_effects=True, vmem_limit_bytes=60 * 1024 * 1024
        ),
    )(queries, keys, extra, values, residual, w_out, norm_gain.reshape(1, -1), w_gate, w_up, w_down.T)


def solution(mesh):
    in_specs = (
        P(("grp", "sp"), None),
        P(("grp", "sp"), "tp"),
        P(("grp", "sp"), "tp"),
        P(("grp", "sp"), "tp"),
        P(("grp", "sp"), "tp"),
        P("tp", None),
        P(),
        P("sp", "tp"),
        P("sp", "tp"),
        P("tp", "sp"),
    )
    out_specs = P(("grp", "sp", "tp"), None)
    return jax.shard_map(body, mesh=mesh, in_specs=in_specs, out_specs=out_specs, check_vma=False)
```

```python
import functools

import jax
import jax.numpy as jnp
from jax import lax
from jax.experimental import pallas as pl
from jax.experimental.pallas import tpu as pltpu
from jax.sharding import PartitionSpec as P

MESH = pl.DeviceIdType.MESH
F32 = jnp.float32
BF16 = jnp.bfloat16
NT_DIMS = (((1,), (1,)), ((), ()))
LANES = 128


def layer_kernel(
    n_sp, n_tp, heads,
    q_ref, k_ref, x_ref, v_ref, res_ref, wout_ref, gain_ref, g_ref, u_ref, d_ref,
    out_ref,
    kbuf, vbuf, gbuf, ubuf, dbuf, q4, m_s, l_s, acc, att, pbuf, rsbuf, resv, mixed, nbuf, hacc, hid, dsend, drecv, total,
    qfar, ofar, osend, sfar, ssend,
    send_sem, recv_sem, sib_sem, loc_sem, x_send, x_recv, ack, kv_send, kv_sib, pair_sem,
):
    s = lax.axis_index("sp")
    t = lax.axis_index("tp")
    c = lax.rem(s, 2)
    z = s // 2
    nz = n_sp // 2
    far, near = nz // 2, nz - 1 - nz // 2
    rows, width = q_ref.shape
    head_width = width // heads
    own_rows = rows // n_tp
    drow, ff = g_ref.shape
    model = drow * n_sp

    def chip(offset):
        return lax.rem(z + offset + nz, nz)

    right = chip(1) * 2 + c
    left = chip(-1) * 2 + c
    sibling = s + 1 - 2 * c
    pair = chip(far) * 2 + c
    upper = z >= far
    peers = [lax.rem(t + d, n_tp) for d in range(1, n_tp)]
    sources = [lax.rem(t - d + n_tp, n_tp) for d in range(1, n_tp)]

    half = drow // 2
    views = (
        (kbuf, 0, kbuf.shape[1]), (vbuf, 0, vbuf.shape[1]), (gbuf, 0, drow), (ubuf, 0, drow),
        (dbuf, 0, half), (dbuf, half, half),
    )

    def piece(st, slot):
        buf, start, size = views[st]
        return buf.at[slot, pl.ds(start, size)]

    right_hops = near - 1
    left_hops = nz - 1 - right_hops
    both_ways = (right_hops, left_hops)
    reaches = ((near, 0), (near, 0), (right_hops - 1, left_hops + 1), both_ways, both_ways, both_ways)
    ways = nz

    def reach(st):
        return reaches[st]

    def link_copy(st, slot, direction, step):
        return pltpu.make_async_remote_copy(
            src_ref=piece(st, slot), dst_ref=piece(st, slot),
            send_sem=kv_send.at[st, step - 1] if st < 2 else send_sem.at[st],
            recv_sem=recv_sem.at[st, direction, step - 1],
            device_id={"sp": right if direction == 0 else left}, device_id_type=MESH,
        )

    def sib_copy(st, slot, index):
        return pltpu.make_async_remote_copy(
            src_ref=piece(st, slot), dst_ref=piece(st, slot),
            send_sem=kv_sib.at[st, index] if st < 2 else send_sem.at[st],
            recv_sem=sib_sem.at[st, index], device_id={"sp": sibling}, device_id_type=MESH,
        )

    def usable(st, direction, step):
        fits = jnp.logical_and(step >= 1, step <= reach(st)[direction])
        return jnp.logical_and(fits, z - step >= 0) if st < 2 else fits

    def source(direction, step):
        return chip(-step if direction == 0 else step)

    def send_own(st, direction):
        link_copy(st, s, direction, 1).start()

    def arrive(st, direction, step):
        @pl.when(usable(st, direction, step))
        def _():
            slot = source(direction, step) * 2 + c
            link_copy(st, slot, direction, step).wait_recv()
            onward = step < reach(st)[direction]

            @pl.when(jnp.logical_and(onward, z < nz - 1) if st < 2 else onward)
            def _():
                link_copy(st, slot, direction, step + 1).start()

            sib_copy(st, slot, step + ways * direction).start()

    def sib_arrive(pair_of, step):
        for st in pair_of:
            for direction in (0, 1):
                @pl.when(usable(st, direction, step))
                def _():
                    slot = source(direction, step) * 2 + 1 - c
                    sib_copy(st, slot, step + ways * direction).wait_recv()

            @pl.when(step == 0)
            def _():
                sib_copy(st, sibling, 0).wait_recv()

    def local(src, dst, index):
        return pltpu.make_async_copy(src, dst, loc_sem.at[index])

    own_slice = pl.ds(pl.multiple_of(t * own_rows, own_rows), own_rows)
    loads = [
        local(k_ref, kbuf.at[s, pl.ds(0, rows)], 0), local(x_ref, kbuf.at[s, pl.ds(rows, 16)], 1),
        local(v_ref, vbuf.at[s], 2), local(g_ref, gbuf.at[s], 3), local(u_ref, ubuf.at[s], 4),
        local(d_ref, dbuf.at[s], 5), local(res_ref.at[own_slice], resv, 6),
    ]
    for load in loads:
        load.start()

    lower = [z == 0, z < nz - 1, c == 1, jnp.logical_not(upper)] + [peer < t for peer in peers]
    axis = ["sp", "sp", "sp", "sp"] + ["tp"] * (n_tp - 1)
    partner = [left, right, sibling, pair] + peers
    theirs = [1, 0, 2, 3] + [3 + n_tp - d for d in range(1, n_tp)]
    barrier = pltpu.get_barrier_semaphore()
    for k in range(3 + n_tp):
        @pl.when(lower[k])
        def _():
            pl.semaphore_signal(barrier, inc=1, device_id={axis[k]: partner[k]}, device_id_type=MESH)

    higher = sum(jnp.where(low, 0, 1) for low in lower)

    @pl.when(higher > 0)
    def _():
        pl.semaphore_wait(barrier, higher)

    for k in range(3 + n_tp):
        @pl.when(jnp.logical_not(lower[k]))
        def _():
            pl.semaphore_signal(
                ack.at[theirs[k]], inc=1, device_id={axis[k]: partner[k]}, device_id_type=MESH
            )

    def ready(k):
        @pl.when(lower[k])
        def _():
            pl.semaphore_wait(ack.at[k], 1)

    kv, gu, dn = (0, 1), (2, 3), (4, 5)
    edge = jnp.logical_or(z == 0, z == nz - 1)
    for load in loads[:3]:
        load.wait()
    ready(1)

    @pl.when(z < nz - 1)
    def _():
        for st in kv:
            send_own(st, 0)

    query_copy = pltpu.make_async_remote_copy(
        src_ref=q_ref, dst_ref=qfar, send_sem=pair_sem.at[0], recv_sem=pair_sem.at[1],
        device_id={"sp": pair}, device_id_type=MESH,
    )

    @pl.when(upper)
    def _():
        query_copy.start()

    for load in loads[3:]:
        load.wait()

    @pl.when(edge)
    def _():
        for st in gu:
            send_own(st, 0)

    ready(2)
    for st in kv:
        sib_copy(st, s, 0).start()
    ready(0)
    for st in gu:
        send_own(st, 1)
    for st in gu + dn:
        sib_copy(st, s, 0).start()

    lane_head = lax.broadcasted_iota(jnp.int32, (rows, width), 1) // head_width

    def prepare(which, ref):
        scaled = ref[...].astype(F32) * (head_width ** -0.5)
        for h in range(heads):
            q4[which, h] = jnp.where(lane_head == h, scaled, 0.0).astype(BF16)
            m_s[which, h] = jnp.full((rows, LANES), -1e30, F32)
            l_s[which, h] = jnp.zeros((rows, LANES), F32)
            acc[which, h] = jnp.zeros((rows, width), F32)

    prepare(0, q_ref)

    def wide(x, size):
        return jnp.concatenate([x] * (size // LANES), axis=1) if size >= LANES else x[:, :size]

    def attend(which, slot, diagonal):
        key = kbuf[slot, 0:rows, :]
        parts = kbuf[slot, rows:rows + 16, :].astype(F32)
        gates = parts[0:heads] + parts[heads:2 * heads] + parts[2 * heads:3 * heads]
        value = vbuf[slot]
        for h in range(heads):
            score = lax.dot_general(q4[which, h], key, NT_DIMS, preferred_element_type=F32) - gates[h:h + 1, :rows]
            if diagonal:
                at = lax.broadcasted_iota(jnp.int32, (rows, rows), 0)
                col = lax.broadcasted_iota(jnp.int32, (rows, rows), 1)
                score = jnp.where(col <= at, score, -1e30)
            before = m_s[which, h]
            top = jnp.maximum(before, jnp.max(score, axis=1, keepdims=True))
            weight = jnp.exp(score - wide(top, rows))
            rescale = jnp.exp(before - top)
            lanes = weight[:, 0:LANES]
            for k in range(1, rows // LANES):
                lanes = lanes + weight[:, k * LANES:(k + 1) * LANES]
            l_s[which, h] = l_s[which, h] * rescale + lanes
            product = jnp.dot(weight.astype(BF16), value, preferred_element_type=F32)
            acc[which, h] = acc[which, h] * wide(rescale, width) + product
            m_s[which, h] = top

    attend(0, s, True)

    ahead_from = near - 1

    def kv_step(i, _):
        for half, st in enumerate(kv):
            arrive(st, 0, i)
            if half == 1:
                @pl.when(jnp.logical_and(jnp.logical_not(edge), i == jnp.minimum(z, near - 1)))
                def _():
                    for own in gu:
                        send_own(own, 0)

                for own in gu:
                    arrive(own, 1, jnp.where(i >= 5, i - 2, jnp.where(i == 4, 0, i - 1)) * (i <= near))

                @pl.when(i <= far)
                def _():
                    sib_arrive(kv, i - 1)

                @pl.when(jnp.logical_and(i == ahead_from - 1, jnp.logical_not(upper)))
                def _():
                    query_copy.wait_recv()
                    prepare(1, qfar)

            turn = 2 * (i - ahead_from) + half

            def block(b, _):
                which = jnp.where(b == 0, 0, 1)
                j = jnp.where(b == 0, i - 1, turn)
                core = jnp.where(b == 0, c if half == 0 else 1 - c, b - 1)
                fits = jnp.logical_and(jnp.logical_and(j >= 0, j <= near), z - j >= 0)
                own = jnp.logical_or(j > 0, jnp.logical_and(half == 1, c == 1))
                needed = jnp.logical_and(fits, jnp.where(b == 0, own, jnp.logical_not(upper)))

                @pl.when(needed)
                def _():
                    attend(which, chip(-j) * 2 + core, False)

                return 0

            lax.fori_loop(0, 3, block, 0)
        return 0

    lax.fori_loop(1, far + 2, kv_step, 0)

    early = near - 2

    def gu_step(k):
        for st in gu:
            arrive(st, 0, k)
            arrive(st, 1, k + early)

    def merge(which):
        merged = jnp.zeros((rows, width), F32)
        for h in range(heads):
            norm = jnp.sum(l_s[which, h], axis=1, keepdims=True)
            merged = jnp.where(lane_head == h, acc[which, h] / norm, merged)
        return merged

    def far_copy(k):
        return pltpu.make_async_remote_copy(
            src_ref=(osend, ssend)[k], dst_ref=(ofar, sfar)[k], send_sem=pair_sem.at[2 + k],
            recv_sem=pair_sem.at[4 + k], device_id={"sp": pair}, device_id_type=MESH,
        )

    lane = lax.broadcasted_iota(jnp.int32, (rows, LANES), 1)

    @pl.when(jnp.logical_not(upper))
    def _():
        osend[...] = merge(1).astype(BF16)
        stats = jnp.zeros((rows, LANES), F32)
        for h in range(heads):
            stats = jnp.where(lane == h, m_s[1, h], stats)
            stats = jnp.where(lane == heads + h, jnp.sum(l_s[1, h], axis=1, keepdims=True), stats)
        ssend[...] = stats.T[0:2 * heads, :]

    for direction_step in (1,):
        gu_step(direction_step)

    @pl.when(jnp.logical_not(upper))
    def _():
        ready(3)
        for k in (0, 1):
            far_copy(k).start()
        att[...] = merge(0).astype(BF16)

    gu_step(2)

    @pl.when(upper)
    def _():
        for k in (0, 1):
            far_copy(k).wait_recv()
        stats = jnp.concatenate([sfar[...], jnp.zeros((LANES - 2 * heads, rows), F32)], axis=0).T
        other = ofar[...].astype(F32)
        merged = jnp.zeros((rows, width), F32)
        for h in range(heads):
            mine, theirs_max = m_s[0, h][:, 0:1], stats[:, h:h + 1]
            top = jnp.maximum(mine, theirs_max)
            mine_scale = jnp.exp(mine - top)
            theirs_sum = stats[:, heads + h:heads + h + 1] * jnp.exp(theirs_max - top)
            norm = jnp.sum(l_s[0, h], axis=1, keepdims=True) * mine_scale + theirs_sum
            merged = jnp.where(lane_head == h, (acc[0, h] * mine_scale + other * theirs_sum) / norm, merged)
        att[...] = merged.astype(BF16)

    tile = min(512, model)

    def project(k, _):
        at = pl.ds(pl.multiple_of(k * tile, tile), tile)
        y = jnp.dot(att[...], wout_ref[:, at], preferred_element_type=F32).astype(BF16)
        pbuf[:, :, at] = y.reshape(n_tp, own_rows, tile)
        return 0

    lax.fori_loop(0, model // tile, project, 0)

    def reduce_copy(d):
        return pltpu.make_async_remote_copy(
            src_ref=pbuf.at[peers[d]], dst_ref=rsbuf.at[t], send_sem=x_send.at[0], recv_sem=x_recv.at[0, d],
            device_id={"tp": peers[d]}, device_id_type=MESH,
        )

    def gather_copy(d):
        return pltpu.make_async_remote_copy(
            src_ref=nbuf.at[t], dst_ref=nbuf.at[t], send_sem=x_send.at[1], recv_sem=x_recv.at[1, d],
            device_id={"tp": peers[d]}, device_id_type=MESH,
        )

    def arrival(buf, sem):
        return pltpu.make_async_copy(buf, buf, sem)

    gu_step(3)
    for d in range(n_tp - 1):
        ready(4 + d)
        reduce_copy(d).start()
    for k in range(4, right_hops):
        gu_step(k)
    for st in dn:
        send_own(st, 1)
        send_own(st, 0)
    for d in range(n_tp - 1):
        arrival(rsbuf.at[sources[d]], x_recv.at[0, d]).wait()
    summed = resv[...].astype(F32) + pbuf[t].astype(F32)
    for d in range(n_tp - 1):
        summed = summed + rsbuf[sources[d]].astype(F32)
    mixed[...] = summed.astype(BF16)
    floats = mixed[...].astype(F32)
    mean = jnp.sum(floats * floats, axis=1, keepdims=True) * (1.0 / model)
    nbuf[t] = (floats * lax.rsqrt(mean + 1e-6) * gain_ref[...]).astype(BF16)
    for d in range(n_tp - 1):
        gather_copy(d).start()

    gu_step(right_hops)

    def dn_step(k):
        for st in dn:
            for direction in (0, 1):
                arrive(st, direction, k)

    dn_step(1)

    def gu_sib(i, _):
        sib_arrive(gu, i)
        return 0

    lax.fori_loop(0, left_hops + 2, gu_sib, 0)
    for d in range(n_tp - 1):
        arrival(nbuf.at[sources[d]], x_recv.at[1, d]).wait()

    tiles = ff // LANES
    chip_rows = 2 * drow

    def accumulate(offsets, first, final):
        chips = [chip(o) for o in offsets]
        left_side = jnp.concatenate(
            [nbuf[:, :, pl.ds(pl.multiple_of(at * chip_rows, chip_rows), chip_rows)] for at in chips], axis=2
        ).reshape(rows, len(chips) * chip_rows)

        def one(k, _):
            at = pl.ds(pl.multiple_of(k * LANES, LANES), LANES)
            sides = [
                jnp.concatenate(
                    [buf[pl.ds(2 * chosen, 2), :, at].reshape(chip_rows, LANES) for chosen in chips], axis=0
                )
                for buf in (gbuf, ubuf)
            ]
            both = jnp.dot(left_side, jnp.concatenate(sides, axis=1), preferred_element_type=F32)
            if not first:
                both = both + hacc[k]
            if final:
                gate, up = both[:, :LANES], both[:, LANES:]
                hid[:, at] = (gate / (1.0 + jnp.exp(-gate)) * up).astype(BF16)
            else:
                hacc[k] = both
            return 0

        lax.fori_loop(0, tiles, one, 0)

    offsets = [0] + [-j for j in range(1, right_hops + 1)] + list(range(1, left_hops + 1))
    group = -(-len(offsets) // 4)
    for k in range(4):
        accumulate(offsets[k * group:(k + 1) * group], k == 0, k == 3)
        dn_step(k + 2)

    def column_copy(d, at):
        return pltpu.make_async_remote_copy(
            src_ref=dsend.at[at, peers[d]], dst_ref=drecv.at[t, at], send_sem=x_send.at[2],
            recv_sem=x_recv.at[2, d], device_id={"tp": peers[d]}, device_id_type=MESH,
        )

    def down_step(j, _):
        @pl.when(jnp.logical_and(lax.rem(j, 2) == 0, 6 + j // 2 <= left_hops))
        def _():
            dn_step(6 + j // 2)

        sib_arrive(dn, j)
        back, ahead = chip(j), chip(jnp.where(j <= right_hops, -j, j))
        weights = jnp.concatenate(
            [dbuf[pl.ds(at * 2, 2)].reshape(2 * drow, ff) for at in (back, ahead)], axis=0
        )
        y = lax.dot_general(hid[...], weights, NT_DIMS, preferred_element_type=F32).astype(BF16)
        y = y.reshape(n_tp, own_rows, 4 * drow)
        dsend[back] = y[:, :, :2 * drow]
        for d in range(n_tp - 1):
            column_copy(d, back).start()

        @pl.when(jnp.logical_and(j >= 1, j <= right_hops))
        def _():
            dsend[ahead] = y[:, :, 2 * drow:]
            for d in range(n_tp - 1):
                column_copy(d, ahead).start()

        return 0

    lax.fori_loop(0, left_hops + 1, down_step, 0)

    for d in range(n_tp - 1):
        arrival(drecv.at[sources[d]], x_recv.at[2, d]).wait()
    square = jnp.zeros((own_rows, 2 * drow), F32)
    for at in range(nz):
        cols = slice(at * 2 * drow, (at + 1) * 2 * drow)
        down = dsend[at, t].astype(F32)
        for d in range(n_tp - 1):
            down = down + drecv[sources[d], at].astype(F32)
        value = mixed[:, cols].astype(F32) + 0.5 * down
        total[:, cols] = value
        square = square + value * value
    mean = jnp.sum(square, axis=1, keepdims=True) * (1.0 / model)
    out_ref[...] = (total[...] * lax.rsqrt(mean + 1e-6)).astype(BF16)

    for st in kv:
        for k in range(near):
            @pl.when(jnp.logical_and(z < nz - 1, z >= k))
            def _():
                link_copy(st, s, 0, k + 1).wait_send()

        for k in range(near + 1):
            @pl.when(z >= k)
            def _():
                sib_copy(st, s, k).wait_send()

    @pl.when(upper)
    def _():
        query_copy.wait_send()

    @pl.when(jnp.logical_not(upper))
    def _():
        for k in (0, 1):
            far_copy(k).wait_send()

    for st in gu + dn:
        buf, start, size = views[st]
        arrival(buf.at[pl.ds(0, 2 * nz - 1), pl.ds(start, size)], send_sem.at[st]).wait()
    arrival(pbuf.at[pl.ds(0, n_tp - 1)], x_send.at[0]).wait()
    arrival(nbuf.at[pl.ds(0, n_tp - 1)], x_send.at[1]).wait()
    arrival(drecv.at[pl.ds(0, n_tp - 1)], x_send.at[2]).wait()


def body(residual, queries, keys, values, log_gates, w_out, norm_gain, w_gate, w_up, w_down):
    n_sp, n_tp = lax.axis_size("sp"), lax.axis_size("tp")
    rows, width = queries.shape
    heads = log_gates.shape[1]
    model = residual.shape[1]
    drow, ff = w_gate.shape
    own_rows = rows // n_tp
    nz = n_sp // 2
    far = nz // 2

    gates = log_gates.T
    high = lax.reduce_precision(gates, 8, 7)
    middle = lax.reduce_precision(gates - high, 8, 7)
    low = gates - high - middle
    extra = jnp.concatenate([high, middle, low, jnp.zeros((16 - 3 * heads, rows), F32)], axis=0).astype(BF16)
    vmem = pl.BlockSpec(memory_space=pltpu.VMEM)
    hbm = pl.BlockSpec(memory_space=pl.ANY)
    return pl.pallas_call(
        functools.partial(layer_kernel, n_sp, n_tp, heads),
        out_shape=jax.ShapeDtypeStruct((own_rows, model), BF16),
        in_specs=[vmem, hbm, hbm, hbm, hbm, vmem, vmem, hbm, hbm, hbm],
        out_specs=vmem,
        scratch_shapes=[
            pltpu.VMEM((n_sp, rows + 16, width), BF16),
            pltpu.VMEM((n_sp, rows, width), BF16),
            pltpu.VMEM((n_sp, drow, ff), BF16),
            pltpu.VMEM((n_sp, drow, ff), BF16),
            pltpu.VMEM((n_sp, drow, ff), BF16),
            pltpu.VMEM((2, heads, rows, width), BF16),
            pltpu.VMEM((2, heads, rows, LANES), F32),
            pltpu.VMEM((2, heads, rows, LANES), F32),
            pltpu.VMEM((2, heads, rows, width), F32),
            pltpu.VMEM((rows, width), BF16),
            pltpu.VMEM((n_tp, own_rows, model), BF16),
            pltpu.VMEM((n_tp, own_rows, model), BF16),
            pltpu.VMEM((own_rows, model), BF16),
            pltpu.VMEM((own_rows, model), BF16),
            pltpu.VMEM((n_tp, own_rows, model), BF16),
            pltpu.VMEM((ff // LANES, rows, 2 * LANES), F32),
            pltpu.VMEM((rows, ff), BF16),
            pltpu.VMEM((nz, n_tp, own_rows, 2 * drow), BF16),
            pltpu.VMEM((n_tp, nz, own_rows, 2 * drow), BF16),
            pltpu.VMEM((own_rows, model), F32),
            pltpu.VMEM((rows, width), BF16),
            pltpu.VMEM((rows, width), BF16),
            pltpu.VMEM((rows, width), BF16),
            pltpu.VMEM((2 * heads, rows), F32),
            pltpu.VMEM((2 * heads, rows), F32),
            pltpu.SemaphoreType.DMA((6,)),
            pltpu.SemaphoreType.DMA((6, 2, nz)),
            pltpu.SemaphoreType.DMA((6, 2 * nz)),
            pltpu.SemaphoreType.DMA((7,)),
            pltpu.SemaphoreType.DMA((3,)),
            pltpu.SemaphoreType.DMA((3, n_tp - 1)),
            pltpu.SemaphoreType.REGULAR((3 + n_tp,)),
            pltpu.SemaphoreType.DMA((2, far)),
            pltpu.SemaphoreType.DMA((2, far)),
            pltpu.SemaphoreType.DMA((6,)),
        ],
        compiler_params=pltpu.CompilerParams(
            collective_id=0, has_side_effects=True, vmem_limit_bytes=60 * 1024 * 1024
        ),
    )(queries, keys, extra, values, residual, w_out, norm_gain.reshape(1, -1), w_gate, w_up, w_down.T)


def solution(mesh):
    in_specs = (
        P(("grp", "sp"), None),
        P(("grp", "sp"), "tp"),
        P(("grp", "sp"), "tp"),
        P(("grp", "sp"), "tp"),
        P(("grp", "sp"), "tp"),
        P("tp", None),
        P(),
        P("sp", "tp"),
        P("sp", "tp"),
        P("tp", "sp"),
    )
    out_specs = P(("grp", "sp", "tp"), None)
    return jax.shard_map(body, mesh=mesh, in_specs=in_specs, out_specs=out_specs, check_vma=False)
```

```python
import functools

import jax
import jax.numpy as jnp
from jax import lax
from jax.experimental import pallas as pl
from jax.experimental.pallas import tpu as pltpu
from jax.sharding import PartitionSpec as P

MESH = pl.DeviceIdType.MESH
F32 = jnp.float32
BF16 = jnp.bfloat16
NT_DIMS = (((1,), (1,)), ((), ()))
LANES = 128


def layer_kernel(
    n_sp, n_tp, heads,
    q_ref, k_ref, x_ref, v_ref, res_ref, wout_ref, gain_ref, g_ref, u_ref, d_ref,
    out_ref,
    kbuf, vbuf, gbuf, ubuf, dbuf, q4, m_s, l_s, acc, att, pbuf, rsbuf, resv, mixed, nbuf, hacc, hid, dsend, drecv, total,
    qfar, ofar, osend, sfar, ssend,
    send_sem, recv_sem, sib_sem, loc_sem, x_send, x_recv, ack, kv_send, kv_sib, pair_sem,
):
    s = lax.axis_index("sp")
    t = lax.axis_index("tp")
    c = lax.rem(s, 2)
    z = s // 2
    nz = n_sp // 2
    far, near = nz // 2, nz - 1 - nz // 2
    rows, width = q_ref.shape
    head_width = width // heads
    own_rows = rows // n_tp
    drow, ff = g_ref.shape
    model = drow * n_sp

    def chip(offset):
        return lax.rem(z + offset + nz, nz)

    right = chip(1) * 2 + c
    left = chip(-1) * 2 + c
    sibling = s + 1 - 2 * c
    pair = chip(far) * 2 + c
    upper = z >= far
    peers = [lax.rem(t + d, n_tp) for d in range(1, n_tp)]
    sources = [lax.rem(t - d + n_tp, n_tp) for d in range(1, n_tp)]

    half = drow // 2
    views = (
        (kbuf, 0, kbuf.shape[1]), (vbuf, 0, vbuf.shape[1]), (gbuf, 0, drow), (ubuf, 0, drow),
        (dbuf, 0, half), (dbuf, half, half),
    )

    def piece(st, slot):
        buf, start, size = views[st]
        return buf.at[slot, pl.ds(start, size)]

    reaches = ((near, 0), (near, 0), (near - 1, far + 1), (near, far), (near, far), (near, far))
    ways = nz

    def reach(st):
        return reaches[st]

    def link_copy(st, slot, direction, step):
        return pltpu.make_async_remote_copy(
            src_ref=piece(st, slot), dst_ref=piece(st, slot),
            send_sem=kv_send.at[st, step - 1] if st < 2 else send_sem.at[st],
            recv_sem=recv_sem.at[st, direction, step - 1],
            device_id={"sp": right if direction == 0 else left}, device_id_type=MESH,
        )

    def sib_copy(st, slot, index):
        return pltpu.make_async_remote_copy(
            src_ref=piece(st, slot), dst_ref=piece(st, slot),
            send_sem=kv_sib.at[st, index] if st < 2 else send_sem.at[st],
            recv_sem=sib_sem.at[st, index], device_id={"sp": sibling}, device_id_type=MESH,
        )

    def usable(st, direction, step):
        fits = jnp.logical_and(step >= 1, step <= reach(st)[direction])
        return jnp.logical_and(fits, z - step >= 0) if st < 2 else fits

    def source(direction, step):
        return chip(-step if direction == 0 else step)

    def send_own(st, direction):
        link_copy(st, s, direction, 1).start()

    def arrive(st, direction, step):
        @pl.when(usable(st, direction, step))
        def _():
            slot = source(direction, step) * 2 + c
            link_copy(st, slot, direction, step).wait_recv()
            onward = step < reach(st)[direction]

            @pl.when(jnp.logical_and(onward, z < nz - 1) if st < 2 else onward)
            def _():
                link_copy(st, slot, direction, step + 1).start()

            sib_copy(st, slot, step + ways * direction).start()

    def sib_arrive(pair_of, step):
        for st in pair_of:
            for direction in (0, 1):
                @pl.when(usable(st, direction, step))
                def _():
                    slot = source(direction, step) * 2 + 1 - c
                    sib_copy(st, slot, step + ways * direction).wait_recv()

            @pl.when(step == 0)
            def _():
                sib_copy(st, sibling, 0).wait_recv()

    def local(src, dst, index):
        return pltpu.make_async_copy(src, dst, loc_sem.at[index])

    own_slice = pl.ds(pl.multiple_of(t * own_rows, own_rows), own_rows)
    loads = [
        local(k_ref, kbuf.at[s, pl.ds(0, rows)], 0), local(x_ref, kbuf.at[s, pl.ds(rows, 16)], 1),
        local(v_ref, vbuf.at[s], 2), local(g_ref, gbuf.at[s], 3), local(u_ref, ubuf.at[s], 4),
        local(d_ref, dbuf.at[s], 5), local(res_ref.at[own_slice], resv, 6),
    ]
    for load in loads:
        load.start()

    lower = [z == 0, z < nz - 1, c == 1, jnp.logical_not(upper)] + [peer < t for peer in peers]
    axis = ["sp", "sp", "sp", "sp"] + ["tp"] * (n_tp - 1)
    partner = [left, right, sibling, pair] + peers
    theirs = [1, 0, 2, 3] + [3 + n_tp - d for d in range(1, n_tp)]
    barrier = pltpu.get_barrier_semaphore()
    for k in range(3 + n_tp):
        @pl.when(lower[k])
        def _():
            pl.semaphore_signal(barrier, inc=1, device_id={axis[k]: partner[k]}, device_id_type=MESH)

    higher = sum(jnp.where(low, 0, 1) for low in lower)

    @pl.when(higher > 0)
    def _():
        pl.semaphore_wait(barrier, higher)

    for k in range(3 + n_tp):
        @pl.when(jnp.logical_not(lower[k]))
        def _():
            pl.semaphore_signal(
                ack.at[theirs[k]], inc=1, device_id={axis[k]: partner[k]}, device_id_type=MESH
            )

    def ready(k):
        @pl.when(lower[k])
        def _():
            pl.semaphore_wait(ack.at[k], 1)

    kv, gu, dn = (0, 1), (2, 3), (4, 5)
    edge = jnp.logical_or(z == 0, z == nz - 1)
    for load in loads[:3]:
        load.wait()
    ready(1)

    @pl.when(z < nz - 1)
    def _():
        for st in kv:
            send_own(st, 0)

    query_copy = pltpu.make_async_remote_copy(
        src_ref=q_ref, dst_ref=qfar, send_sem=pair_sem.at[0], recv_sem=pair_sem.at[1],
        device_id={"sp": pair}, device_id_type=MESH,
    )

    @pl.when(upper)
    def _():
        query_copy.start()

    for load in loads[3:]:
        load.wait()

    @pl.when(edge)
    def _():
        for st in gu:
            send_own(st, 0)

    ready(2)
    for st in kv:
        sib_copy(st, s, 0).start()
    ready(0)
    for st in gu:
        send_own(st, 1)
    for st in gu + dn:
        sib_copy(st, s, 0).start()

    lane_head = lax.broadcasted_iota(jnp.int32, (rows, width), 1) // head_width

    def prepare(which, ref):
        scaled = ref[...].astype(F32) * (head_width ** -0.5)
        for h in range(heads):
            q4[which, h] = jnp.where(lane_head == h, scaled, 0.0).astype(BF16)
            m_s[which, h] = jnp.full((rows, LANES), -1e30, F32)
            l_s[which, h] = jnp.zeros((rows, LANES), F32)
            acc[which, h] = jnp.zeros((rows, width), F32)

    prepare(0, q_ref)

    def wide(x, size):
        return jnp.concatenate([x] * (size // LANES), axis=1) if size >= LANES else x[:, :size]

    def attend(which, slot, diagonal):
        key = kbuf[slot, 0:rows, :]
        parts = kbuf[slot, rows:rows + 16, :].astype(F32)
        gates = parts[0:heads] + parts[heads:2 * heads] + parts[2 * heads:3 * heads]
        value = vbuf[slot]
        for h in range(heads):
            score = lax.dot_general(q4[which, h], key, NT_DIMS, preferred_element_type=F32) - gates[h:h + 1, :rows]
            if diagonal:
                at = lax.broadcasted_iota(jnp.int32, (rows, rows), 0)
                col = lax.broadcasted_iota(jnp.int32, (rows, rows), 1)
                score = jnp.where(col <= at, score, -1e30)
            before = m_s[which, h]
            top = jnp.maximum(before, jnp.max(score, axis=1, keepdims=True))
            weight = jnp.exp(score - wide(top, rows))
            rescale = jnp.exp(before - top)
            lanes = weight[:, 0:LANES]
            for k in range(1, rows // LANES):
                lanes = lanes + weight[:, k * LANES:(k + 1) * LANES]
            l_s[which, h] = l_s[which, h] * rescale + lanes
            product = jnp.dot(weight.astype(BF16), value, preferred_element_type=F32)
            acc[which, h] = acc[which, h] * wide(rescale, width) + product
            m_s[which, h] = top

    attend(0, s, True)

    ahead_from = near - 1

    def kv_step(i, _):
        for half, st in enumerate(kv):
            arrive(st, 0, i)
            if half == 1:
                @pl.when(jnp.logical_and(jnp.logical_not(edge), i == jnp.minimum(z, near - 1)))
                def _():
                    for own in gu:
                        send_own(own, 0)

                @pl.when(lax.rem(i, 2) == 0)
                def _():
                    for own in gu:
                        arrive(own, 1, jnp.where(i <= near, i // 2, 0))

                @pl.when(i <= far)
                def _():
                    sib_arrive(kv, i - 1)

                @pl.when(jnp.logical_and(i == ahead_from - 1, jnp.logical_not(upper)))
                def _():
                    query_copy.wait_recv()
                    prepare(1, qfar)

            turn = 2 * (i - ahead_from) + half

            def block(b, _):
                which = jnp.where(b == 0, 0, 1)
                j = jnp.where(b == 0, i - 1, turn)
                core = jnp.where(b == 0, c if half == 0 else 1 - c, b - 1)
                fits = jnp.logical_and(jnp.logical_and(j >= 0, j <= near), z - j >= 0)
                own = jnp.logical_or(j > 0, jnp.logical_and(half == 1, c == 1))
                needed = jnp.logical_and(fits, jnp.where(b == 0, own, jnp.logical_not(upper)))

                @pl.when(needed)
                def _():
                    attend(which, chip(-j) * 2 + core, False)

                return 0

            lax.fori_loop(0, 3, block, 0)
        return 0

    lax.fori_loop(1, far + 2, kv_step, 0)

    early = near // 2

    def gu_step(k):
        for st in gu:
            arrive(st, 0, k)
            arrive(st, 1, k + early)

    def merge(which):
        merged = jnp.zeros((rows, width), F32)
        for h in range(heads):
            norm = jnp.sum(l_s[which, h], axis=1, keepdims=True)
            merged = jnp.where(lane_head == h, acc[which, h] / norm, merged)
        return merged

    def far_copy(k):
        return pltpu.make_async_remote_copy(
            src_ref=(osend, ssend)[k], dst_ref=(ofar, sfar)[k], send_sem=pair_sem.at[2 + k],
            recv_sem=pair_sem.at[4 + k], device_id={"sp": pair}, device_id_type=MESH,
        )

    lane = lax.broadcasted_iota(jnp.int32, (rows, LANES), 1)

    @pl.when(jnp.logical_not(upper))
    def _():
        osend[...] = merge(1).astype(BF16)
        stats = jnp.zeros((rows, LANES), F32)
        for h in range(heads):
            stats = jnp.where(lane == h, m_s[1, h], stats)
            stats = jnp.where(lane == heads + h, jnp.sum(l_s[1, h], axis=1, keepdims=True), stats)
        ssend[...] = stats.T[0:2 * heads, :]

    for direction_step in (1,):
        gu_step(direction_step)

    @pl.when(jnp.logical_not(upper))
    def _():
        ready(3)
        for k in (0, 1):
            far_copy(k).start()
        att[...] = merge(0).astype(BF16)

    gu_step(2)

    @pl.when(upper)
    def _():
        for k in (0, 1):
            far_copy(k).wait_recv()
        stats = jnp.concatenate([sfar[...], jnp.zeros((LANES - 2 * heads, rows), F32)], axis=0).T
        other = ofar[...].astype(F32)
        merged = jnp.zeros((rows, width), F32)
        for h in range(heads):
            mine, theirs_max = m_s[0, h][:, 0:1], stats[:, h:h + 1]
            top = jnp.maximum(mine, theirs_max)
            mine_scale = jnp.exp(mine - top)
            theirs_sum = stats[:, heads + h:heads + h + 1] * jnp.exp(theirs_max - top)
            norm = jnp.sum(l_s[0, h], axis=1, keepdims=True) * mine_scale + theirs_sum
            merged = jnp.where(lane_head == h, (acc[0, h] * mine_scale + other * theirs_sum) / norm, merged)
        att[...] = merged.astype(BF16)

    tile = min(512, model)

    def project(k, _):
        at = pl.ds(pl.multiple_of(k * tile, tile), tile)
        y = jnp.dot(att[...], wout_ref[:, at], preferred_element_type=F32).astype(BF16)
        pbuf[:, :, at] = y.reshape(n_tp, own_rows, tile)
        return 0

    lax.fori_loop(0, model // tile, project, 0)

    def reduce_copy(d):
        return pltpu.make_async_remote_copy(
            src_ref=pbuf.at[peers[d]], dst_ref=rsbuf.at[t], send_sem=x_send.at[0], recv_sem=x_recv.at[0, d],
            device_id={"tp": peers[d]}, device_id_type=MESH,
        )

    def gather_copy(d):
        return pltpu.make_async_remote_copy(
            src_ref=nbuf.at[t], dst_ref=nbuf.at[t], send_sem=x_send.at[1], recv_sem=x_recv.at[1, d],
            device_id={"tp": peers[d]}, device_id_type=MESH,
        )

    def arrival(buf, sem):
        return pltpu.make_async_copy(buf, buf, sem)

    gu_step(3)
    for d in range(n_tp - 1):
        ready(4 + d)
        reduce_copy(d).start()
    for k in range(4, near - 1):
        gu_step(k)
    for d in range(n_tp - 1):
        arrival(rsbuf.at[sources[d]], x_recv.at[0, d]).wait()
    summed = resv[...].astype(F32) + pbuf[t].astype(F32)
    for d in range(n_tp - 1):
        summed = summed + rsbuf[sources[d]].astype(F32)
    mixed[...] = summed.astype(BF16)
    floats = mixed[...].astype(F32)
    mean = jnp.sum(floats * floats, axis=1, keepdims=True) * (1.0 / model)
    nbuf[t] = (floats * lax.rsqrt(mean + 1e-6) * gain_ref[...]).astype(BF16)
    for d in range(n_tp - 1):
        gather_copy(d).start()

    gu_step(near - 1)
    for st in dn:
        send_own(st, 1)
        send_own(st, 0)
    gu_step(near)

    def dn_step(k):
        for st in dn:
            for direction in (0, 1):
                arrive(st, direction, k)

    dn_step(1)

    def gu_sib(i, _):
        sib_arrive(gu, i)
        return 0

    lax.fori_loop(0, far + 2, gu_sib, 0)
    for d in range(n_tp - 1):
        arrival(nbuf.at[sources[d]], x_recv.at[1, d]).wait()

    tiles = ff // LANES
    chip_rows = 2 * drow

    def accumulate(offsets, first, final):
        chips = [chip(o) for o in offsets]
        left_side = jnp.concatenate(
            [nbuf[:, :, pl.ds(pl.multiple_of(at * chip_rows, chip_rows), chip_rows)] for at in chips], axis=2
        ).reshape(rows, len(chips) * chip_rows)

        def one(k, _):
            at = pl.ds(pl.multiple_of(k * LANES, LANES), LANES)
            sides = [
                jnp.concatenate(
                    [buf[pl.ds(2 * chosen, 2), :, at].reshape(chip_rows, LANES) for chosen in chips], axis=0
                )
                for buf in (gbuf, ubuf)
            ]
            both = jnp.dot(left_side, jnp.concatenate(sides, axis=1), preferred_element_type=F32)
            if not first:
                both = both + hacc[k]
            if final:
                gate, up = both[:, :LANES], both[:, LANES:]
                hid[:, at] = (gate / (1.0 + jnp.exp(-gate)) * up).astype(BF16)
            else:
                hacc[k] = both
            return 0

        lax.fori_loop(0, tiles, one, 0)

    offsets = [0] + [o for j in range(1, far) for o in (-j, j)] + [far]
    group = -(-len(offsets) // 4)
    for k in range(4):
        accumulate(offsets[k * group:(k + 1) * group], k == 0, k == 3)
        dn_step(k + 2)

    def column_copy(d, at):
        return pltpu.make_async_remote_copy(
            src_ref=dsend.at[at, peers[d]], dst_ref=drecv.at[t, at], send_sem=x_send.at[2],
            recv_sem=x_recv.at[2, d], device_id={"tp": peers[d]}, device_id_type=MESH,
        )

    def down_step(j, _):
        @pl.when(jnp.logical_and(lax.rem(j, 3) == 0, 6 + j // 3 <= far))
        def _():
            dn_step(6 + j // 3)

        sib_arrive(dn, j)
        back, ahead = chip(j), chip(-j)
        weights = jnp.concatenate(
            [dbuf[pl.ds(at * 2, 2)].reshape(2 * drow, ff) for at in (back, ahead)], axis=0
        )
        y = lax.dot_general(hid[...], weights, NT_DIMS, preferred_element_type=F32).astype(BF16)
        y = y.reshape(n_tp, own_rows, 4 * drow)
        dsend[back] = y[:, :, :2 * drow]
        for d in range(n_tp - 1):
            column_copy(d, back).start()

        @pl.when(jnp.logical_and(j >= 1, j <= near))
        def _():
            dsend[ahead] = y[:, :, 2 * drow:]
            for d in range(n_tp - 1):
                column_copy(d, ahead).start()

        return 0

    lax.fori_loop(0, far + 1, down_step, 0)

    for d in range(n_tp - 1):
        arrival(drecv.at[sources[d]], x_recv.at[2, d]).wait()
    square = jnp.zeros((own_rows, 2 * drow), F32)
    for at in range(nz):
        cols = slice(at * 2 * drow, (at + 1) * 2 * drow)
        down = dsend[at, t].astype(F32)
        for d in range(n_tp - 1):
            down = down + drecv[sources[d], at].astype(F32)
        value = mixed[:, cols].astype(F32) + 0.5 * down
        total[:, cols] = value
        square = square + value * value
    mean = jnp.sum(square, axis=1, keepdims=True) * (1.0 / model)
    out_ref[...] = (total[...] * lax.rsqrt(mean + 1e-6)).astype(BF16)

    for st in kv:
        for k in range(near):
            @pl.when(jnp.logical_and(z < nz - 1, z >= k))
            def _():
                link_copy(st, s, 0, k + 1).wait_send()

        for k in range(near + 1):
            @pl.when(z >= k)
            def _():
                sib_copy(st, s, k).wait_send()

    @pl.when(upper)
    def _():
        query_copy.wait_send()

    @pl.when(jnp.logical_not(upper))
    def _():
        for k in (0, 1):
            far_copy(k).wait_send()

    for st in gu + dn:
        buf, start, size = views[st]
        arrival(buf.at[pl.ds(0, 2 * nz - 1), pl.ds(start, size)], send_sem.at[st]).wait()
    arrival(pbuf.at[pl.ds(0, n_tp - 1)], x_send.at[0]).wait()
    arrival(nbuf.at[pl.ds(0, n_tp - 1)], x_send.at[1]).wait()
    arrival(drecv.at[pl.ds(0, n_tp - 1)], x_send.at[2]).wait()


def body(residual, queries, keys, values, log_gates, w_out, norm_gain, w_gate, w_up, w_down):
    n_sp, n_tp = lax.axis_size("sp"), lax.axis_size("tp")
    rows, width = queries.shape
    heads = log_gates.shape[1]
    model = residual.shape[1]
    drow, ff = w_gate.shape
    own_rows = rows // n_tp
    nz = n_sp // 2
    far = nz // 2

    gates = log_gates.T
    high = lax.reduce_precision(gates, 8, 7)
    middle = lax.reduce_precision(gates - high, 8, 7)
    low = gates - high - middle
    extra = jnp.concatenate([high, middle, low, jnp.zeros((16 - 3 * heads, rows), F32)], axis=0).astype(BF16)
    vmem = pl.BlockSpec(memory_space=pltpu.VMEM)
    hbm = pl.BlockSpec(memory_space=pl.ANY)
    return pl.pallas_call(
        functools.partial(layer_kernel, n_sp, n_tp, heads),
        out_shape=jax.ShapeDtypeStruct((own_rows, model), BF16),
        in_specs=[vmem, hbm, hbm, hbm, hbm, vmem, vmem, hbm, hbm, hbm],
        out_specs=vmem,
        scratch_shapes=[
            pltpu.VMEM((n_sp, rows + 16, width), BF16),
            pltpu.VMEM((n_sp, rows, width), BF16),
            pltpu.VMEM((n_sp, drow, ff), BF16),
            pltpu.VMEM((n_sp, drow, ff), BF16),
            pltpu.VMEM((n_sp, drow, ff), BF16),
            pltpu.VMEM((2, heads, rows, width), BF16),
            pltpu.VMEM((2, heads, rows, LANES), F32),
            pltpu.VMEM((2, heads, rows, LANES), F32),
            pltpu.VMEM((2, heads, rows, width), F32),
            pltpu.VMEM((rows, width), BF16),
            pltpu.VMEM((n_tp, own_rows, model), BF16),
            pltpu.VMEM((n_tp, own_rows, model), BF16),
            pltpu.VMEM((own_rows, model), BF16),
            pltpu.VMEM((own_rows, model), BF16),
            pltpu.VMEM((n_tp, own_rows, model), BF16),
            pltpu.VMEM((ff // LANES, rows, 2 * LANES), F32),
            pltpu.VMEM((rows, ff), BF16),
            pltpu.VMEM((nz, n_tp, own_rows, 2 * drow), BF16),
            pltpu.VMEM((n_tp, nz, own_rows, 2 * drow), BF16),
            pltpu.VMEM((own_rows, model), F32),
            pltpu.VMEM((rows, width), BF16),
            pltpu.VMEM((rows, width), BF16),
            pltpu.VMEM((rows, width), BF16),
            pltpu.VMEM((2 * heads, rows), F32),
            pltpu.VMEM((2 * heads, rows), F32),
            pltpu.SemaphoreType.DMA((6,)),
            pltpu.SemaphoreType.DMA((6, 2, far + 1)),
            pltpu.SemaphoreType.DMA((6, nz + far + 2)),
            pltpu.SemaphoreType.DMA((7,)),
            pltpu.SemaphoreType.DMA((3,)),
            pltpu.SemaphoreType.DMA((3, n_tp - 1)),
            pltpu.SemaphoreType.REGULAR((3 + n_tp,)),
            pltpu.SemaphoreType.DMA((2, far)),
            pltpu.SemaphoreType.DMA((2, far)),
            pltpu.SemaphoreType.DMA((6,)),
        ],
        compiler_params=pltpu.CompilerParams(
            collective_id=0, has_side_effects=True, vmem_limit_bytes=60 * 1024 * 1024
        ),
    )(queries, keys, extra, values, residual, w_out, norm_gain.reshape(1, -1), w_gate, w_up, w_down.T)


def solution(mesh):
    in_specs = (
        P(("grp", "sp"), None),
        P(("grp", "sp"), "tp"),
        P(("grp", "sp"), "tp"),
        P(("grp", "sp"), "tp"),
        P(("grp", "sp"), "tp"),
        P("tp", None),
        P(),
        P("sp", "tp"),
        P("sp", "tp"),
        P("tp", "sp"),
    )
    out_specs = P(("grp", "sp", "tp"), None)
    return jax.shard_map(body, mesh=mesh, in_specs=in_specs, out_specs=out_specs, check_vma=False)
```

```python
import functools

import jax
import jax.numpy as jnp
from jax import lax
from jax.experimental import pallas as pl
from jax.experimental.pallas import tpu as pltpu
from jax.sharding import PartitionSpec as P

MESH = pl.DeviceIdType.MESH
F32 = jnp.float32
BF16 = jnp.bfloat16
NT_DIMS = (((1,), (1,)), ((), ()))
LANES = 128


def layer_kernel(
    n_sp, n_tp, heads,
    q_ref, k_ref, x_ref, v_ref, res_ref, wout_ref, gain_ref, g_ref, u_ref, d_ref,
    out_ref,
    kbuf, vbuf, gbuf, ubuf, dbuf, q4, m_s, l_s, acc, att, pbuf, rsbuf, resv, mixed, nbuf, hacc, hid, dsend, drecv, total,
    qfar, ofar, osend, sfar, ssend,
    send_sem, recv_sem, sib_sem, loc_sem, x_send, x_recv, ack, kv_send, kv_sib, pair_sem,
):
    s = lax.axis_index("sp")
    t = lax.axis_index("tp")
    c = lax.rem(s, 2)
    z = s // 2
    nz = n_sp // 2
    far, near = nz // 2, nz - 1 - nz // 2
    rows, width = q_ref.shape
    head_width = width // heads
    own_rows = rows // n_tp
    drow, ff = g_ref.shape
    model = drow * n_sp

    def chip(offset):
        return lax.rem(z + offset + nz, nz)

    right = chip(1) * 2 + c
    left = chip(-1) * 2 + c
    sibling = s + 1 - 2 * c
    pair = chip(far) * 2 + c
    upper = z >= far
    peers = [lax.rem(t + d, n_tp) for d in range(1, n_tp)]
    sources = [lax.rem(t - d + n_tp, n_tp) for d in range(1, n_tp)]

    half = drow // 2
    views = (
        (kbuf, 0, kbuf.shape[1]), (vbuf, 0, vbuf.shape[1]), (gbuf, 0, drow), (ubuf, 0, drow),
        (dbuf, 0, half), (dbuf, half, half),
    )

    def piece(st, slot):
        buf, start, size = views[st]
        return buf.at[slot, pl.ds(start, size)]

    reaches = ((near, 0), (near, 0), (near - 1, far + 1), (near, far), (near, far), (near, far))
    ways = nz

    def reach(st):
        return reaches[st]

    def link_copy(st, slot, direction, step):
        return pltpu.make_async_remote_copy(
            src_ref=piece(st, slot), dst_ref=piece(st, slot),
            send_sem=kv_send.at[st, step - 1] if st < 2 else send_sem.at[st],
            recv_sem=recv_sem.at[st, direction, step - 1],
            device_id={"sp": right if direction == 0 else left}, device_id_type=MESH,
        )

    def sib_copy(st, slot, index):
        return pltpu.make_async_remote_copy(
            src_ref=piece(st, slot), dst_ref=piece(st, slot),
            send_sem=kv_sib.at[st, index] if st < 2 else send_sem.at[st],
            recv_sem=sib_sem.at[st, index], device_id={"sp": sibling}, device_id_type=MESH,
        )

    def usable(st, direction, step):
        fits = jnp.logical_and(step >= 1, step <= reach(st)[direction])
        return jnp.logical_and(fits, z - step >= 0) if st < 2 else fits

    def source(direction, step):
        return chip(-step if direction == 0 else step)

    def send_own(st, direction):
        link_copy(st, s, direction, 1).start()

    def arrive(st, direction, step):
        @pl.when(usable(st, direction, step))
        def _():
            slot = source(direction, step) * 2 + c
            link_copy(st, slot, direction, step).wait_recv()
            onward = step < reach(st)[direction]

            @pl.when(jnp.logical_and(onward, z < nz - 1) if st < 2 else onward)
            def _():
                link_copy(st, slot, direction, step + 1).start()

            sib_copy(st, slot, step + ways * direction).start()

    def sib_arrive(pair_of, step):
        for st in pair_of:
            for direction in (0, 1):
                @pl.when(usable(st, direction, step))
                def _():
                    slot = source(direction, step) * 2 + 1 - c
                    sib_copy(st, slot, step + ways * direction).wait_recv()

            @pl.when(step == 0)
            def _():
                sib_copy(st, sibling, 0).wait_recv()

    def local(src, dst, index):
        return pltpu.make_async_copy(src, dst, loc_sem.at[index])

    own_slice = pl.ds(pl.multiple_of(t * own_rows, own_rows), own_rows)
    loads = [
        local(k_ref, kbuf.at[s, pl.ds(0, rows)], 0), local(x_ref, kbuf.at[s, pl.ds(rows, 16)], 1),
        local(v_ref, vbuf.at[s], 2), local(g_ref, gbuf.at[s], 3), local(u_ref, ubuf.at[s], 4),
        local(d_ref, dbuf.at[s], 5), local(res_ref.at[own_slice], resv, 6),
    ]
    for load in loads:
        load.start()

    lower = [z == 0, z < nz - 1, c == 1, jnp.logical_not(upper)] + [peer < t for peer in peers]
    axis = ["sp", "sp", "sp", "sp"] + ["tp"] * (n_tp - 1)
    partner = [left, right, sibling, pair] + peers
    theirs = [1, 0, 2, 3] + [3 + n_tp - d for d in range(1, n_tp)]
    barrier = pltpu.get_barrier_semaphore()
    for k in range(3 + n_tp):
        @pl.when(lower[k])
        def _():
            pl.semaphore_signal(barrier, inc=1, device_id={axis[k]: partner[k]}, device_id_type=MESH)

    higher = sum(jnp.where(low, 0, 1) for low in lower)

    @pl.when(higher > 0)
    def _():
        pl.semaphore_wait(barrier, higher)

    for k in range(3 + n_tp):
        @pl.when(jnp.logical_not(lower[k]))
        def _():
            pl.semaphore_signal(
                ack.at[theirs[k]], inc=1, device_id={axis[k]: partner[k]}, device_id_type=MESH
            )

    def ready(k):
        @pl.when(lower[k])
        def _():
            pl.semaphore_wait(ack.at[k], 1)

    kv, gu, dn = (0, 1), (2, 3), (4, 5)
    edge = jnp.logical_or(z == 0, z == nz - 1)
    for load in loads[:3]:
        load.wait()
    ready(1)

    @pl.when(z < nz - 1)
    def _():
        for st in kv:
            send_own(st, 0)

    query_copy = pltpu.make_async_remote_copy(
        src_ref=q_ref, dst_ref=qfar, send_sem=pair_sem.at[0], recv_sem=pair_sem.at[1],
        device_id={"sp": pair}, device_id_type=MESH,
    )

    @pl.when(upper)
    def _():
        query_copy.start()

    for load in loads[3:]:
        load.wait()

    @pl.when(edge)
    def _():
        for st in gu:
            send_own(st, 0)

    ready(2)
    for st in kv:
        sib_copy(st, s, 0).start()
    ready(0)
    for st in gu:
        send_own(st, 1)
    for st in gu + dn:
        sib_copy(st, s, 0).start()

    lane_head = lax.broadcasted_iota(jnp.int32, (rows, width), 1) // head_width

    def prepare(which, ref):
        scaled = ref[...].astype(F32) * (head_width ** -0.5)
        for h in range(heads):
            q4[which, h] = jnp.where(lane_head == h, scaled, 0.0).astype(BF16)
            m_s[which, h] = jnp.full((rows, LANES), -1e30, F32)
            l_s[which, h] = jnp.zeros((rows, LANES), F32)
            acc[which, h] = jnp.zeros((rows, width), F32)

    prepare(0, q_ref)

    def wide(x, size):
        return jnp.concatenate([x] * (size // LANES), axis=1) if size >= LANES else x[:, :size]

    def attend(which, slot, diagonal):
        key = kbuf[slot, 0:rows, :]
        parts = kbuf[slot, rows:rows + 16, :].astype(F32)
        gates = parts[0:heads] + parts[heads:2 * heads] + parts[2 * heads:3 * heads]
        value = vbuf[slot]
        for h in range(heads):
            score = lax.dot_general(q4[which, h], key, NT_DIMS, preferred_element_type=F32) - gates[h:h + 1, :rows]
            if diagonal:
                at = lax.broadcasted_iota(jnp.int32, (rows, rows), 0)
                col = lax.broadcasted_iota(jnp.int32, (rows, rows), 1)
                score = jnp.where(col <= at, score, -1e30)
            before = m_s[which, h]
            top = jnp.maximum(before, jnp.max(score, axis=1, keepdims=True))
            weight = jnp.exp(score - wide(top, rows))
            rescale = jnp.exp(before - top)
            lanes = weight[:, 0:LANES]
            for k in range(1, rows // LANES):
                lanes = lanes + weight[:, k * LANES:(k + 1) * LANES]
            l_s[which, h] = l_s[which, h] * rescale + lanes
            product = jnp.dot(weight.astype(BF16), value, preferred_element_type=F32)
            acc[which, h] = acc[which, h] * wide(rescale, width) + product
            m_s[which, h] = top

    attend(0, s, True)

    ahead_from = near - 1

    def kv_step(i, _):
        for half, st in enumerate(kv):
            arrive(st, 0, i)
            if half == 1:
                @pl.when(jnp.logical_and(jnp.logical_not(edge), i == jnp.minimum(z, near - 1)))
                def _():
                    for own in gu:
                        send_own(own, 0)

                @pl.when(lax.rem(i, 2) == 0)
                def _():
                    for own in gu:
                        arrive(own, 1, jnp.where(i <= near, i // 2, 0))

                @pl.when(i <= far)
                def _():
                    sib_arrive(kv, i - 1)

                @pl.when(jnp.logical_and(i == ahead_from - 1, jnp.logical_not(upper)))
                def _():
                    query_copy.wait_recv()
                    prepare(1, qfar)

            turn = 2 * (i - ahead_from) + half

            def block(b, _):
                which = jnp.where(b == 0, 0, 1)
                j = jnp.where(b == 0, i - 1, turn)
                core = jnp.where(b == 0, c if half == 0 else 1 - c, b - 1)
                fits = jnp.logical_and(jnp.logical_and(j >= 0, j <= near), z - j >= 0)
                own = jnp.logical_or(j > 0, jnp.logical_and(half == 1, c == 1))
                needed = jnp.logical_and(fits, jnp.where(b == 0, own, jnp.logical_not(upper)))

                @pl.when(needed)
                def _():
                    attend(which, chip(-j) * 2 + core, False)

                return 0

            lax.fori_loop(0, 3, block, 0)
        return 0

    lax.fori_loop(1, far + 2, kv_step, 0)

    early = near // 2

    def gu_step(k):
        for st in gu:
            arrive(st, 0, k)
            arrive(st, 1, k + early)

    def merge(which):
        merged = jnp.zeros((rows, width), F32)
        for h in range(heads):
            norm = jnp.sum(l_s[which, h], axis=1, keepdims=True)
            merged = jnp.where(lane_head == h, acc[which, h] / norm, merged)
        return merged

    def far_copy(k):
        return pltpu.make_async_remote_copy(
            src_ref=(osend, ssend)[k], dst_ref=(ofar, sfar)[k], send_sem=pair_sem.at[2 + k],
            recv_sem=pair_sem.at[4 + k], device_id={"sp": pair}, device_id_type=MESH,
        )

    lane = lax.broadcasted_iota(jnp.int32, (rows, LANES), 1)

    @pl.when(jnp.logical_not(upper))
    def _():
        osend[...] = merge(1).astype(BF16)
        stats = jnp.zeros((rows, LANES), F32)
        for h in range(heads):
            stats = jnp.where(lane == h, m_s[1, h], stats)
            stats = jnp.where(lane == heads + h, jnp.sum(l_s[1, h], axis=1, keepdims=True), stats)
        ssend[...] = stats.T[0:2 * heads, :]

    for direction_step in (1,):
        gu_step(direction_step)

    @pl.when(jnp.logical_not(upper))
    def _():
        ready(3)
        for k in (0, 1):
            far_copy(k).start()
        att[...] = merge(0).astype(BF16)

    gu_step(2)

    @pl.when(upper)
    def _():
        for k in (0, 1):
            far_copy(k).wait_recv()
        stats = jnp.concatenate([sfar[...], jnp.zeros((LANES - 2 * heads, rows), F32)], axis=0).T
        other = ofar[...].astype(F32)
        merged = jnp.zeros((rows, width), F32)
        for h in range(heads):
            mine, theirs_max = m_s[0, h][:, 0:1], stats[:, h:h + 1]
            top = jnp.maximum(mine, theirs_max)
            mine_scale = jnp.exp(mine - top)
            theirs_sum = stats[:, heads + h:heads + h + 1] * jnp.exp(theirs_max - top)
            norm = jnp.sum(l_s[0, h], axis=1, keepdims=True) * mine_scale + theirs_sum
            merged = jnp.where(lane_head == h, (acc[0, h] * mine_scale + other * theirs_sum) / norm, merged)
        att[...] = merged.astype(BF16)

    tile = min(512, model)

    def project(k, _):
        at = pl.ds(pl.multiple_of(k * tile, tile), tile)
        y = jnp.dot(att[...], wout_ref[:, at], preferred_element_type=F32).astype(BF16)
        pbuf[:, :, at] = y.reshape(n_tp, own_rows, tile)
        return 0

    lax.fori_loop(0, model // tile, project, 0)

    def reduce_copy(d):
        return pltpu.make_async_remote_copy(
            src_ref=pbuf.at[peers[d]], dst_ref=rsbuf.at[t], send_sem=x_send.at[0], recv_sem=x_recv.at[0, d],
            device_id={"tp": peers[d]}, device_id_type=MESH,
        )

    def gather_copy(d):
        return pltpu.make_async_remote_copy(
            src_ref=nbuf.at[t], dst_ref=nbuf.at[t], send_sem=x_send.at[1], recv_sem=x_recv.at[1, d],
            device_id={"tp": peers[d]}, device_id_type=MESH,
        )

    def arrival(buf, sem):
        return pltpu.make_async_copy(buf, buf, sem)

    def gu_half(half, k):
        arrive(gu[half], 0, k)
        arrive(gu[half], 1, k + early)

    gu_half(0, 3)
    for d in range(n_tp - 1):
        ready(4 + d)
        reduce_copy(d).start()
    gu_half(1, 3)
    for k in range(4, near - 2):
        gu_step(k)
    gu_half(0, near - 2)
    for d in range(n_tp - 1):
        arrival(rsbuf.at[sources[d]], x_recv.at[0, d]).wait()
    summed = resv[...].astype(F32) + pbuf[t].astype(F32)
    for d in range(n_tp - 1):
        summed = summed + rsbuf[sources[d]].astype(F32)
    mixed[...] = summed.astype(BF16)
    floats = mixed[...].astype(F32)
    mean = jnp.sum(floats * floats, axis=1, keepdims=True) * (1.0 / model)
    nbuf[t] = (floats * lax.rsqrt(mean + 1e-6) * gain_ref[...]).astype(BF16)
    for d in range(n_tp - 1):
        gather_copy(d).start()

    gu_half(1, near - 2)
    gu_step(near - 1)
    for st in dn:
        send_own(st, 1)
        send_own(st, 0)
    gu_step(near)

    def dn_step(k):
        for st in dn:
            for direction in (0, 1):
                arrive(st, direction, k)

    dn_step(1)

    def gu_sib(i, _):
        sib_arrive(gu, i)
        return 0

    lax.fori_loop(0, far + 2, gu_sib, 0)
    for d in range(n_tp - 1):
        arrival(nbuf.at[sources[d]], x_recv.at[1, d]).wait()

    tiles = ff // LANES
    chip_rows = 2 * drow

    def accumulate(offsets, first, final):
        chips = [chip(o) for o in offsets]
        left_side = jnp.concatenate(
            [nbuf[:, :, pl.ds(pl.multiple_of(at * chip_rows, chip_rows), chip_rows)] for at in chips], axis=2
        ).reshape(rows, len(chips) * chip_rows)

        def one(k, _):
            at = pl.ds(pl.multiple_of(k * LANES, LANES), LANES)
            sides = [
                jnp.concatenate(
                    [buf[pl.ds(2 * chosen, 2), :, at].reshape(chip_rows, LANES) for chosen in chips], axis=0
                )
                for buf in (gbuf, ubuf)
            ]
            both = jnp.dot(left_side, jnp.concatenate(sides, axis=1), preferred_element_type=F32)
            if not first:
                both = both + hacc[k]
            if final:
                gate, up = both[:, :LANES], both[:, LANES:]
                hid[:, at] = (gate / (1.0 + jnp.exp(-gate)) * up).astype(BF16)
            else:
                hacc[k] = both
            return 0

        lax.fori_loop(0, tiles, one, 0)

    offsets = [0] + [o for j in range(1, far) for o in (-j, j)] + [far]
    group = -(-len(offsets) // 4)
    for k in range(4):
        accumulate(offsets[k * group:(k + 1) * group], k == 0, k == 3)
        dn_step(k + 2)

    def column_copy(d, at):
        return pltpu.make_async_remote_copy(
            src_ref=dsend.at[at, peers[d]], dst_ref=drecv.at[t, at], send_sem=x_send.at[2],
            recv_sem=x_recv.at[2, d], device_id={"tp": peers[d]}, device_id_type=MESH,
        )

    def down_step(j, _):
        @pl.when(jnp.logical_and(lax.rem(j, 3) == 0, 6 + j // 3 <= far))
        def _():
            dn_step(6 + j // 3)

        sib_arrive(dn, j)
        back, ahead = chip(j), chip(-j)
        weights = jnp.concatenate(
            [dbuf[pl.ds(at * 2, 2)].reshape(2 * drow, ff) for at in (back, ahead)], axis=0
        )
        y = lax.dot_general(hid[...], weights, NT_DIMS, preferred_element_type=F32).astype(BF16)
        y = y.reshape(n_tp, own_rows, 4 * drow)
        dsend[back] = y[:, :, :2 * drow]
        for d in range(n_tp - 1):
            column_copy(d, back).start()

        @pl.when(jnp.logical_and(j >= 1, j <= near))
        def _():
            dsend[ahead] = y[:, :, 2 * drow:]
            for d in range(n_tp - 1):
                column_copy(d, ahead).start()

        return 0

    lax.fori_loop(0, far + 1, down_step, 0)

    for d in range(n_tp - 1):
        arrival(drecv.at[sources[d]], x_recv.at[2, d]).wait()
    square = jnp.zeros((own_rows, 2 * drow), F32)
    for at in range(nz):
        cols = slice(at * 2 * drow, (at + 1) * 2 * drow)
        down = dsend[at, t].astype(F32)
        for d in range(n_tp - 1):
            down = down + drecv[sources[d], at].astype(F32)
        value = mixed[:, cols].astype(F32) + 0.5 * down
        total[:, cols] = value
        square = square + value * value
    mean = jnp.sum(square, axis=1, keepdims=True) * (1.0 / model)
    out_ref[...] = (total[...] * lax.rsqrt(mean + 1e-6)).astype(BF16)

    for st in kv:
        for k in range(near):
            @pl.when(jnp.logical_and(z < nz - 1, z >= k))
            def _():
                link_copy(st, s, 0, k + 1).wait_send()

        for k in range(near + 1):
            @pl.when(z >= k)
            def _():
                sib_copy(st, s, k).wait_send()

    @pl.when(upper)
    def _():
        query_copy.wait_send()

    @pl.when(jnp.logical_not(upper))
    def _():
        for k in (0, 1):
            far_copy(k).wait_send()

    for st in gu + dn:
        buf, start, size = views[st]
        arrival(buf.at[pl.ds(0, 2 * nz - 1), pl.ds(start, size)], send_sem.at[st]).wait()
    arrival(pbuf.at[pl.ds(0, n_tp - 1)], x_send.at[0]).wait()
    arrival(nbuf.at[pl.ds(0, n_tp - 1)], x_send.at[1]).wait()
    arrival(drecv.at[pl.ds(0, n_tp - 1)], x_send.at[2]).wait()


def body(residual, queries, keys, values, log_gates, w_out, norm_gain, w_gate, w_up, w_down):
    n_sp, n_tp = lax.axis_size("sp"), lax.axis_size("tp")
    rows, width = queries.shape
    heads = log_gates.shape[1]
    model = residual.shape[1]
    drow, ff = w_gate.shape
    own_rows = rows // n_tp
    nz = n_sp // 2
    far = nz // 2

    gates = log_gates.T
    high = lax.reduce_precision(gates, 8, 7)
    middle = lax.reduce_precision(gates - high, 8, 7)
    low = gates - high - middle
    extra = jnp.concatenate([high, middle, low, jnp.zeros((16 - 3 * heads, rows), F32)], axis=0).astype(BF16)
    vmem = pl.BlockSpec(memory_space=pltpu.VMEM)
    hbm = pl.BlockSpec(memory_space=pl.ANY)
    return pl.pallas_call(
        functools.partial(layer_kernel, n_sp, n_tp, heads),
        out_shape=jax.ShapeDtypeStruct((own_rows, model), BF16),
        in_specs=[vmem, hbm, hbm, hbm, hbm, vmem, vmem, hbm, hbm, hbm],
        out_specs=vmem,
        scratch_shapes=[
            pltpu.VMEM((n_sp, rows + 16, width), BF16),
            pltpu.VMEM((n_sp, rows, width), BF16),
            pltpu.VMEM((n_sp, drow, ff), BF16),
            pltpu.VMEM((n_sp, drow, ff), BF16),
            pltpu.VMEM((n_sp, drow, ff), BF16),
            pltpu.VMEM((2, heads, rows, width), BF16),
            pltpu.VMEM((2, heads, rows, LANES), F32),
            pltpu.VMEM((2, heads, rows, LANES), F32),
            pltpu.VMEM((2, heads, rows, width), F32),
            pltpu.VMEM((rows, width), BF16),
            pltpu.VMEM((n_tp, own_rows, model), BF16),
            pltpu.VMEM((n_tp, own_rows, model), BF16),
            pltpu.VMEM((own_rows, model), BF16),
            pltpu.VMEM((own_rows, model), BF16),
            pltpu.VMEM((n_tp, own_rows, model), BF16),
            pltpu.VMEM((ff // LANES, rows, 2 * LANES), F32),
            pltpu.VMEM((rows, ff), BF16),
            pltpu.VMEM((nz, n_tp, own_rows, 2 * drow), BF16),
            pltpu.VMEM((n_tp, nz, own_rows, 2 * drow), BF16),
            pltpu.VMEM((own_rows, model), F32),
            pltpu.VMEM((rows, width), BF16),
            pltpu.VMEM((rows, width), BF16),
            pltpu.VMEM((rows, width), BF16),
            pltpu.VMEM((2 * heads, rows), F32),
            pltpu.VMEM((2 * heads, rows), F32),
            pltpu.SemaphoreType.DMA((6,)),
            pltpu.SemaphoreType.DMA((6, 2, far + 1)),
            pltpu.SemaphoreType.DMA((6, nz + far + 2)),
            pltpu.SemaphoreType.DMA((7,)),
            pltpu.SemaphoreType.DMA((3,)),
            pltpu.SemaphoreType.DMA((3, n_tp - 1)),
            pltpu.SemaphoreType.REGULAR((3 + n_tp,)),
            pltpu.SemaphoreType.DMA((2, far)),
            pltpu.SemaphoreType.DMA((2, far)),
            pltpu.SemaphoreType.DMA((6,)),
        ],
        compiler_params=pltpu.CompilerParams(
            collective_id=0, has_side_effects=True, vmem_limit_bytes=60 * 1024 * 1024
        ),
    )(queries, keys, extra, values, residual, w_out, norm_gain.reshape(1, -1), w_gate, w_up, w_down.T)


def solution(mesh):
    in_specs = (
        P(("grp", "sp"), None),
        P(("grp", "sp"), "tp"),
        P(("grp", "sp"), "tp"),
        P(("grp", "sp"), "tp"),
        P(("grp", "sp"), "tp"),
        P("tp", None),
        P(),
        P("sp", "tp"),
        P("sp", "tp"),
        P("tp", "sp"),
    )
    out_specs = P(("grp", "sp", "tp"), None)
    return jax.shard_map(body, mesh=mesh, in_specs=in_specs, out_specs=out_specs, check_vma=False)
```
